32 devices in a mesh: fs: 8 (over z, y), tp: 4 (over x, core).
Axes of the slice: x: 2, y: 2, z: 4, core: 2. Of those that a mesh axis runs over, the one named last changes fastest.
Arguments:
- tokens: bfloat16 [1280, 2048], P('fs', 'tp'), may hold values from -6 to 6
- mix_gain: float32 [2048], replicated, may hold values from 0.1 to 1.9
- in_x_w: bfloat16 [2048, 1024], P('fs', 'tp'), may hold values from -0.125 to 0.125
- in_gate_w: bfloat16 [2048, 1024], P('fs', 'tp'), may hold values from -0.125 to 0.125
- conv_taps: float32 [4, 1024], P(None, 'tp'), may hold values from -3 to 3
- gate_x_blocks: bfloat16 [8, 128, 128], P('tp'), may hold values from -0.5 to 0.5
- gate_a_blocks: bfloat16 [8, 128, 128], P('tp'), may hold values from -0.5 to 0.5
- forget_rate: float32 [1024], P('tp'), may hold values from 0.002 to 0.08
- out_w: bfloat16 [1024, 2048], P('tp', 'fs'), may hold values from -0.1875 to 0.1875
- ffn_gain: float32 [2048], replicated, may hold values from 0.1 to 1.9
- ffn_gate_w: bfloat16 [2048, 2816], P('fs', 'tp'), may hold values from -0.125 to 0.125
- ffn_up_w: bfloat16 [2048, 2816], P('fs', 'tp'), may hold values from -0.125 to 0.125
- ffn_down_w: bfloat16 [2816, 2048], P('tp', 'fs'), may hold values from -0.109375 to 0.109375
Outputs:
- layer_out: bfloat16 [1280, 2048], P('fs', 'tp')
The draws below stay inside these ranges and needn't reach their ends.
All inputs are finite; a program needn't handle non-finite values.
Results may differ from the reference program's by a relative error of at most 0.015.
Values may be sent and summed in bfloat16 or wider, within the bound.
A program may use at most 64 MiB of HBM per device.

```python
import math
import jax
import jax.numpy as jnp
from jax import lax

D = 2048
BLOCK_DIM = 128
RG_BLOCKS = 8
RG = 1024
FF = 2816
TAPS = 4
TOK_DEV = 160
TOKENS = 1280
N_FS = 8
N_TP = 4


def steps_of(stream_key, shape, pieces, least, top_value):
    loudness, own = 1.0, jax.random.fold_in(stream_key, 6)
    for position, blocks in pieces:
        steps = jnp.exp(jax.random.uniform(jax.random.fold_in(own, position), (blocks,), jnp.float32, least / len(pieces), top_value / len(pieces)))
        loudness = loudness * jnp.repeat(steps, shape[position] // blocks).reshape([-1 if axis == position else 1 for axis in range(len(shape))])
    return loudness


def scatter_about(stream_key, dims, spread, limit, pieces=(), dtype=jnp.bfloat16):
    result = spread * jax.random.normal(stream_key, dims, jnp.float32)
    if pieces:
        result = result * steps_of(stream_key, dims, pieces, -0.22, 0.18)
    return jnp.clip(result, -limit, limit).astype(dtype)


def setup_inputs(seed: int = 0) -> dict:
    streams_of = jax.random.split(jax.random.key(seed), 14)
    return {
        "tokens": scatter_about(streams_of[0], (TOKENS, D), 1.0, 6.0, ((0, 8), (1, 4))),
        "mix_gain": jnp.clip(1.0 + 0.18 * jax.random.normal(streams_of[1], (D,), jnp.float32), 0.1, 1.9),
        "in_x_w": scatter_about(streams_of[2], (D, RG), D ** -0.5, 0.125, ((0, 8), (1, 4))),
        "in_gate_w": scatter_about(streams_of[3], (D, RG), D ** -0.5, 0.125, ((0, 8), (1, 4))),
        "conv_taps": scatter_about(streams_of[4], (TAPS, RG), TAPS ** -0.5, 3.0, ((1, 4),), jnp.float32),
        "gate_x_blocks": scatter_about(streams_of[5], (RG_BLOCKS, BLOCK_DIM, BLOCK_DIM), BLOCK_DIM ** -0.5, 0.5, ((0, 4),)),
        "gate_a_blocks": scatter_about(streams_of[6], (RG_BLOCKS, BLOCK_DIM, BLOCK_DIM), BLOCK_DIM ** -0.5, 0.5, ((0, 4),)),
        "forget_rate": jnp.clip(jnp.exp(math.log(0.08) - 3.6888794 * jax.random.uniform(streams_of[7], (RG,), jnp.float32) ** steps_of(streams_of[7], (RG,), ((0, 4),), -0.2, 0.2)), 0.002, 0.08),
        "out_w": scatter_about(streams_of[8], (RG, D), RG ** -0.5, 0.1875, ((0, 4), (1, 8))),
        "ffn_gain": jnp.clip(1.0 + 0.18 * jax.random.normal(streams_of[9], (D,), jnp.float32), 0.1, 1.9),
        "ffn_gate_w": scatter_about(streams_of[10], (D, FF), D ** -0.5, 0.125, ((0, 8), (1, 4))),
        "ffn_up_w": scatter_about(streams_of[11], (D, FF), D ** -0.5, 0.125, ((0, 8), (1, 4))),
        "ffn_down_w": scatter_about(streams_of[12], (FF, D), FF ** -0.5, 0.109375, ((0, 4), (1, 8))),
    }


epsilon = 1e-06
gate_power = 8.0

def rms_norm(values, gain):
    wide = values.astype(jnp.float32)
    mean_square = lax.optimization_barrier(jnp.mean(wide * wide, axis=-1, keepdims=True))
    return (wide * lax.rsqrt(mean_square + epsilon) * gain).astype(jnp.bfloat16)

def grouped_sum(acts, weight):
    group_width = acts.shape[1] // N_TP
    total = jnp.zeros((acts.shape[0], weight.shape[1]), jnp.float32)
    for index in range(N_TP):
        part = jnp.dot(acts[:, index * group_width:(index + 1) * group_width], weight[index * group_width:(index + 1) * group_width], preferred_element_type=jnp.float32)
        part = lax.optimization_barrier(part.astype(jnp.bfloat16))
        total = total + part.astype(jnp.float32)
    return total

def combine(earlier, later):
    return (earlier[0] * later[0], later[0] * earlier[1] + later[1])

def reference(tokens, mix_gain, in_x_w, in_gate_w, conv_taps, gate_x_blocks, gate_a_blocks, forget_rate, out_w, ffn_gain, ffn_gate_w, ffn_up_w, ffn_down_w):
    normed = rms_norm(tokens, mix_gain)
    branch_in = jnp.dot(normed, in_x_w, preferred_element_type=jnp.float32).reshape(N_FS, TOK_DEV, RG)
    branch_gate = jnp.dot(normed, in_gate_w, preferred_element_type=jnp.float32).reshape(N_FS, TOK_DEV, RG)
    padded = jnp.pad(branch_in, ((0, 0), (TAPS - 1, 0), (0, 0)))
    conv_sum = padded[:, 0:TOK_DEV] * conv_taps[0]
    for index in range(1, TAPS):
        conv_sum = conv_sum + padded[:, index:index + TOK_DEV] * conv_taps[index]
    conv_out = conv_sum.astype(jnp.bfloat16)
    grouped = conv_out.reshape(N_FS, TOK_DEV, RG_BLOCKS, BLOCK_DIM).astype(jnp.float32)
    gate_x = jax.nn.sigmoid(jnp.einsum('stbi,bij->stbj', grouped, gate_x_blocks.astype(jnp.float32)).reshape(N_FS, TOK_DEV, RG))
    gate_a = jax.nn.sigmoid(jnp.einsum('stbi,bij->stbj', grouped, gate_a_blocks.astype(jnp.float32)).reshape(N_FS, TOK_DEV, RG))
    log_decay = -gate_power * gate_a * forget_rate
    decay = jnp.exp(log_decay)
    scale = jnp.sqrt(-jnp.expm1(2.0 * log_decay))
    first = (jnp.arange(TOK_DEV) == 0)[None, :, None]
    scale = jnp.where(first, 1.0, scale)
    driven = conv_out.astype(jnp.float32) * gate_x * scale
    _, state = lax.associative_scan(combine, (decay, driven), axis=1)
    mixer_out = (state * jax.nn.gelu(branch_gate)).reshape(TOKENS, RG).astype(jnp.bfloat16)
    after_mix = (tokens.astype(jnp.float32) + grouped_sum(mixer_out, out_w)).astype(jnp.bfloat16)
    normed_ffn = rms_norm(after_mix, ffn_gain)
    gate_val = jnp.dot(normed_ffn, ffn_gate_w, preferred_element_type=jnp.float32)
    up_val = jnp.dot(normed_ffn, ffn_up_w, preferred_element_type=jnp.float32)
    hidden = (jax.nn.silu(gate_val) * up_val).astype(jnp.bfloat16)
    return (after_mix.astype(jnp.float32) + grouped_sum(hidden, ffn_down_w)).astype(jnp.bfloat16)
```

```python
import functools

import jax
import jax.numpy as jnp
from jax import lax
from jax.experimental import pallas as pl
from jax.experimental.pallas import tpu as pltpu
from jax.sharding import PartitionSpec as P

LANES = 128

epsilon = 1e-06
gate_power = 8.0


def rms_norm(values, gain):
    wide = values.astype(jnp.float32)
    mean_square = jnp.mean(wide * wide, axis=-1, keepdims=True)
    return (wide * lax.rsqrt(mean_square + epsilon) * gain).astype(jnp.bfloat16)


def full_rows(shard):
    return lax.all_gather(shard, "tp", axis=1, tiled=True)


def pair_folder(left_rows, pieces):
    return (
        jnp.dot(left_rows, pieces[0], preferred_element_type=jnp.float32),
        jnp.dot(left_rows, pieces[1], preferred_element_type=jnp.float32),
    )


def project_out(acts, weight):
    partial_terms = jnp.dot(
        acts, lax.all_gather(weight, "fs", axis=1, tiled=True), preferred_element_type=jnp.float32
    )
    return lax.psum_scatter(
        partial_terms.astype(jnp.bfloat16), "tp", scatter_dimension=1, tiled=True
    ).astype(jnp.float32)


def combine(earlier, later):
    return (earlier[0] * later[0], later[0] * earlier[1] + later[1])


def on_device(
    tokens,
    mix_gain,
    in_x_w,
    in_gate_w,
    conv_taps,
    gate_x_blocks,
    gate_a_blocks,
    forget_rate,
    out_w,
    ffn_gain,
    ffn_gate_w,
    ffn_up_w,
    ffn_down_w,
):
    normed = rms_norm(full_rows(tokens), mix_gain)
    length = normed.shape[0]
    chan_width = in_x_w.shape[1]
    branch_in, branch_gate = pair_folder(
        normed,
        (
            lax.all_gather(in_x_w, "fs", axis=0, tiled=True),
            lax.all_gather(in_gate_w, "fs", axis=0, tiled=True),
        ),
    )
    tap_count = conv_taps.shape[0]
    padded = jnp.pad(branch_in, ((tap_count - 1, 0), (0, 0)))
    conv_sum = padded[0:length] * conv_taps[0]
    for index in range(1, tap_count):
        conv_sum = conv_sum + padded[index : index + length] * conv_taps[index]
    conv_out = conv_sum.astype(jnp.bfloat16)
    blocks = gate_x_blocks.shape[0]
    block_dim = gate_x_blocks.shape[1]
    grouped = conv_out.reshape(length, blocks, block_dim)
    gate_x = jax.nn.sigmoid(
        jnp.einsum(
            "tbi,bij->tbj", grouped, gate_x_blocks, preferred_element_type=jnp.float32
        ).reshape(length, chan_width)
    )
    gate_a = jax.nn.sigmoid(
        jnp.einsum(
            "tbi,bij->tbj", grouped, gate_a_blocks, preferred_element_type=jnp.float32
        ).reshape(length, chan_width)
    )
    log_decay = -gate_power * gate_a * forget_rate
    decay = jnp.exp(log_decay)
    scale = jnp.sqrt(-jnp.expm1(2.0 * log_decay))
    scale = jnp.where((jnp.arange(length) == 0)[:, None], 1.0, scale)
    driven = conv_out.astype(jnp.float32) * gate_x * scale
    _, state = lax.associative_scan(combine, (decay, driven), axis=0)
    mixer_out = (state * jax.nn.gelu(branch_gate)).astype(jnp.bfloat16)
    after_mix = (tokens.astype(jnp.float32) + project_out(mixer_out, out_w)).astype(jnp.bfloat16)
    normed_ffn = rms_norm(full_rows(after_mix), ffn_gain)
    gate_val, up_val = pair_folder(
        normed_ffn,
        (
            lax.all_gather(ffn_gate_w, "fs", axis=0, tiled=True),
            lax.all_gather(ffn_up_w, "fs", axis=0, tiled=True),
        ),
    )
    hidden = (jax.nn.silu(gate_val) * up_val).astype(jnp.bfloat16)
    return (after_mix.astype(jnp.float32) + project_out(hidden, ffn_down_w)).astype(jnp.bfloat16)


def paired(mesh, tokens, mix_gain, in_x_w, in_gate_w, conv_taps, gate_x_blocks, *rest):
    ffn_down_w = rest[-1]
    return (
        mesh.shape["fs"] == 8
        and mesh.shape["tp"] == 4
        and gate_x_blocks.shape == (2, LANES, LANES)
        and tokens.shape[0] % 16 == 0
        and tokens.shape[1] % (2 * LANES) == 0
        and ffn_down_w.shape[0] % 32 == 0
    )


def kernel(
    h_tok, h_gain1, h_x, h_g, h_taps, h_gxb, h_gab, h_forget, h_out, h_gain2, h_gate, h_up, h_dn,
    result,
    tok, gain1, w_x, w_g, taps, gxb, gab, forget, w_out, gain2, w_gate, w_up, w_dn, load_sem,
    x1, nb, win, wout, wgate, wup, wdn, s1, s1r, k1, x1r, zs1, z1r, after, mix, x2, hid,
    s2, s2r, k2, x2r, zs2, z2r,
    send_z, recv_z, send_y, recv_y, own_sem, ag_send, ag_recv, rs_send, rs_recv,
):
    f, t = lax.axis_index("fs"), lax.axis_index("tp")
    z, y = f // 2, f % 2
    h = z % 2
    rows, feats = tok.shape
    zs = (z, z + 1 - 2 * h, (z + 2) % 4, 3 - z)
    fz = tuple(zz * 2 + y for zz in zs)
    fy = z * 2 + 1 - y
    t_core = t + 1 - 2 * (t % 2)
    t_x = (t + 2) % 4
    t_xc = (t_core + 2) % 4
    model = x1.shape[1]

    held = (tok, w_x, w_g, w_out, w_gate, w_up, w_dn, gain1, taps, gxb, gab, forget, gain2)
    given = (h_tok, h_x, h_g, h_out, h_gate, h_up, h_dn, h_gain1, h_taps, h_gxb, h_gab, h_forget, h_gain2)
    loads = [pltpu.make_async_copy(src, dst, load_sem.at[i]) for i, (src, dst) in enumerate(zip(given, held))]
    for load in loads:
        load.start()

    barrier = pltpu.get_barrier_semaphore()
    peers = [(fz[1], t), (fz[2], t), (fz[3], t), (fy, t), (f, t_core), (f, t_x)]
    for peer in peers:
        pl.semaphore_signal(barrier, inc=1, device_id=peer, device_id_type=pl.DeviceIdType.MESH)
    pl.semaphore_wait(barrier, len(peers))

    started = []

    def send(src, dst, s_sem, r_sem, peer):
        copy = pltpu.make_async_remote_copy(
            src_ref=src, dst_ref=dst, send_sem=s_sem, recv_sem=r_sem,
            device_id=peer, device_id_type=pl.DeviceIdType.MESH,
        )
        copy.start()
        started.append(copy)
        return copy

    def span(index, width):
        return pl.ds(pl.multiple_of(index * width, width), width)

    depth = w_x.shape[0]
    cols = w_out.shape[1]
    half_ff = w_dn.shape[0] // 2
    fill = wdn.shape[0] - half_ff

    def piece(group, half, stored=False):
        if group < 2:
            return ((h_x, h_g) if stored else (w_x, w_g))[group].at[:, span(half, LANES)]
        if group == 2:
            return (h_out if stored else w_out).at[span(half, LANES), :]
        return ((h_gate, h_up, h_dn) if stored else (w_gate, w_up, w_dn))[group - 3].at[span(half, half_ff), :]

    def place(group, source):
        if group < 2:
            return win.at[span(source, depth), pl.ds(group * LANES, LANES)]
        if group == 2:
            return wout.at[:, span(source, cols)]
        return (wgate, wup, wdn)[group - 3].at[pl.ds(0, half_ff), span(source, cols)]

    own_copies = {}
    z_copies = {}
    y_copies = {}

    for group in range(6):
        own_copies[group] = pltpu.make_async_copy(piece(group, h, True), place(group, f), own_sem.at[group])
        own_copies[group].start()

    def launch(group):
        for d in (1, 2, 3):
            half = h if d == 2 else 1 - h
            z_copies[group, d] = send(
                piece(group, half), place(group, f), send_z.at[group, d - 1], recv_z.at[group, d - 1], (fz[d], t)
            )
            if d == 1:
                y_copies[group, 0] = send(
                    piece(group, h), place(group, f), send_y.at[group, 0], recv_y.at[group, 0], (fy, t)
                )

    def forward(group, d):
        z_copies[group, d].wait_recv()
        y_copies[group, d] = send(
            place(group, fz[d]), place(group, fz[d]), send_y.at[group, d], recv_y.at[group, d], (fy, t)
        )

    def arrive(group):
        own_copies[group].wait()
        for d in range(4):
            y_copies[group, d].wait_recv()

    cut = feats // 2
    mine, theirs = span(h, rows), span(1 - h, rows)

    def gather_start(k, own, x):
        def go(i, r, c, peer):
            src = own if i < 3 else x.at[r, span(c, feats)]
            return send(src, x.at[r, span(c, feats)], ag_send.at[k, i], ag_recv.at[k, i], peer)

        x_peer, core_peer = (f, t_x), (f, t_core)
        first = go(0, mine, t, (fz[1], t)), go(1, mine, t, x_peer), go(2, mine, t, core_peer)
        x[mine, span(t, feats)] = own[...]
        return go, first, x_peer, core_peer

    def gather_rest(state, hooks):
        go, (by_z, by_x, by_core), x_peer, core_peer = state
        by_z.wait_recv()
        c3 = go(3, theirs, t, x_peer)
        c4 = go(4, theirs, t, core_peer)
        hooks[0]()
        by_x.wait_recv()
        c5 = go(5, mine, t_x, core_peer)
        hooks[1]()
        c3.wait_recv()
        c6 = go(6, theirs, t_x, core_peer)
        hooks[2]()
        for c in (by_core, c4, c5, c6):
            c.wait_recv()

    def norm(x, gain, out):
        step = 32

        def one(i, carry):
            at = pl.ds(pl.multiple_of(i * step, step), step)
            wide = x[at, :].astype(jnp.float32)
            scale = lax.rsqrt(jnp.mean(wide * wide, axis=-1, keepdims=True) + epsilon)
            out[at, :] = (wide * scale * gain[...]).astype(jnp.bfloat16)
            return carry

        lax.fori_loop(0, x.shape[0] // step, one, 0)

    def scatter(k, acts, weight, s, r1, keep, r2, s3, r3, base, out, hooks):
        core_peer, x_peer = (f, t_core), (f, t_x)

        def project(block):
            at = span(block, feats)
            s[:, at] = jnp.dot(acts[...], weight[:, at], preferred_element_type=jnp.float32).astype(jnp.bfloat16)
            return s.at[:, at]

        a = send(project(t_xc), r1.at[0], rs_send.at[k, 0], rs_recv.at[k, 0], core_peer)
        b = send(project(t_core), r1.at[1], rs_send.at[k, 1], rs_recv.at[k, 1], core_peer)
        project(t_x)
        project(t)
        hooks[0]()
        a.wait_recv()
        keep[0] = (s[:, span(t_x, feats)].astype(jnp.float32) + r1[0].astype(jnp.float32)).astype(jnp.bfloat16)
        c0 = send(keep.at[0, theirs], r2.at[theirs], rs_send.at[k, 2], rs_recv.at[k, 2], x_peer)
        c1 = send(keep.at[0, mine], r2.at[mine], rs_send.at[k, 3], rs_recv.at[k, 3], x_peer)
        b.wait_recv()
        hooks[1]()
        c0.wait_recv()

        def total(where):
            return (
                s[where, span(t, feats)].astype(jnp.float32)
                + r1[1, where, :].astype(jnp.float32)
                + r2[where, :].astype(jnp.float32)
            )

        s3[...] = total(theirs).astype(jnp.bfloat16)
        e = send(s3, r3, rs_send.at[k, 4], rs_recv.at[k, 4], (fz[1], t))
        c1.wait_recv()
        part = total(mine)
        hooks[2]()
        e.wait_recv()
        out[...] = (base[...].astype(jnp.float32) + (part + r3[...].astype(jnp.float32))).astype(jnp.bfloat16)

    def finish(k, acts, weight, s, r1, keep, r2, s3, r3, base, out):
        core_peer, x_peer, z_peer = (f, t_core), (f, t_x), (fz[1], t)
        low, high = pl.ds(0, cut), pl.ds(cut, feats - cut)

        def project(block):
            at = span(block, feats)
            s[:, at] = jnp.dot(acts[...], weight[:, at], preferred_element_type=jnp.float32).astype(jnp.bfloat16)
            return s.at[:, at]

        def go(i, src, dst, peer):
            return send(src, dst, rs_send.at[k, i], rs_recv.at[k, i], peer)

        def pair_sum(block, i):
            return s[:, span(block, feats)].astype(jnp.float32) + r1[i].astype(jnp.float32)

        a = go(0, project(t_xc), r1.at[0], core_peer)
        b = go(1, project(t_core), r1.at[1], core_peer)
        project(t_x)
        project(t)
        a.wait_recv()
        keep[0] = pair_sum(t_x, 0).astype(jnp.bfloat16)
        c = go(2, keep.at[0, :, low], r2.at[:, low], x_peer)
        d = go(3, keep.at[0, theirs, high], r3.at[0, :, high], z_peer)
        b.wait_recv()
        keep[1] = pair_sum(t, 1).astype(jnp.bfloat16)
        e = go(4, keep.at[1, theirs, high], r3.at[1, :, high], z_peer)
        d.wait_recv()
        s3[:, high] = (
            keep[0, mine, high].astype(jnp.float32) + r3[0, :, high].astype(jnp.float32)
        ).astype(jnp.bfloat16)
        g = go(5, s3.at[:, high], r2.at[pl.ds(0, rows), high], x_peer)
        c.wait_recv()
        s3[:, low] = (
            keep[1, theirs, low].astype(jnp.float32) + r2[theirs, low].astype(jnp.float32)
        ).astype(jnp.bfloat16)
        l = go(6, s3.at[:, low], r3.at[0, :, low], z_peer)
        e.wait_recv()
        g.wait_recv()
        out[:, high] = (
            base[:, high].astype(jnp.float32)
            + (keep[1, mine, high].astype(jnp.float32) + r3[1, :, high].astype(jnp.float32))
            + r2[pl.ds(0, rows), high].astype(jnp.float32)
        ).astype(jnp.bfloat16)
        l.wait_recv()
        out[:, low] = (
            base[:, low].astype(jnp.float32)
            + (keep[1, mine, low].astype(jnp.float32) + r2[mine, low].astype(jnp.float32))
            + r3[0, :, low].astype(jnp.float32)
        ).astype(jnp.bfloat16)

    def forwards(*pairs):
        def go():
            for group, d in pairs:
                forward(group, d)

        return go

    loads[0].wait()
    state = gather_start(0, tok, x1)
    for group in range(5):
        loads[1 + group].wait()
        launch(group)
    for load in loads[6:]:
        load.wait()
    if fill:
        for w in (wgate, wup, wdn):
            w[pl.ds(half_ff, fill), :] = jnp.zeros((fill, model), jnp.bfloat16)
    gather_rest(state, (forwards((0, 1), (1, 1)), forwards((0, 2), (1, 2)), forwards((0, 3), (1, 3))))
    norm(x1, gain1, nb)
    forwards((2, 1), (2, 2), (2, 3))()
    arrive(0)
    arrive(1)
    forward(3, 1)
    both = jnp.dot(nb[...], win[...], preferred_element_type=jnp.float32)
    branch_in, branch_gate = both[:, :LANES], both[:, LANES:]
    row = lax.broadcasted_iota(jnp.int32, branch_in.shape, 0)
    pos = jnp.where(row >= rows, row - rows, row)

    def shifted(values, by, fill):
        return jnp.where(pos >= by, pltpu.roll(values, by, 0), fill)

    tap_count = taps.shape[0]
    my = span(h, LANES)
    conv = branch_in * taps[tap_count - 1 :, my]
    for j in range(tap_count - 1):
        conv = conv + shifted(branch_in, tap_count - 1 - j, 0.0) * taps[j : j + 1, my]
    conv = conv.astype(jnp.bfloat16)
    gate_x = jax.nn.sigmoid(jnp.dot(conv, gxb[h], preferred_element_type=jnp.float32))
    gate_a = jax.nn.sigmoid(jnp.dot(conv, gab[h], preferred_element_type=jnp.float32))
    log_decay = -gate_power * gate_a * forget[:, my]
    decay = jnp.exp(log_decay)
    scale = jnp.sqrt(-jnp.tanh(log_decay) * (1.0 + decay * decay))
    scale = jnp.where(pos == 0, 1.0, scale)
    run = conv.astype(jnp.float32) * gate_x * scale
    by = 1
    while by < rows:
        run = decay * shifted(run, by, 0.0) + run
        decay = decay * shifted(decay, by, 1.0)
        by *= 2
    mix[...] = (run * jax.nn.gelu(branch_gate)).astype(jnp.bfloat16)
    arrive(2)
    forward(3, 2)
    scatter(
        0, mix, wout, s1, s1r, k1, x1r, zs1, z1r, tok, after,
        (forwards((3, 3)), forwards((4, 1)), forwards((4, 2))),
    )
    state = gather_start(1, after, x2)
    launch(5)
    gather_rest(state, (forwards((4, 3)), forwards(), forwards((5, 1))))
    norm(x2, gain2, nb)
    forward(5, 2)
    arrive(3)
    arrive(4)
    forward(5, 3)
    last = (((1,), (1,)), ((), ()))

    def ffn(i, carry):
        at = span(i, LANES)
        gate_val = lax.dot_general(nb[...], wgate[at, :], last, preferred_element_type=jnp.float32)
        up_val = lax.dot_general(nb[...], wup[at, :], last, preferred_element_type=jnp.float32)
        hid[:, at] = (jax.nn.silu(gate_val) * up_val).astype(jnp.bfloat16)
        return carry

    lax.fori_loop(0, wgate.shape[0] // LANES, ffn, 0)
    arrive(5)
    finish(1, hid, wdn, s2, s2r, k2, x2r, zs2, z2r, after, result)
    for copy in started:
        copy.wait_send()


def on_device_paired(
    tokens, mix_gain, in_x_w, in_gate_w, conv_taps, gate_x_blocks, gate_a_blocks, forget_rate,
    out_w, ffn_gain, ffn_gate_w, ffn_up_w, ffn_down_w,
):
    rows, feats = tokens.shape
    model = mix_gain.shape[0]
    both = 2 * rows
    wide = -(-ffn_down_w.shape[0] // (2 * LANES)) * LANES
    bf, dma = jnp.bfloat16, pltpu.SemaphoreType.DMA
    exchange = [
        pltpu.VMEM((both, model), bf),
        pltpu.VMEM((2, both, feats), bf),
        pltpu.VMEM((2, both, feats), bf),
        pltpu.VMEM((both, feats), bf),
    ]
    vmem = pl.BlockSpec(memory_space=pltpu.VMEM)
    operands = (
        tokens, mix_gain.reshape(1, model), in_x_w, in_gate_w, conv_taps, gate_x_blocks, gate_a_blocks,
        forget_rate.reshape(1, -1), out_w, ffn_gain.reshape(1, model), ffn_gate_w.T, ffn_up_w.T, ffn_down_w,
    )
    return pl.pallas_call(
        kernel,
        out_shape=jax.ShapeDtypeStruct((rows, feats), bf),
        in_specs=[pl.BlockSpec(memory_space=pltpu.HBM)] * 13,
        out_specs=vmem,
        scratch_shapes=[
            *[pltpu.VMEM(operand.shape, operand.dtype) for operand in operands],
            dma((13,)),
            pltpu.VMEM((both, model), bf),
            pltpu.VMEM((both, model), bf),
            pltpu.VMEM((model, 2 * LANES), bf),
            pltpu.VMEM((LANES, model), bf),
            pltpu.VMEM((wide, model), bf),
            pltpu.VMEM((wide, model), bf),
            pltpu.VMEM((wide, model), bf),
            *exchange,
            pltpu.VMEM((rows, feats), bf),
            pltpu.VMEM((rows, feats), bf),
            pltpu.VMEM((rows, feats), bf),
            pltpu.VMEM((both, LANES), bf),
            pltpu.VMEM((both, model), bf),
            pltpu.VMEM((both, wide), bf),
            *exchange,
            pltpu.VMEM((rows, feats), bf),
            pltpu.VMEM((2, rows, feats), bf),
            dma((6, 3)), dma((6, 3)), dma((6, 4)), dma((6, 4)), dma((6,)),
            dma((2, 7)), dma((2, 7)), dma((2, 7)), dma((2, 7)),
        ],
        compiler_params=pltpu.CompilerParams(
            collective_id=0, has_side_effects=True, vmem_limit_bytes=64 * 1024 * 1024 - 64 * 1024
        ),
    )(*operands)


def solution(mesh):
    def body(*args):
        if paired(mesh, *args):
            return on_device_paired(*args)
        return on_device(*args)

    placed = (
        P("fs", "tp"),
        P(),
        P("fs", "tp"),
        P("fs", "tp"),
        P(None, "tp"),
        P("tp", None, None),
        P("tp", None, None),
        P("tp"),
        P("tp", "fs"),
        P(),
        P("fs", "tp"),
        P("fs", "tp"),
        P("tp", "fs"),
    )
    return jax.shard_map(
        body, mesh=mesh, in_specs=placed, out_specs=P("fs", "tp"), check_vma=False
    )
```

```python
import functools

import jax
import jax.numpy as jnp
from jax import lax
from jax.experimental import pallas as pl
from jax.experimental.pallas import tpu as pltpu
from jax.sharding import PartitionSpec as P

LANES = 128

epsilon = 1e-06
gate_power = 8.0


def rms_norm(values, gain):
    wide = values.astype(jnp.float32)
    mean_square = jnp.mean(wide * wide, axis=-1, keepdims=True)
    return (wide * lax.rsqrt(mean_square + epsilon) * gain).astype(jnp.bfloat16)


def full_rows(shard):
    return lax.all_gather(shard, "tp", axis=1, tiled=True)


def pair_folder(left_rows, pieces):
    return (
        jnp.dot(left_rows, pieces[0], preferred_element_type=jnp.float32),
        jnp.dot(left_rows, pieces[1], preferred_element_type=jnp.float32),
    )


def project_out(acts, weight):
    partial_terms = jnp.dot(
        acts, lax.all_gather(weight, "fs", axis=1, tiled=True), preferred_element_type=jnp.float32
    )
    return lax.psum_scatter(
        partial_terms.astype(jnp.bfloat16), "tp", scatter_dimension=1, tiled=True
    ).astype(jnp.float32)


def combine(earlier, later):
    return (earlier[0] * later[0], later[0] * earlier[1] + later[1])


def on_device(
    tokens,
    mix_gain,
    in_x_w,
    in_gate_w,
    conv_taps,
    gate_x_blocks,
    gate_a_blocks,
    forget_rate,
    out_w,
    ffn_gain,
    ffn_gate_w,
    ffn_up_w,
    ffn_down_w,
):
    normed = rms_norm(full_rows(tokens), mix_gain)
    length = normed.shape[0]
    chan_width = in_x_w.shape[1]
    branch_in, branch_gate = pair_folder(
        normed,
        (
            lax.all_gather(in_x_w, "fs", axis=0, tiled=True),
            lax.all_gather(in_gate_w, "fs", axis=0, tiled=True),
        ),
    )
    tap_count = conv_taps.shape[0]
    padded = jnp.pad(branch_in, ((tap_count - 1, 0), (0, 0)))
    conv_sum = padded[0:length] * conv_taps[0]
    for index in range(1, tap_count):
        conv_sum = conv_sum + padded[index : index + length] * conv_taps[index]
    conv_out = conv_sum.astype(jnp.bfloat16)
    blocks = gate_x_blocks.shape[0]
    block_dim = gate_x_blocks.shape[1]
    grouped = conv_out.reshape(length, blocks, block_dim)
    gate_x = jax.nn.sigmoid(
        jnp.einsum(
            "tbi,bij->tbj", grouped, gate_x_blocks, preferred_element_type=jnp.float32
        ).reshape(length, chan_width)
    )
    gate_a = jax.nn.sigmoid(
        jnp.einsum(
            "tbi,bij->tbj", grouped, gate_a_blocks, preferred_element_type=jnp.float32
        ).reshape(length, chan_width)
    )
    log_decay = -gate_power * gate_a * forget_rate
    decay = jnp.exp(log_decay)
    scale = jnp.sqrt(-jnp.expm1(2.0 * log_decay))
    scale = jnp.where((jnp.arange(length) == 0)[:, None], 1.0, scale)
    driven = conv_out.astype(jnp.float32) * gate_x * scale
    _, state = lax.associative_scan(combine, (decay, driven), axis=0)
    mixer_out = (state * jax.nn.gelu(branch_gate)).astype(jnp.bfloat16)
    after_mix = (tokens.astype(jnp.float32) + project_out(mixer_out, out_w)).astype(jnp.bfloat16)
    normed_ffn = rms_norm(full_rows(after_mix), ffn_gain)
    gate_val, up_val = pair_folder(
        normed_ffn,
        (
            lax.all_gather(ffn_gate_w, "fs", axis=0, tiled=True),
            lax.all_gather(ffn_up_w, "fs", axis=0, tiled=True),
        ),
    )
    hidden = (jax.nn.silu(gate_val) * up_val).astype(jnp.bfloat16)
    return (after_mix.astype(jnp.float32) + project_out(hidden, ffn_down_w)).astype(jnp.bfloat16)


def paired(mesh, tokens, mix_gain, in_x_w, in_gate_w, conv_taps, gate_x_blocks, *rest):
    ffn_down_w = rest[-1]
    return (
        mesh.shape["fs"] == 8
        and mesh.shape["tp"] == 4
        and gate_x_blocks.shape == (2, LANES, LANES)
        and tokens.shape[0] % 32 == 0
        and tokens.shape[1] == 4 * LANES
        and ffn_down_w.shape[1] == 2 * LANES
        and ffn_down_w.shape[0] % 32 == 0
    )


PARTS = 2


def kernel(
    h_tok, h_gain1, h_x, h_g, h_taps, h_gxb, h_gab, h_forget, h_out, h_gain2, h_gate, h_up, h_dn,
    result,
    tok, gain1, w_x, w_g, taps, gxb, gab, forget, w_out, gain2, w_gate, w_up, w_dn, load_sem,
    x1, nb, win, wout, wgate, wup, wdn, s1, s1r, k1, x1r, zs1, z1r, after, mix, x2, hid,
    s2, s2r, k2, x2r, zs2, z2r,
    send_z, recv_z, send_y, recv_y, own_sem, ag_send, ag_recv, rs_send, rs_recv, fin_send, fin_recv,
):
    f, t = lax.axis_index("fs"), lax.axis_index("tp")
    z, y = f // 2, f % 2
    h = z % 2
    outer = (z == 0) | (z == 3)
    inner = (z == 1) | (z == 2)
    rows, feats = tok.shape
    near_z = z + 1 - 2 * h
    far_outer = 3 * (1 - z // 2)
    far_inner = 2 - z // 2
    sources = (z, near_z, far_outer, far_inner)
    fz = tuple(zz * 2 + y for zz in sources)
    fy = z * 2 + 1 - y
    t_core = t + 1 - 2 * (t % 2)
    t_x = (t + 2) % 4
    t_xc = (t_core + 2) % 4
    model = x1.shape[1]
    scope = jax.named_scope

    held = (tok, w_x, w_g, w_out, w_gate, w_up, w_dn, gain1, taps, gxb, gab, forget, gain2)
    given = (h_tok, h_x, h_g, h_out, h_gate, h_up, h_dn, h_gain1, h_taps, h_gxb, h_gab, h_forget, h_gain2)
    loads = [pltpu.make_async_copy(src, dst, load_sem.at[i]) for i, (src, dst) in enumerate(zip(given, held))]
    for load in loads:
        load.start()

    barrier = pltpu.get_barrier_semaphore()
    peers = [(fz[1], t), (fz[2], t), (fz[3], t), (fy, t), (f, t_core), (f, t_x)]
    for peer in peers:
        pl.semaphore_signal(barrier, inc=1, device_id=peer, device_id_type=pl.DeviceIdType.MESH)
    with scope("barrier"):
        pl.semaphore_wait(barrier, len(peers))

    started = []

    def describe(src, dst, s_sem, r_sem, peer):
        return pltpu.make_async_remote_copy(
            src_ref=src, dst_ref=dst, send_sem=s_sem, recv_sem=r_sem,
            device_id=peer, device_id_type=pl.DeviceIdType.MESH,
        )

    def send(src, dst, s_sem, r_sem, peer):
        copy = describe(src, dst, s_sem, r_sem, peer)
        copy.start()
        started.append(copy)
        return copy

    def span(index, width):
        return pl.ds(pl.multiple_of(index * width, width), width)

    depth = w_x.shape[0]
    cols = w_out.shape[1]
    part_cols = cols // PARTS
    half_ff = w_dn.shape[0] // 2
    fill = wgate.shape[0] - half_ff
    last_group = 4 + PARTS

    def piece(group, half, stored=False):
        if group < 2:
            return ((h_x, h_g) if stored else (w_x, w_g))[group].at[:, span(half, LANES)]
        if group == 2:
            return (h_out if stored else w_out).at[span(half, LANES), :]
        if group < 5:
            return ((h_gate, h_up) if stored else (w_gate, w_up))[group - 3].at[span(half, half_ff), :]
        return (h_dn if stored else w_dn).at[span(half, half_ff), pl.ds((group - 5) * part_cols, part_cols)]

    def place(group, source):
        if group < 2:
            return win.at[span(source, depth), pl.ds(group * LANES, LANES)]
        if group == 2:
            return wout.at[:, span(source, cols)]
        if group < 5:
            return (wgate, wup)[group - 3].at[pl.ds(0, half_ff), span(source, cols)]
        return wdn.at[group - 5, pl.ds(0, half_ff), span(source, part_cols)]

    groups = range(last_group + 1)
    own_copies = {}
    for group in groups:
        own_copies[group] = pltpu.make_async_copy(piece(group, h, True), place(group, f), own_sem.at[group])
        own_copies[group].start()

    slot = jnp.where(outer, 2, 3)
    z_sends = {}
    for group in groups:
        for way, peer in ((1, fz[1]), (2, fz[2]), (3, fz[3])):
            half = (1 - h, far_outer % 2, far_inner % 2)[way - 1]
            at = 1 if way == 1 else slot
            z_sends[group, way] = describe(
                piece(group, half), place(group, f), send_z.at[group, way - 1], recv_z.at[group, at - 1], (peer, t)
            )
            if way != 2:
                started.append(z_sends[group, way])
    y_copies, relays = {}, {}

    after_relay = {0: (2,), 2: (3,), 3: (4,), 4: (5, 6)}

    def near(*names):
        for group in names:
            z_sends[group, 1].start()

    def far(*names):
        @pl.when(outer)
        def _():
            for group in names:
                z_sends[group, 3].start()

    def y_own(*names):
        for group in names:
            y_copies[group, 0] = send(
                piece(group, h), place(group, f), send_y.at[group, 0], recv_y.at[group, 0], (fy, t)
            )

    def pick(when_inner, when_outer):
        return jnp.where(inner, when_inner, when_outer)

    arrival = (pick(1, 3), pick(2, 1), pick(3, 2))
    arrival_fz = (pick(fz[1], fz[3]), pick(fz[2], fz[1]), pick(fz[3], fz[2]))

    def forward(group, d):
        block = place(group, arrival_fz[d - 1])
        describe(
            block, block, send_z.at[group, 0], recv_z.at[group, arrival[d - 1] - 1], (fz[1], t)
        ).wait_recv()
        y_copies[group, d] = send(block, block, send_y.at[group, d], recv_y.at[group, d], (fy, t))
        if d == 1:
            relays[group] = describe(block, block, send_z.at[group, 3], recv_z.at[group, 1], (fz[2], t))

            @pl.when(inner)
            def _():
                relays[group].start()
                for next_group in after_relay.get(group, ()):
                    z_sends[next_group, 2].start()
                    z_sends[next_group, 3].start()

    def arrive(group):
        own_copies[group].wait()
        for d in range(4):
            y_copies[group, d].wait_recv()

    mine, theirs = span(h, rows), span(1 - h, rows)
    cut = rows // 2

    def some(block, c):
        return pl.ds(pl.multiple_of(block * rows + c * cut, cut), cut)

    def gather_start(k, own, x):
        x_peer, core_peer = (f, t_x), (f, t_core)

        def go(i, src, dst, peer):
            return send(src, dst, ag_send.at[k, i], ag_recv.at[k, i], peer)

        at = span(t, feats)
        by_z = [go(c, own.at[pl.ds(c * cut, cut), :], x.at[some(h, c), at], (fz[1], t)) for c in range(2)]
        by_x = go(2, own, x.at[mine, at], x_peer)
        by_core = go(3, own, x.at[mine, at], core_peer)
        x[mine, at] = own[...]
        return go, by_z, by_x, by_core, x_peer, core_peer, x

    def gather_relay(state):
        go, by_z, by_x, by_core, x_peer, core_peer, x = state
        across, inside = [], [by_core]
        at = span(t, feats)
        with scope("byz"):
            for c in range(2):
                by_z[c].wait_recv()
                block = x.at[some(1 - h, c), at]
                across.append(go(4 + c, block, block, x_peer))
                inside.append(go(6 + c, block, block, core_peer))
        with scope("byx"):
            by_x.wait_recv()
        block = x.at[mine, span(t_x, feats)]
        inside.append(go(8, block, block, core_peer))
        return across, inside

    def gather_pass(state, relayed):
        go, core_peer, x = state[0], state[5], state[6]
        across, inside = relayed
        with scope("across"):
            for c in range(2):
                across[c].wait_recv()
                block = x.at[some(1 - h, c), span(t_x, feats)]
                inside.append(go(9 + c, block, block, core_peer))

    def gather_end(relayed):
        with scope("inside"):
            for copy in relayed[1]:
                copy.wait_recv()

    def norm(x, gain, out):
        step = 32

        def one(i, carry):
            at = pl.ds(pl.multiple_of(i * step, step), step)
            wide = x[at, :].astype(jnp.float32)
            scale = lax.rsqrt(jnp.mean(wide * wide, axis=-1, keepdims=True) + epsilon)
            out[at, :] = (wide * scale * gain[...]).astype(jnp.bfloat16)
            return carry

        lax.fori_loop(0, x.shape[0] // step, one, 0)

    def scatter(k, acts, weight, s, r1, keep, r2, s3, r3, base, out, hooks):
        core_peer, x_peer = (f, t_core), (f, t_x)

        def project(block):
            at = span(block, feats)
            s[:, at] = jnp.dot(acts[...], weight[:, at], preferred_element_type=jnp.float32).astype(jnp.bfloat16)
            return s.at[:, at]

        a = send(project(t_xc), r1.at[0], rs_send.at[k, 0], rs_recv.at[k, 0], core_peer)
        b = send(project(t_core), r1.at[1], rs_send.at[k, 1], rs_recv.at[k, 1], core_peer)
        project(t_x)
        project(t)
        with scope("rs_a"):
            a.wait_recv()
        at = span(t_x, feats)
        for i, block in ((0, theirs), (1, mine)):
            keep[0, block, :] = (s[block, at].astype(jnp.float32) + r1[0, block, :].astype(jnp.float32)).astype(jnp.bfloat16)
            copy = send(keep.at[0, block], r2.at[block], rs_send.at[k, 2 + i], rs_recv.at[k, 2 + i], x_peer)
            if i == 0:
                c0 = copy
        c1 = copy
        hooks[0]()
        with scope("rs_c0"):
            b.wait_recv()
            c0.wait_recv()

        def total(where):
            return (
                s[where, span(t, feats)].astype(jnp.float32)
                + r1[1, where, :].astype(jnp.float32)
                + r2[where, :].astype(jnp.float32)
            )

        s3[...] = total(theirs).astype(jnp.bfloat16)
        e = send(s3, r3, rs_send.at[k, 4], rs_recv.at[k, 4], (fz[1], t))
        hooks[1]()
        with scope("rs_c1"):
            c1.wait_recv()
        part = total(mine)
        hooks[2]()
        with scope("rs_e"):
            e.wait_recv()
        out[...] = (base[...].astype(jnp.float32) + (part + r3[...].astype(jnp.float32))).astype(jnp.bfloat16)

    def finish(p, acts):
        core_peer, x_peer, z_peer = (f, t_core), (f, t_x), (fz[1], t)
        wide = feats // PARTS
        low, high = pl.ds(0, wide // 2), pl.ds(wide // 2, wide // 2)
        s, r1, keep, r2, s3, r3 = s2.at[p], s2r.at[p], k2.at[p], x2r.at[p], zs2.at[p], z2r.at[p]

        def project(block):
            at = span(block, wide)
            s[:, at] = jnp.dot(acts[...], wdn[p, :, at], preferred_element_type=jnp.float32).astype(jnp.bfloat16)
            return s.at[:, at]

        def go(i, src, dst, peer):
            return send(src, dst, fin_send.at[p, i], fin_recv.at[p, i], peer)

        def pair_sum(block, i):
            return s[:, span(block, wide)].astype(jnp.float32) + r1[i].astype(jnp.float32)

        a = go(0, project(t_xc), r1.at[0], core_peer)
        b = go(1, project(t_core), r1.at[1], core_peer)
        project(t_x)
        project(t)
        waits = {}

        def cross():
            with scope(f"fin_a{p}"):
                a.wait_recv()
            keep[0] = pair_sum(t_x, 0).astype(jnp.bfloat16)
            waits["d"] = go(3, keep.at[0, theirs, high], r3.at[0, :, high], z_peer)
            waits["c"] = go(2, keep.at[0, theirs, low], r2.at[theirs, low], x_peer)
            waits["m"] = go(7, keep.at[0, mine, low], r2.at[mine, low], x_peer)
            with scope(f"fin_b{p}"):
                b.wait_recv()
            keep[1] = pair_sum(t, 1).astype(jnp.bfloat16)
            waits["e"] = go(4, keep.at[1, theirs, high], r3.at[1, :, high], z_peer)

        def turn():
            with scope(f"fin_d{p}"):
                waits["d"].wait_recv()
            s3[:, high] = (
                keep[0, mine, high].astype(jnp.float32) + r3[0, :, high].astype(jnp.float32)
            ).astype(jnp.bfloat16)
            waits["g"] = go(5, s3.at[:, high], r2.at[pl.ds(0, rows), high], x_peer)
            with scope(f"fin_c{p}"):
                waits["c"].wait_recv()
            s3[:, low] = (
                keep[1, theirs, low].astype(jnp.float32) + r2[theirs, low].astype(jnp.float32)
            ).astype(jnp.bfloat16)
            waits["l"] = go(6, s3.at[:, low], r3.at[0, :, low], z_peer)

        def end():
            with scope(f"fin_g{p}"):
                waits["e"].wait_recv()
                waits["g"].wait_recv()
            left, right = pl.ds(p * part_cols, part_cols), pl.ds(cols + p * part_cols, part_cols)
            result[:, right] = (
                after[:, right].astype(jnp.float32)
                + (keep[1, mine, high].astype(jnp.float32) + r3[1, :, high].astype(jnp.float32))
                + r2[pl.ds(0, rows), high].astype(jnp.float32)
            ).astype(jnp.bfloat16)
            with scope(f"fin_l{p}"):
                waits["m"].wait_recv()
                waits["l"].wait_recv()
            result[:, left] = (
                after[:, left].astype(jnp.float32)
                + (keep[1, mine, low].astype(jnp.float32) + r2[mine, low].astype(jnp.float32))
                + r3[0, :, low].astype(jnp.float32)
            ).astype(jnp.bfloat16)

        return cross, turn, end

    def forwards(*pairs):
        def go():
            for group, d in pairs:
                with scope(f"fw{group}{d}"):
                    forward(group, d)

        return go

    nothing = forwards()
    for load in loads[:1]:
        load.wait()
    state = gather_start(0, tok, x1)
    for load in loads[1:]:
        load.wait()
    y_own(0, 1)

    for group in range(4):
        near(group)
        far(group)

    @pl.when(inner)
    def _():
        for group in range(2):
            z_sends[group, 2].start()
            z_sends[group, 3].start()

    y_own(2, 3)
    if fill:
        for w in (wgate, wup):
            w[pl.ds(half_ff, fill), :] = jnp.zeros((fill, model), jnp.bfloat16)
        for p in range(PARTS):
            wdn[p, pl.ds(half_ff, fill), :] = jnp.zeros((fill, wdn.shape[2]), jnp.bfloat16)
    relayed = gather_relay(state)
    forwards((0, 1), (0, 2), (0, 3), (1, 1), (1, 2), (1, 3))()
    gather_pass(state, relayed)
    forwards((2, 1))()
    gather_end(relayed)
    forwards((2, 2))()
    with scope("norm1"):
        norm(x1, gain1, nb)
    forwards((2, 3))()
    y_own(4)
    near(4)
    far(4)

    with scope("arrive01"):
        arrive(0)
        arrive(1)
    both = jnp.dot(nb[...], win[...], preferred_element_type=jnp.float32)
    branch_in, branch_gate = both[:, :LANES], both[:, LANES:]
    row = lax.broadcasted_iota(jnp.int32, branch_in.shape, 0)
    pos = jnp.where(row >= rows, row - rows, row)

    def shifted(values, by, fill):
        return jnp.where(pos >= by, pltpu.roll(values, by, 0), fill)

    tap_count = taps.shape[0]
    my = span(h, LANES)
    conv = branch_in * taps[tap_count - 1 :, my]
    for j in range(tap_count - 1):
        conv = conv + shifted(branch_in, tap_count - 1 - j, 0.0) * taps[j : j + 1, my]
    conv = conv.astype(jnp.bfloat16)
    gate_x = jax.nn.sigmoid(jnp.dot(conv, gxb[h], preferred_element_type=jnp.float32))
    gate_a = jax.nn.sigmoid(jnp.dot(conv, gab[h], preferred_element_type=jnp.float32))
    log_decay = -gate_power * gate_a * forget[:, my]
    decay = jnp.exp(log_decay)
    scale = jnp.sqrt(-jnp.tanh(log_decay) * (1.0 + decay * decay))
    scale = jnp.where(pos == 0, 1.0, scale)
    run = conv.astype(jnp.float32) * gate_x * scale
    by = 1
    while by < rows:
        run = decay * shifted(run, by, 0.0) + run
        decay = decay * shifted(decay, by, 1.0)
        by *= 2
    mix[...] = (run * jax.nn.gelu(branch_gate)).astype(jnp.bfloat16)
    y_own(*groups[5:])
    with scope("arrive2"):
        arrive(2)

    def refill():
        near(5)
        far(5)
        forwards((3, 2))()

    scatter(0, mix, wout, s1, s1r, k1, x1r, zs1, z1r, tok, after, (forwards((3, 1)), refill, forwards((3, 3))))
    state = gather_start(1, after, x2)
    near(6)
    far(6)

    forwards((4, 1), (4, 2))()
    relayed = gather_relay(state)
    forwards((4, 3))()
    gather_pass(state, relayed)
    forwards((5, 1), (5, 2))()
    gather_end(relayed)
    forwards((6, 1))()
    with scope("norm2"):
        norm(x2, gain2, nb)
    forwards((6, 2))()
    with scope("arrive34"):
        arrive(3)
        arrive(4)
    last = (((1,), (1,)), ((), ()))

    def ffn(i, carry):
        at = span(i, LANES)
        gate_val = lax.dot_general(nb[...], wgate[at, :], last, preferred_element_type=jnp.float32)
        up_val = lax.dot_general(nb[...], wup[at, :], last, preferred_element_type=jnp.float32)
        hid[:, at] = (jax.nn.silu(gate_val) * up_val).astype(jnp.bfloat16)
        return carry

    with scope("ffn"):
        lax.fori_loop(0, wgate.shape[0] // LANES, ffn, 0)
    forwards((5, 3), (6, 3))()
    with scope("arrive5"):
        arrive(5)
    first = finish(0, hid)
    first[0]()
    with scope("arrive6"):
        arrive(6)
    second = finish(1, hid)
    second[0]()
    first[1]()
    second[1]()
    first[2]()
    second[2]()
    with scope("drain"):
        for copy in started:
            copy.wait_send()

        @pl.when(inner)
        def _():
            for group in groups:
                z_sends[group, 2].wait_send()
                relays[group].wait_send()


def on_device_paired(
    tokens, mix_gain, in_x_w, in_gate_w, conv_taps, gate_x_blocks, gate_a_blocks, forget_rate,
    out_w, ffn_gain, ffn_gate_w, ffn_up_w, ffn_down_w,
):
    rows, feats = tokens.shape
    model = mix_gain.shape[0]
    both = 2 * rows
    share = feats // PARTS
    wide = -(-ffn_down_w.shape[0] // (2 * LANES)) * LANES
    bf, dma = jnp.bfloat16, pltpu.SemaphoreType.DMA
    exchange = [
        pltpu.VMEM((both, model), bf),
        pltpu.VMEM((2, both, feats), bf),
        pltpu.VMEM((2, both, feats), bf),
        pltpu.VMEM((both, feats), bf),
    ]
    vmem = pl.BlockSpec(memory_space=pltpu.VMEM)
    operands = (
        tokens, mix_gain.reshape(1, model), in_x_w, in_gate_w, conv_taps, gate_x_blocks, gate_a_blocks,
        forget_rate.reshape(1, -1), out_w, ffn_gain.reshape(1, model), ffn_gate_w.T, ffn_up_w.T, ffn_down_w,
    )
    return pl.pallas_call(
        kernel,
        out_shape=jax.ShapeDtypeStruct((rows, feats), bf),
        in_specs=[pl.BlockSpec(memory_space=pltpu.HBM)] * 13,
        out_specs=vmem,
        scratch_shapes=[
            *[pltpu.VMEM(operand.shape, operand.dtype) for operand in operands],
            dma((13,)),
            pltpu.VMEM((both, model), bf),
            pltpu.VMEM((both, model), bf),
            pltpu.VMEM((model, 2 * LANES), bf),
            pltpu.VMEM((LANES, model), bf),
            pltpu.VMEM((wide, model), bf),
            pltpu.VMEM((wide, model), bf),
            pltpu.VMEM((PARTS, wide, model // PARTS), bf),
            *exchange,
            pltpu.VMEM((rows, feats), bf),
            pltpu.VMEM((rows, feats), bf),
            pltpu.VMEM((rows, feats), bf),
            pltpu.VMEM((both, LANES), bf),
            pltpu.VMEM((both, model), bf),
            pltpu.VMEM((both, wide), bf),
            pltpu.VMEM((PARTS, both, model // PARTS), bf),
            pltpu.VMEM((PARTS, 2, both, share), bf),
            pltpu.VMEM((PARTS, 2, both, share), bf),
            pltpu.VMEM((PARTS, both, share), bf),
            pltpu.VMEM((PARTS, rows, share), bf),
            pltpu.VMEM((PARTS, 2, rows, share), bf),
            dma((7, 4)), dma((7, 3)), dma((7, 4)), dma((7, 4)), dma((7,)),
            dma((2, 11)), dma((2, 11)), dma((1, 5)), dma((1, 5)), dma((PARTS, 8)), dma((PARTS, 8)),
        ],
        compiler_params=pltpu.CompilerParams(
            collective_id=0, has_side_effects=True, vmem_limit_bytes=48 * 1024 * 1024
        ),
    )(*[pltpu.with_memory_space_constraint(operand, pltpu.HBM) for operand in operands])


def solution(mesh):
    def body(*args):
        if paired(mesh, *args):
            return on_device_paired(*args)
        return on_device(*args)

    placed = (
        P("fs", "tp"),
        P(),
        P("fs", "tp"),
        P("fs", "tp"),
        P(None, "tp"),
        P("tp", None, None),
        P("tp", None, None),
        P("tp"),
        P("tp", "fs"),
        P(),
        P("fs", "tp"),
        P("fs", "tp"),
        P("tp", "fs"),
    )
    return jax.shard_map(
        body, mesh=mesh, in_specs=placed, out_specs=P("fs", "tp"), check_vma=False
    )
```

```python
import functools

import jax
import jax.numpy as jnp
from jax import lax
from jax.experimental import pallas as pl
from jax.experimental.pallas import tpu as pltpu
from jax.sharding import PartitionSpec as P

LANES = 128

epsilon = 1e-06
gate_power = 8.0


def rms_norm(values, gain):
    wide = values.astype(jnp.float32)
    mean_square = jnp.mean(wide * wide, axis=-1, keepdims=True)
    return (wide * lax.rsqrt(mean_square + epsilon) * gain).astype(jnp.bfloat16)


def full_rows(shard):
    return lax.all_gather(shard, "tp", axis=1, tiled=True)


def pair_folder(left_rows, pieces):
    return (
        jnp.dot(left_rows, pieces[0], preferred_element_type=jnp.float32),
        jnp.dot(left_rows, pieces[1], preferred_element_type=jnp.float32),
    )


def project_out(acts, weight):
    partial_terms = jnp.dot(
        acts, lax.all_gather(weight, "fs", axis=1, tiled=True), preferred_element_type=jnp.float32
    )
    return lax.psum_scatter(
        partial_terms.astype(jnp.bfloat16), "tp", scatter_dimension=1, tiled=True
    ).astype(jnp.float32)


def combine(earlier, later):
    return (earlier[0] * later[0], later[0] * earlier[1] + later[1])


def on_device(
    tokens,
    mix_gain,
    in_x_w,
    in_gate_w,
    conv_taps,
    gate_x_blocks,
    gate_a_blocks,
    forget_rate,
    out_w,
    ffn_gain,
    ffn_gate_w,
    ffn_up_w,
    ffn_down_w,
):
    normed = rms_norm(full_rows(tokens), mix_gain)
    length = normed.shape[0]
    chan_width = in_x_w.shape[1]
    branch_in, branch_gate = pair_folder(
        normed,
        (
            lax.all_gather(in_x_w, "fs", axis=0, tiled=True),
            lax.all_gather(in_gate_w, "fs", axis=0, tiled=True),
        ),
    )
    tap_count = conv_taps.shape[0]
    padded = jnp.pad(branch_in, ((tap_count - 1, 0), (0, 0)))
    conv_sum = padded[0:length] * conv_taps[0]
    for index in range(1, tap_count):
        conv_sum = conv_sum + padded[index : index + length] * conv_taps[index]
    conv_out = conv_sum.astype(jnp.bfloat16)
    blocks = gate_x_blocks.shape[0]
    block_dim = gate_x_blocks.shape[1]
    grouped = conv_out.reshape(length, blocks, block_dim)
    gate_x = jax.nn.sigmoid(
        jnp.einsum(
            "tbi,bij->tbj", grouped, gate_x_blocks, preferred_element_type=jnp.float32
        ).reshape(length, chan_width)
    )
    gate_a = jax.nn.sigmoid(
        jnp.einsum(
            "tbi,bij->tbj", grouped, gate_a_blocks, preferred_element_type=jnp.float32
        ).reshape(length, chan_width)
    )
    log_decay = -gate_power * gate_a * forget_rate
    decay = jnp.exp(log_decay)
    scale = jnp.sqrt(-jnp.expm1(2.0 * log_decay))
    scale = jnp.where((jnp.arange(length) == 0)[:, None], 1.0, scale)
    driven = conv_out.astype(jnp.float32) * gate_x * scale
    _, state = lax.associative_scan(combine, (decay, driven), axis=0)
    mixer_out = (state * jax.nn.gelu(branch_gate)).astype(jnp.bfloat16)
    after_mix = (tokens.astype(jnp.float32) + project_out(mixer_out, out_w)).astype(jnp.bfloat16)
    normed_ffn = rms_norm(full_rows(after_mix), ffn_gain)
    gate_val, up_val = pair_folder(
        normed_ffn,
        (
            lax.all_gather(ffn_gate_w, "fs", axis=0, tiled=True),
            lax.all_gather(ffn_up_w, "fs", axis=0, tiled=True),
        ),
    )
    hidden = (jax.nn.silu(gate_val) * up_val).astype(jnp.bfloat16)
    return (after_mix.astype(jnp.float32) + project_out(hidden, ffn_down_w)).astype(jnp.bfloat16)


def paired(mesh, tokens, mix_gain, in_x_w, in_gate_w, conv_taps, gate_x_blocks, *rest):
    ffn_down_w = rest[-1]
    return (
        mesh.shape["fs"] == 8
        and mesh.shape["tp"] == 4
        and gate_x_blocks.shape == (2, LANES, LANES)
        and tokens.shape[0] % 32 == 0
        and tokens.shape[1] == 4 * LANES
        and ffn_down_w.shape[1] == 2 * LANES
        and ffn_down_w.shape[0] % 32 == 0
    )


PARTS = 2


def kernel(
    h_tok, h_gain1, h_x, h_g, h_taps, h_gxb, h_gab, h_forget, h_out, h_gain2, h_gate, h_up, h_dn,
    result,
    tok, gain1, w_x, w_g, taps, gxb, gab, forget, w_out, gain2, w_gate, w_up, w_dn, load_sem,
    x1, nb, win, wout, wgate, wup, wdn, s1, s1r, k1, x1r, zs1, z1r, after, mix, x2, hid,
    s2, s2r, k2, x2r, zs2, z2r,
    send_z, recv_z, send_y, recv_y, own_sem, ag_send, ag_recv, rs_send, rs_recv, fin_send, fin_recv,
):
    f, t = lax.axis_index("fs"), lax.axis_index("tp")
    z, y = f // 2, f % 2
    h = z % 2
    outer = (z == 0) | (z == 3)
    inner = (z == 1) | (z == 2)
    rows, feats = tok.shape
    near_z = z + 1 - 2 * h
    far_outer = 3 * (1 - z // 2)
    far_inner = 2 - z // 2
    sources = (z, near_z, far_outer, far_inner)
    fz = tuple(zz * 2 + y for zz in sources)
    fy = z * 2 + 1 - y
    t_core = t + 1 - 2 * (t % 2)
    t_x = (t + 2) % 4
    t_xc = (t_core + 2) % 4
    model = x1.shape[1]
    scope = jax.named_scope

    held = (tok, w_x, w_g, w_out, w_gate, w_up, w_dn, gain1, taps, gxb, gab, forget, gain2)
    given = (h_tok, h_x, h_g, h_out, h_gate, h_up, h_dn, h_gain1, h_taps, h_gxb, h_gab, h_forget, h_gain2)
    loads = [pltpu.make_async_copy(src, dst, load_sem.at[i]) for i, (src, dst) in enumerate(zip(given, held))]
    for load in loads:
        load.start()

    barrier = pltpu.get_barrier_semaphore()
    peers = [(fz[1], t), (fz[3], t), (fy, t), (f, t_core), (f, t_x)]

    def greet(peer):
        pl.semaphore_signal(barrier, inc=1, device_id=peer, device_id_type=pl.DeviceIdType.MESH)

    for peer in peers:
        greet(peer)

    @pl.when(inner)
    def _():
        greet((fz[2], t))

    with scope("barrier"):
        pl.semaphore_wait(barrier, len(peers) + jnp.where(inner, 1, 0))

    started = []

    def describe(src, dst, s_sem, r_sem, peer):
        return pltpu.make_async_remote_copy(
            src_ref=src, dst_ref=dst, send_sem=s_sem, recv_sem=r_sem,
            device_id=peer, device_id_type=pl.DeviceIdType.MESH,
        )

    def send(src, dst, s_sem, r_sem, peer):
        copy = describe(src, dst, s_sem, r_sem, peer)
        copy.start()
        started.append(copy)
        return copy

    def span(index, width):
        return pl.ds(pl.multiple_of(index * width, width), width)

    depth = w_x.shape[0]
    cols = w_out.shape[1]
    part_cols = cols // PARTS
    half_ff = w_dn.shape[0] // 2
    fill = wgate.shape[0] - half_ff
    last_group = 4 + PARTS

    def piece(group, half, stored=False):
        if group < 2:
            return ((h_x, h_g) if stored else (w_x, w_g))[group].at[:, span(half, LANES)]
        if group == 2:
            return (h_out if stored else w_out).at[span(half, LANES), :]
        if group < 5:
            return ((h_gate, h_up) if stored else (w_gate, w_up))[group - 3].at[span(half, half_ff), :]
        return (h_dn if stored else w_dn).at[span(half, half_ff), pl.ds((group - 5) * part_cols, part_cols)]

    def place(group, source):
        if group < 2:
            return win.at[span(source, depth), pl.ds(group * LANES, LANES)]
        if group == 2:
            return wout.at[:, span(source, cols)]
        if group < 5:
            return (wgate, wup)[group - 3].at[pl.ds(0, half_ff), span(source, cols)]
        return wdn.at[group - 5, pl.ds(0, half_ff), span(source, part_cols)]

    groups = range(last_group + 1)
    own_copies = {}
    for group in groups:
        own_copies[group] = pltpu.make_async_copy(piece(group, h, True), place(group, f), own_sem.at[group])
        own_copies[group].start()

    slot = jnp.where(outer, 2, 3)
    z_sends = {}
    for group in groups:
        for way, peer in ((1, fz[1]), (2, fz[2]), (3, fz[3])):
            half = (1 - h, far_outer % 2, far_inner % 2)[way - 1]
            at = 1 if way == 1 else slot
            z_sends[group, way] = describe(
                piece(group, half), place(group, f), send_z.at[group, way - 1], recv_z.at[group, at - 1], (peer, t)
            )
            if way != 2:
                started.append(z_sends[group, way])
    y_copies, relays = {}, {}

    after_relay = {
        0: ((2, 2), (2, 3)), 2: ((3, 2), (3, 3)), 3: ((4, 2), (4, 3)), 4: ((5, 2), (6, 2), (5, 3)), 6: ((6, 3),),
    }

    def near(*names):
        for group in names:
            z_sends[group, 1].start()

    def far(*names):
        @pl.when(outer)
        def _():
            for group in names:
                z_sends[group, 3].start()

    def y_own(*names):
        for group in names:
            y_copies[group, 0] = send(
                piece(group, h), place(group, f), send_y.at[group, 0], recv_y.at[group, 0], (fy, t)
            )

    def pick(when_inner, when_outer):
        return jnp.where(inner, when_inner, when_outer)

    early = (pick(1, 3), pick(2, 1), pick(3, 2)), (pick(fz[1], fz[3]), pick(fz[2], fz[1]), pick(fz[3], fz[2]))
    late = (1, pick(2, 3), pick(3, 2)), (fz[1], pick(fz[2], fz[3]), pick(fz[3], fz[2]))

    def forward(group, d):
        arrival, arrival_fz = early if group < 5 else late
        block = place(group, arrival_fz[d - 1])
        describe(
            block, block, send_z.at[group, 0], recv_z.at[group, arrival[d - 1] - 1], (fz[1], t)
        ).wait_recv()
        y_copies[group, d] = send(block, block, send_y.at[group, d], recv_y.at[group, d], (fy, t))
        if d == 1:
            relays[group] = describe(block, block, send_z.at[group, 3], recv_z.at[group, 1], (fz[2], t))

            @pl.when(inner)
            def _():
                relays[group].start()
                for key in after_relay.get(group, ()):
                    z_sends[key].start()

    def arrive(group):
        own_copies[group].wait()
        for d in range(4):
            y_copies[group, d].wait_recv()

    mine, theirs = span(h, rows), span(1 - h, rows)
    cut = rows // 2

    def some(block, c):
        return pl.ds(pl.multiple_of(block * rows + c * cut, cut), cut)

    def gather_start(k, own, x):
        x_peer, core_peer = (f, t_x), (f, t_core)

        def go(i, src, dst, peer):
            return send(src, dst, ag_send.at[k, i], ag_recv.at[k, i], peer)

        at = span(t, feats)
        by_z = [go(c, own.at[pl.ds(c * cut, cut), :], x.at[some(h, c), at], (fz[1], t)) for c in range(2)]
        by_x = go(2, own, x.at[mine, at], x_peer)
        by_core = go(3, own, x.at[mine, at], core_peer)
        x[mine, at] = own[...]
        return go, by_z, by_x, by_core, x_peer, core_peer, x

    def gather_relay(state):
        go, by_z, by_x, by_core, x_peer, core_peer, x = state
        across, inside = [], [by_core]
        at = span(t, feats)
        with scope("byz"):
            for c in range(2):
                by_z[c].wait_recv()
                block = x.at[some(1 - h, c), at]
                across.append(go(4 + c, block, block, x_peer))
                inside.append(go(6 + c, block, block, core_peer))
        with scope("byx"):
            by_x.wait_recv()
        block = x.at[mine, span(t_x, feats)]
        inside.append(go(8, block, block, core_peer))
        return across, inside

    def gather_pass(state, relayed):
        go, core_peer, x = state[0], state[5], state[6]
        across, inside = relayed
        with scope("across"):
            for c in range(2):
                across[c].wait_recv()
                block = x.at[some(1 - h, c), span(t_x, feats)]
                inside.append(go(9 + c, block, block, core_peer))

    def gather_end(relayed):
        with scope("inside"):
            for copy in relayed[1]:
                copy.wait_recv()

    def norm(x, gain, out):
        step = 32

        def one(i, carry):
            at = pl.ds(pl.multiple_of(i * step, step), step)
            wide = x[at, :].astype(jnp.float32)
            scale = lax.rsqrt(jnp.mean(wide * wide, axis=-1, keepdims=True) + epsilon)
            out[at, :] = (wide * scale * gain[...]).astype(jnp.bfloat16)
            return carry

        lax.fori_loop(0, x.shape[0] // step, one, 0)

    def scatter(k, acts, weight, s, r1, keep, r2, s3, r3, base, out, hooks):
        core_peer, x_peer = (f, t_core), (f, t_x)

        def project(block):
            at = span(block, feats)
            s[:, at] = jnp.dot(acts[...], weight[:, at], preferred_element_type=jnp.float32).astype(jnp.bfloat16)
            return s.at[:, at]

        a = send(project(t_xc), r1.at[0], rs_send.at[k, 0], rs_recv.at[k, 0], core_peer)
        b = send(project(t_core), r1.at[1], rs_send.at[k, 1], rs_recv.at[k, 1], core_peer)
        project(t_x)
        project(t)
        with scope("rs_a"):
            a.wait_recv()
        at = span(t_x, feats)
        for i, block in ((0, theirs), (1, mine)):
            keep[0, block, :] = (s[block, at].astype(jnp.float32) + r1[0, block, :].astype(jnp.float32)).astype(jnp.bfloat16)
            copy = send(keep.at[0, block], r2.at[block], rs_send.at[k, 2 + i], rs_recv.at[k, 2 + i], x_peer)
            if i == 0:
                c0 = copy
        c1 = copy
        hooks[0]()
        with scope("rs_c0"):
            b.wait_recv()
            c0.wait_recv()

        def total(where):
            return (
                s[where, span(t, feats)].astype(jnp.float32)
                + r1[1, where, :].astype(jnp.float32)
                + r2[where, :].astype(jnp.float32)
            )

        s3[...] = total(theirs).astype(jnp.bfloat16)
        e = send(s3, r3, rs_send.at[k, 4], rs_recv.at[k, 4], (fz[1], t))
        hooks[1]()
        with scope("rs_c1"):
            c1.wait_recv()
        part = total(mine)
        hooks[2]()
        with scope("rs_e"):
            e.wait_recv()
        out[...] = (base[...].astype(jnp.float32) + (part + r3[...].astype(jnp.float32))).astype(jnp.bfloat16)

    def finish(p, acts):
        core_peer, x_peer, z_peer = (f, t_core), (f, t_x), (fz[1], t)
        wide = feats // PARTS
        low, high = pl.ds(0, wide // 2), pl.ds(wide // 2, wide // 2)
        s, r1, keep, r2, s3, r3 = s2.at[p], s2r.at[p], k2.at[p], x2r.at[p], zs2.at[p], z2r.at[p]

        def project(block):
            at = span(block, wide)
            s[:, at] = jnp.dot(acts[...], wdn[p, :, at], preferred_element_type=jnp.float32).astype(jnp.bfloat16)
            return s.at[:, at]

        def go(i, src, dst, peer):
            return send(src, dst, fin_send.at[p, i], fin_recv.at[p, i], peer)

        def pair_sum(block, i):
            return s[:, span(block, wide)].astype(jnp.float32) + r1[i].astype(jnp.float32)

        a = go(0, project(t_xc), r1.at[0], core_peer)
        b = go(1, project(t_core), r1.at[1], core_peer)
        project(t_x)
        project(t)
        waits = {}

        def cross():
            with scope(f"fin_a{p}"):
                a.wait_recv()
            keep[0] = pair_sum(t_x, 0).astype(jnp.bfloat16)
            waits["d"] = go(3, keep.at[0, theirs, high], r3.at[0, :, high], z_peer)
            waits["c"] = go(2, keep.at[0, theirs, low], r2.at[theirs, low], x_peer)
            waits["m"] = go(7, keep.at[0, mine, low], r2.at[mine, low], x_peer)
            with scope(f"fin_b{p}"):
                b.wait_recv()
            keep[1] = pair_sum(t, 1).astype(jnp.bfloat16)
            waits["e"] = go(4, keep.at[1, theirs, high], r3.at[1, :, high], z_peer)

        def turn():
            with scope(f"fin_d{p}"):
                waits["d"].wait_recv()
            s3[:, high] = (
                keep[0, mine, high].astype(jnp.float32) + r3[0, :, high].astype(jnp.float32)
            ).astype(jnp.bfloat16)
            waits["g"] = go(5, s3.at[:, high], r2.at[pl.ds(0, rows), high], x_peer)
            with scope(f"fin_c{p}"):
                waits["c"].wait_recv()
            s3[:, low] = (
                keep[1, theirs, low].astype(jnp.float32) + r2[theirs, low].astype(jnp.float32)
            ).astype(jnp.bfloat16)
            waits["l"] = go(6, s3.at[:, low], r3.at[0, :, low], z_peer)

        def end():
            with scope(f"fin_g{p}"):
                waits["e"].wait_recv()
                waits["g"].wait_recv()
            left, right = pl.ds(p * part_cols, part_cols), pl.ds(cols + p * part_cols, part_cols)
            result[:, right] = (
                after[:, right].astype(jnp.float32)
                + (keep[1, mine, high].astype(jnp.float32) + r3[1, :, high].astype(jnp.float32))
                + r2[pl.ds(0, rows), high].astype(jnp.float32)
            ).astype(jnp.bfloat16)
            with scope(f"fin_l{p}"):
                waits["m"].wait_recv()
                waits["l"].wait_recv()
            result[:, left] = (
                after[:, left].astype(jnp.float32)
                + (keep[1, mine, low].astype(jnp.float32) + r2[mine, low].astype(jnp.float32))
                + r3[0, :, low].astype(jnp.float32)
            ).astype(jnp.bfloat16)

        return cross, turn, end

    def forwards(*pairs):
        def go():
            for group, d in pairs:
                with scope(f"fw{group}{d}"):
                    forward(group, d)

        return go

    nothing = forwards()
    for load in loads[:1]:
        load.wait()
    state = gather_start(0, tok, x1)
    for load in loads[1:]:
        load.wait()
    y_own(0, 1)

    for group in range(4):
        near(group)
        far(group)

    @pl.when(inner)
    def _():
        for group in range(2):
            z_sends[group, 2].start()
            z_sends[group, 3].start()

    y_own(2, 3)
    if fill:
        for w in (wgate, wup):
            w[pl.ds(half_ff, fill), :] = jnp.zeros((fill, model), jnp.bfloat16)
        for p in range(PARTS):
            wdn[p, pl.ds(half_ff, fill), :] = jnp.zeros((fill, wdn.shape[2]), jnp.bfloat16)
    relayed = gather_relay(state)
    forwards((0, 1), (0, 2), (0, 3), (1, 1), (1, 2), (1, 3))()
    gather_pass(state, relayed)
    forwards((2, 1))()
    gather_end(relayed)
    forwards((2, 2))()
    with scope("norm1"):
        norm(x1, gain1, nb)
    forwards((2, 3))()
    y_own(4)
    near(4)
    far(4)

    @pl.when(inner)
    def _():
        near(5, 6)


    with scope("arrive01"):
        arrive(0)
        arrive(1)
    both = jnp.dot(nb[...], win[...], preferred_element_type=jnp.float32)
    branch_in, branch_gate = both[:, :LANES], both[:, LANES:]
    row = lax.broadcasted_iota(jnp.int32, branch_in.shape, 0)
    pos = jnp.where(row >= rows, row - rows, row)

    def shifted(values, by, fill):
        return jnp.where(pos >= by, pltpu.roll(values, by, 0), fill)

    tap_count = taps.shape[0]
    my = span(h, LANES)
    conv = branch_in * taps[tap_count - 1 :, my]
    for j in range(tap_count - 1):
        conv = conv + shifted(branch_in, tap_count - 1 - j, 0.0) * taps[j : j + 1, my]
    conv = conv.astype(jnp.bfloat16)
    gate_x = jax.nn.sigmoid(jnp.dot(conv, gxb[h], preferred_element_type=jnp.float32))
    gate_a = jax.nn.sigmoid(jnp.dot(conv, gab[h], preferred_element_type=jnp.float32))
    log_decay = -gate_power * gate_a * forget[:, my]
    decay = jnp.exp(log_decay)
    scale = jnp.sqrt(-jnp.tanh(log_decay) * (1.0 + decay * decay))
    scale = jnp.where(pos == 0, 1.0, scale)
    run = conv.astype(jnp.float32) * gate_x * scale
    by = 1
    while by < rows:
        run = decay * shifted(run, by, 0.0) + run
        decay = decay * shifted(decay, by, 1.0)
        by *= 2
    mix[...] = (run * jax.nn.gelu(branch_gate)).astype(jnp.bfloat16)
    y_own(*groups[5:])
    with scope("arrive2"):
        arrive(2)

    def refill():
        @pl.when(outer)
        def _():
            near(5, 6)

        far(5)
        forwards((3, 2))()

    scatter(0, mix, wout, s1, s1r, k1, x1r, zs1, z1r, tok, after, (forwards((3, 1)), refill, forwards((3, 3))))
    state = gather_start(1, after, x2)
    far(6)

    forwards((4, 1), (4, 2), (5, 1))()
    relayed = gather_relay(state)
    forwards((4, 3), (6, 1))()
    gather_pass(state, relayed)
    forwards((5, 2))()
    gather_end(relayed)
    with scope("norm2"):
        norm(x2, gain2, nb)
    forwards((6, 2))()
    with scope("arrive34"):
        arrive(3)
        arrive(4)
    last = (((1,), (1,)), ((), ()))

    with scope("ffn"):
        gate_val = lax.dot_general(nb[...], wgate[...], last, preferred_element_type=jnp.float32)
        up_val = lax.dot_general(nb[...], wup[...], last, preferred_element_type=jnp.float32)
        hid[...] = (jax.nn.silu(gate_val) * up_val).astype(jnp.bfloat16)
    forwards((5, 3), (6, 3))()
    with scope("arrive5"):
        arrive(5)
    first = finish(0, hid)
    first[0]()
    with scope("arrive6"):
        arrive(6)
    second = finish(1, hid)
    second[0]()
    first[1]()
    second[1]()
    first[2]()
    second[2]()
    with scope("drain"):
        for copy in started:
            copy.wait_send()

        @pl.when(inner)
        def _():
            for group in groups:
                z_sends[group, 2].wait_send()
                relays[group].wait_send()


def on_device_paired(
    tokens, mix_gain, in_x_w, in_gate_w, conv_taps, gate_x_blocks, gate_a_blocks, forget_rate,
    out_w, ffn_gain, ffn_gate_w, ffn_up_w, ffn_down_w,
):
    rows, feats = tokens.shape
    model = mix_gain.shape[0]
    both = 2 * rows
    share = feats // PARTS
    wide = -(-ffn_down_w.shape[0] // (2 * LANES)) * LANES
    bf, dma = jnp.bfloat16, pltpu.SemaphoreType.DMA
    exchange = [
        pltpu.VMEM((both, model), bf),
        pltpu.VMEM((2, both, feats), bf),
        pltpu.VMEM((2, both, feats), bf),
        pltpu.VMEM((both, feats), bf),
    ]
    vmem = pl.BlockSpec(memory_space=pltpu.VMEM)
    operands = (
        tokens, mix_gain.reshape(1, model), in_x_w, in_gate_w, conv_taps, gate_x_blocks, gate_a_blocks,
        forget_rate.reshape(1, -1), out_w, ffn_gain.reshape(1, model), ffn_gate_w.T, ffn_up_w.T, ffn_down_w,
    )
    return pl.pallas_call(
        kernel,
        out_shape=jax.ShapeDtypeStruct((rows, feats), bf),
        in_specs=[pl.BlockSpec(memory_space=pltpu.HBM)] * 13,
        out_specs=vmem,
        scratch_shapes=[
            *[pltpu.VMEM(operand.shape, operand.dtype) for operand in operands],
            dma((13,)),
            pltpu.VMEM((both, model), bf),
            pltpu.VMEM((both, model), bf),
            pltpu.VMEM((model, 2 * LANES), bf),
            pltpu.VMEM((LANES, model), bf),
            pltpu.VMEM((wide, model), bf),
            pltpu.VMEM((wide, model), bf),
            pltpu.VMEM((PARTS, wide, model // PARTS), bf),
            *exchange,
            pltpu.VMEM((rows, feats), bf),
            pltpu.VMEM((rows, feats), bf),
            pltpu.VMEM((rows, feats), bf),
            pltpu.VMEM((both, LANES), bf),
            pltpu.VMEM((both, model), bf),
            pltpu.VMEM((both, wide), bf),
            pltpu.VMEM((PARTS, both, model // PARTS), bf),
            pltpu.VMEM((PARTS, 2, both, share), bf),
            pltpu.VMEM((PARTS, 2, both, share), bf),
            pltpu.VMEM((PARTS, both, share), bf),
            pltpu.VMEM((PARTS, rows, share), bf),
            pltpu.VMEM((PARTS, 2, rows, share), bf),
            dma((7, 4)), dma((7, 3)), dma((7, 4)), dma((7, 4)), dma((7,)),
            dma((2, 11)), dma((2, 11)), dma((1, 5)), dma((1, 5)), dma((PARTS, 8)), dma((PARTS, 8)),
        ],
        compiler_params=pltpu.CompilerParams(
            collective_id=0, has_side_effects=True, vmem_limit_bytes=48 * 1024 * 1024
        ),
    )(*[pltpu.with_memory_space_constraint(operand, pltpu.HBM) for operand in operands])


def solution(mesh):
    def body(*args):
        if paired(mesh, *args):
            return on_device_paired(*args)
        return on_device(*args)

    placed = (
        P("fs", "tp"),
        P(),
        P("fs", "tp"),
        P("fs", "tp"),
        P(None, "tp"),
        P("tp", None, None),
        P("tp", None, None),
        P("tp"),
        P("tp", "fs"),
        P(),
        P("fs", "tp"),
        P("fs", "tp"),
        P("tp", "fs"),
    )
    return jax.shard_map(
        body, mesh=mesh, in_specs=placed, out_specs=P("fs", "tp"), check_vma=False
    )
```

```python
import functools

import jax
import jax.numpy as jnp
from jax import lax
from jax.experimental import pallas as pl
from jax.experimental.pallas import tpu as pltpu
from jax.sharding import PartitionSpec as P

LANES = 128

epsilon = 1e-06
gate_power = 8.0


def rms_norm(values, gain):
    wide = values.astype(jnp.float32)
    mean_square = jnp.mean(wide * wide, axis=-1, keepdims=True)
    return (wide * lax.rsqrt(mean_square + epsilon) * gain).astype(jnp.bfloat16)


def full_rows(shard):
    return lax.all_gather(shard, "tp", axis=1, tiled=True)


def pair_folder(left_rows, pieces):
    return (
        jnp.dot(left_rows, pieces[0], preferred_element_type=jnp.float32),
        jnp.dot(left_rows, pieces[1], preferred_element_type=jnp.float32),
    )


def project_out(acts, weight):
    partial_terms = jnp.dot(
        acts, lax.all_gather(weight, "fs", axis=1, tiled=True), preferred_element_type=jnp.float32
    )
    return lax.psum_scatter(
        partial_terms.astype(jnp.bfloat16), "tp", scatter_dimension=1, tiled=True
    ).astype(jnp.float32)


def combine(earlier, later):
    return (earlier[0] * later[0], later[0] * earlier[1] + later[1])


def on_device(
    tokens,
    mix_gain,
    in_x_w,
    in_gate_w,
    conv_taps,
    gate_x_blocks,
    gate_a_blocks,
    forget_rate,
    out_w,
    ffn_gain,
    ffn_gate_w,
    ffn_up_w,
    ffn_down_w,
):
    normed = rms_norm(full_rows(tokens), mix_gain)
    length = normed.shape[0]
    chan_width = in_x_w.shape[1]
    branch_in, branch_gate = pair_folder(
        normed,
        (
            lax.all_gather(in_x_w, "fs", axis=0, tiled=True),
            lax.all_gather(in_gate_w, "fs", axis=0, tiled=True),
        ),
    )
    tap_count = conv_taps.shape[0]
    padded = jnp.pad(branch_in, ((tap_count - 1, 0), (0, 0)))
    conv_sum = padded[0:length] * conv_taps[0]
    for index in range(1, tap_count):
        conv_sum = conv_sum + padded[index : index + length] * conv_taps[index]
    conv_out = conv_sum.astype(jnp.bfloat16)
    blocks = gate_x_blocks.shape[0]
    block_dim = gate_x_blocks.shape[1]
    grouped = conv_out.reshape(length, blocks, block_dim)
    gate_x = jax.nn.sigmoid(
        jnp.einsum(
            "tbi,bij->tbj", grouped, gate_x_blocks, preferred_element_type=jnp.float32
        ).reshape(length, chan_width)
    )
    gate_a = jax.nn.sigmoid(
        jnp.einsum(
            "tbi,bij->tbj", grouped, gate_a_blocks, preferred_element_type=jnp.float32
        ).reshape(length, chan_width)
    )
    log_decay = -gate_power * gate_a * forget_rate
    decay = jnp.exp(log_decay)
    scale = jnp.sqrt(-jnp.expm1(2.0 * log_decay))
    scale = jnp.where((jnp.arange(length) == 0)[:, None], 1.0, scale)
    driven = conv_out.astype(jnp.float32) * gate_x * scale
    _, state = lax.associative_scan(combine, (decay, driven), axis=0)
    mixer_out = (state * jax.nn.gelu(branch_gate)).astype(jnp.bfloat16)
    after_mix = (tokens.astype(jnp.float32) + project_out(mixer_out, out_w)).astype(jnp.bfloat16)
    normed_ffn = rms_norm(full_rows(after_mix), ffn_gain)
    gate_val, up_val = pair_folder(
        normed_ffn,
        (
            lax.all_gather(ffn_gate_w, "fs", axis=0, tiled=True),
            lax.all_gather(ffn_up_w, "fs", axis=0, tiled=True),
        ),
    )
    hidden = (jax.nn.silu(gate_val) * up_val).astype(jnp.bfloat16)
    return (after_mix.astype(jnp.float32) + project_out(hidden, ffn_down_w)).astype(jnp.bfloat16)


def paired(mesh, tokens, mix_gain, in_x_w, in_gate_w, conv_taps, gate_x_blocks, *rest):
    ffn_down_w = rest[-1]
    return (
        mesh.shape["fs"] == 8
        and mesh.shape["tp"] == 4
        and gate_x_blocks.shape == (2, LANES, LANES)
        and tokens.shape[0] % 32 == 0
        and tokens.shape[1] == 4 * LANES
        and ffn_down_w.shape[1] == 2 * LANES
        and ffn_down_w.shape[0] % 32 == 0
    )


PARTS = 2


def kernel(
    h_tok, h_gain1, h_x, h_g, h_taps, h_gxb, h_gab, h_forget, h_out, h_gain2, h_gate, h_up, h_dn,
    result,
    tok, gain1, w_x, w_g, taps, gxb, gab, forget, w_out, gain2, w_gate, w_up, w_dn, load_sem,
    x1, nb, win, wout, wgate, wup, wdn, s1, s1r, k1, x1r, zs1, z1r, after, mix, x2, hid,
    s2, s2r, k2, x2r, zs2, z2r,
    send_z, recv_z, send_y, recv_y, own_sem, ag_send, ag_recv, rs_send, rs_recv, fin_send, fin_recv,
):
    f, t = lax.axis_index("fs"), lax.axis_index("tp")
    z, y = f // 2, f % 2
    h = z % 2
    outer = (z == 0) | (z == 3)
    inner = (z == 1) | (z == 2)
    rows, feats = tok.shape
    near_z = z + 1 - 2 * h
    far_outer = 3 * (1 - z // 2)
    far_inner = 2 - z // 2
    sources = (z, near_z, far_outer, far_inner)
    fz = tuple(zz * 2 + y for zz in sources)
    fy = z * 2 + 1 - y
    t_core = t + 1 - 2 * (t % 2)
    t_x = (t + 2) % 4
    t_xc = (t_core + 2) % 4
    model = x1.shape[1]
    scope = jax.named_scope

    held = (tok, w_x, w_g, w_out, w_gate, w_up, w_dn, gain1, taps, gxb, gab, forget, gain2)
    given = (h_tok, h_x, h_g, h_out, h_gate, h_up, h_dn, h_gain1, h_taps, h_gxb, h_gab, h_forget, h_gain2)
    loads = [pltpu.make_async_copy(src, dst, load_sem.at[i]) for i, (src, dst) in enumerate(zip(given, held))]
    for load in loads:
        load.start()

    barrier = pltpu.get_barrier_semaphore()
    peers = [(fz[1], t), (fz[3], t), (fy, t), (f, t_core), (f, t_x)]

    def greet(peer):
        pl.semaphore_signal(barrier, inc=1, device_id=peer, device_id_type=pl.DeviceIdType.MESH)

    for peer in peers:
        greet(peer)

    @pl.when(inner)
    def _():
        greet((fz[2], t))

    with scope("barrier"):
        pl.semaphore_wait(barrier, len(peers) + jnp.where(inner, 1, 0))

    started = []

    def describe(src, dst, s_sem, r_sem, peer):
        return pltpu.make_async_remote_copy(
            src_ref=src, dst_ref=dst, send_sem=s_sem, recv_sem=r_sem,
            device_id=peer, device_id_type=pl.DeviceIdType.MESH,
        )

    def send(src, dst, s_sem, r_sem, peer):
        copy = describe(src, dst, s_sem, r_sem, peer)
        copy.start()
        started.append(copy)
        return copy

    def span(index, width):
        return pl.ds(pl.multiple_of(index * width, width), width)

    depth = w_x.shape[0]
    cols = w_out.shape[1]
    part_cols = cols // PARTS
    half_ff = w_dn.shape[0] // 2
    fill = wgate.shape[0] - half_ff
    last_group = 4 + PARTS

    def piece(group, half, stored=False):
        if group < 2:
            return ((h_x, h_g) if stored else (w_x, w_g))[group].at[:, span(half, LANES)]
        if group == 2:
            return (h_out if stored else w_out).at[span(half, LANES), :]
        if group < 5:
            return ((h_gate, h_up) if stored else (w_gate, w_up))[group - 3].at[span(half, half_ff), :]
        return (h_dn if stored else w_dn).at[span(half, half_ff), pl.ds((group - 5) * part_cols, part_cols)]

    def place(group, source):
        if group < 2:
            return win.at[span(source, depth), pl.ds(group * LANES, LANES)]
        if group == 2:
            return wout.at[:, span(source, cols)]
        if group < 5:
            return (wgate, wup)[group - 3].at[pl.ds(0, half_ff), span(source, cols)]
        return wdn.at[group - 5, pl.ds(0, half_ff), span(source, part_cols)]

    groups = range(last_group + 1)
    own_copies = {}
    for group in groups:
        own_copies[group] = pltpu.make_async_copy(piece(group, h, True), place(group, f), own_sem.at[group])
        own_copies[group].start()

    slot = jnp.where(outer, 2, 3)
    z_sends = {}
    for group in groups:
        for way, peer in ((1, fz[1]), (2, fz[2]), (3, fz[3])):
            half = (1 - h, far_outer % 2, far_inner % 2)[way - 1]
            at = 1 if way == 1 else slot
            z_sends[group, way] = describe(
                piece(group, half), place(group, f), send_z.at[group, way - 1], recv_z.at[group, at - 1], (peer, t)
            )
            if way != 2:
                started.append(z_sends[group, way])
    y_copies, relays = {}, {}

    after_relay = {
        0: ((2, 2), (2, 3)), 2: ((3, 2), (3, 3)), 3: ((4, 2), (4, 3)), 4: ((5, 2), (6, 2), (5, 3)), 6: ((6, 3),),
    }

    def near(*names):
        for group in names:
            z_sends[group, 1].start()

    def far(*names):
        @pl.when(outer)
        def _():
            for group in names:
                z_sends[group, 3].start()

    for group in groups:
        y_copies[group, 0] = describe(
            piece(group, h), place(group, f), send_y.at[group, 0], recv_y.at[group, 0], (fy, t)
        )
        started.append(y_copies[group, 0])

    def y_own(*names, role=None):
        def go():
            for group in names:
                y_copies[group, 0].start()

        go() if role is None else pl.when(role)(go)

    def pick(when_inner, when_outer):
        return jnp.where(inner, when_inner, when_outer)

    early = (pick(1, 3), pick(2, 1), pick(3, 2)), (pick(fz[1], fz[3]), pick(fz[2], fz[1]), pick(fz[3], fz[2]))
    middle = (1, 3, 2), (fz[1], fz[3], fz[2])
    late = (1, pick(2, 3), pick(3, 2)), (fz[1], pick(fz[2], fz[3]), pick(fz[3], fz[2]))

    def forward(group, d):
        arrival, arrival_fz = early if group < 3 else middle if group < 5 else late
        block = place(group, arrival_fz[d - 1])
        describe(
            block, block, send_z.at[group, 0], recv_z.at[group, arrival[d - 1] - 1], (fz[1], t)
        ).wait_recv()
        y_copies[group, d] = send(block, block, send_y.at[group, d], recv_y.at[group, d], (fy, t))
        if d == 1:
            relays[group] = describe(block, block, send_z.at[group, 3], recv_z.at[group, 1], (fz[2], t))

            @pl.when(inner)
            def _():
                relays[group].start()
                for key in after_relay.get(group, ()):
                    z_sends[key].start()

    def arrive(group):
        own_copies[group].wait()
        for d in range(4):
            y_copies[group, d].wait_recv()

    mine, theirs = span(h, rows), span(1 - h, rows)
    cut = rows // 2

    def some(block, c):
        return pl.ds(pl.multiple_of(block * rows + c * cut, cut), cut)

    def gather_start(k, own, x):
        x_peer, core_peer = (f, t_x), (f, t_core)

        def go(i, src, dst, peer):
            return send(src, dst, ag_send.at[k, i], ag_recv.at[k, i], peer)

        at = span(t, feats)
        by_z = [go(c, own.at[pl.ds(c * cut, cut), :], x.at[some(h, c), at], (fz[1], t)) for c in range(2)]
        by_x = go(2, own, x.at[mine, at], x_peer)
        by_core = go(3, own, x.at[mine, at], core_peer)
        x[mine, at] = own[...]
        return go, by_z, by_x, by_core, x_peer, core_peer, x

    def gather_relay(state):
        go, by_z, by_x, by_core, x_peer, core_peer, x = state
        across, inside = [], [by_core]
        at = span(t, feats)
        with scope("byz"):
            for c in range(2):
                by_z[c].wait_recv()
                block = x.at[some(1 - h, c), at]
                across.append(go(4 + c, block, block, x_peer))
                inside.append(go(6 + c, block, block, core_peer))
        with scope("byx"):
            by_x.wait_recv()
        block = x.at[mine, span(t_x, feats)]
        inside.append(go(8, block, block, core_peer))
        return across, inside

    def gather_pass(state, relayed):
        go, core_peer, x = state[0], state[5], state[6]
        across, inside = relayed
        with scope("across"):
            for c in range(2):
                across[c].wait_recv()
                block = x.at[some(1 - h, c), span(t_x, feats)]
                inside.append(go(9 + c, block, block, core_peer))

    def gather_end(relayed):
        with scope("inside"):
            for copy in relayed[1]:
                copy.wait_recv()

    def norm(x, gain, out):
        step = 32

        def one(i, carry):
            at = pl.ds(pl.multiple_of(i * step, step), step)
            wide = x[at, :].astype(jnp.float32)
            scale = lax.rsqrt(jnp.mean(wide * wide, axis=-1, keepdims=True) + epsilon)
            out[at, :] = (wide * scale * gain[...]).astype(jnp.bfloat16)
            return carry

        lax.fori_loop(0, x.shape[0] // step, one, 0)

    def scatter(k, acts, weight, s, r1, keep, r2, s3, r3, base, out, hooks):
        core_peer, x_peer = (f, t_core), (f, t_x)

        def project(block):
            at = span(block, feats)
            s[:, at] = jnp.dot(acts[...], weight[:, at], preferred_element_type=jnp.float32).astype(jnp.bfloat16)
            return s.at[:, at]

        a = send(project(t_xc), r1.at[0], rs_send.at[k, 0], rs_recv.at[k, 0], core_peer)
        b = send(project(t_core), r1.at[1], rs_send.at[k, 1], rs_recv.at[k, 1], core_peer)
        project(t_x)
        project(t)
        with scope("rs_a"):
            a.wait_recv()
        at = span(t_x, feats)
        for i, block in ((0, theirs), (1, mine)):
            keep[0, block, :] = (s[block, at].astype(jnp.float32) + r1[0, block, :].astype(jnp.float32)).astype(jnp.bfloat16)
            copy = send(keep.at[0, block], r2.at[block], rs_send.at[k, 2 + i], rs_recv.at[k, 2 + i], x_peer)
            if i == 0:
                c0 = copy
        c1 = copy
        hooks[0]()
        with scope("rs_c0"):
            b.wait_recv()
            c0.wait_recv()

        def total(where):
            return (
                s[where, span(t, feats)].astype(jnp.float32)
                + r1[1, where, :].astype(jnp.float32)
                + r2[where, :].astype(jnp.float32)
            )

        s3[...] = total(theirs).astype(jnp.bfloat16)
        e = send(s3, r3, rs_send.at[k, 4], rs_recv.at[k, 4], (fz[1], t))
        hooks[1]()
        with scope("rs_c1"):
            c1.wait_recv()
        part = total(mine)
        hooks[2]()
        with scope("rs_e"):
            e.wait_recv()
        out[...] = (base[...].astype(jnp.float32) + (part + r3[...].astype(jnp.float32))).astype(jnp.bfloat16)

    def finish(p, acts):
        core_peer, x_peer, z_peer = (f, t_core), (f, t_x), (fz[1], t)
        wide = feats // PARTS
        low, high = pl.ds(0, wide // 2), pl.ds(wide // 2, wide // 2)
        s, r1, keep, r2, s3, r3 = s2.at[p], s2r.at[p], k2.at[p], x2r.at[p], zs2.at[p], z2r.at[p]

        def project(block):
            at = span(block, wide)
            s[:, at] = jnp.dot(acts[...], wdn[p, :, at], preferred_element_type=jnp.float32).astype(jnp.bfloat16)
            return s.at[:, at]

        def go(i, src, dst, peer):
            return send(src, dst, fin_send.at[p, i], fin_recv.at[p, i], peer)

        def pair_sum(block, i):
            return s[:, span(block, wide)].astype(jnp.float32) + r1[i].astype(jnp.float32)

        a = go(0, project(t_xc), r1.at[0], core_peer)
        b = go(1, project(t_core), r1.at[1], core_peer)
        project(t_x)
        project(t)
        waits = {}

        def cross():
            with scope(f"fin_a{p}"):
                a.wait_recv()
            keep[0] = pair_sum(t_x, 0).astype(jnp.bfloat16)
            waits["d"] = go(3, keep.at[0, theirs, high], r3.at[0, :, high], z_peer)
            waits["c"] = go(2, keep.at[0, theirs, low], r2.at[theirs, low], x_peer)
            waits["m"] = go(7, keep.at[0, mine, low], r2.at[mine, low], x_peer)
            with scope(f"fin_b{p}"):
                b.wait_recv()
            keep[1] = pair_sum(t, 1).astype(jnp.bfloat16)
            waits["e"] = go(4, keep.at[1, theirs, high], r3.at[1, :, high], z_peer)

        def turn():
            with scope(f"fin_d{p}"):
                waits["d"].wait_recv()
            s3[:, high] = (
                keep[0, mine, high].astype(jnp.float32) + r3[0, :, high].astype(jnp.float32)
            ).astype(jnp.bfloat16)
            waits["g"] = go(5, s3.at[:, high], r2.at[pl.ds(0, rows), high], x_peer)
            with scope(f"fin_c{p}"):
                waits["c"].wait_recv()
            s3[:, low] = (
                keep[1, theirs, low].astype(jnp.float32) + r2[theirs, low].astype(jnp.float32)
            ).astype(jnp.bfloat16)
            waits["l"] = go(6, s3.at[:, low], r3.at[0, :, low], z_peer)

        def end():
            with scope(f"fin_g{p}"):
                waits["e"].wait_recv()
                waits["g"].wait_recv()
            left, right = pl.ds(p * part_cols, part_cols), pl.ds(cols + p * part_cols, part_cols)
            result[:, right] = (
                after[:, right].astype(jnp.float32)
                + (keep[1, mine, high].astype(jnp.float32) + r3[1, :, high].astype(jnp.float32))
                + r2[pl.ds(0, rows), high].astype(jnp.float32)
            ).astype(jnp.bfloat16)
            with scope(f"fin_l{p}"):
                waits["m"].wait_recv()
                waits["l"].wait_recv()
            result[:, left] = (
                after[:, left].astype(jnp.float32)
                + (keep[1, mine, low].astype(jnp.float32) + r2[mine, low].astype(jnp.float32))
                + r3[0, :, low].astype(jnp.float32)
            ).astype(jnp.bfloat16)

        return cross, turn, end

    def forwards(*pairs):
        def go():
            for group, d in pairs:
                with scope(f"fw{group}{d}"):
                    forward(group, d)

        return go

    nothing = forwards()
    for load in loads[:1]:
        load.wait()
    state = gather_start(0, tok, x1)
    for load in loads[1:]:
        load.wait()
    y_own(0, 1)

    for group in range(4):
        near(group)
        far(group)

    @pl.when(inner)
    def _():
        for group in range(2):
            z_sends[group, 2].start()
            z_sends[group, 3].start()

    y_own(2, 3)
    y_own(5, role=outer)
    if fill:
        for w in (wgate, wup):
            w[pl.ds(half_ff, fill), :] = jnp.zeros((fill, model), jnp.bfloat16)
        for p in range(PARTS):
            wdn[p, pl.ds(half_ff, fill), :] = jnp.zeros((fill, wdn.shape[2]), jnp.bfloat16)
    relayed = gather_relay(state)
    forwards((0, 1), (0, 2), (0, 3), (1, 1), (1, 2))()
    y_own(6, role=outer)
    forwards((1, 3))()
    gather_pass(state, relayed)
    forwards((2, 1))()
    gather_end(relayed)
    forwards((2, 2))()
    with scope("norm1"):
        norm(x1, gain1, nb)
    forwards((2, 3))()
    y_own(4)
    near(4)
    far(4)

    @pl.when(inner)
    def _():
        near(5, 6)


    with scope("arrive01"):
        arrive(0)
        arrive(1)
    both = jnp.dot(nb[...], win[...], preferred_element_type=jnp.float32)
    branch_in, branch_gate = both[:, :LANES], both[:, LANES:]
    row = lax.broadcasted_iota(jnp.int32, branch_in.shape, 0)
    pos = jnp.where(row >= rows, row - rows, row)

    def shifted(values, by, fill):
        return jnp.where(pos >= by, pltpu.roll(values, by, 0), fill)

    tap_count = taps.shape[0]
    my = span(h, LANES)
    conv = branch_in * taps[tap_count - 1 :, my]
    for j in range(tap_count - 1):
        conv = conv + shifted(branch_in, tap_count - 1 - j, 0.0) * taps[j : j + 1, my]
    conv = conv.astype(jnp.bfloat16)
    gate_x = jax.nn.sigmoid(jnp.dot(conv, gxb[h], preferred_element_type=jnp.float32))
    gate_a = jax.nn.sigmoid(jnp.dot(conv, gab[h], preferred_element_type=jnp.float32))
    log_decay = -gate_power * gate_a * forget[:, my]
    decay = jnp.exp(log_decay)
    scale = jnp.sqrt(-jnp.tanh(log_decay) * (1.0 + decay * decay))
    scale = jnp.where(pos == 0, 1.0, scale)
    run = conv.astype(jnp.float32) * gate_x * scale
    by = 1
    while by < rows:
        run = decay * shifted(run, by, 0.0) + run
        decay = decay * shifted(decay, by, 1.0)
        by *= 2
    mix[...] = (run * jax.nn.gelu(branch_gate)).astype(jnp.bfloat16)
    y_own(5, 6, role=inner)
    forwards((3, 1))()
    with scope("arrive2"):
        arrive(2)

    def refill():
        @pl.when(outer)
        def _():
            near(5, 6)

        far(5)
        forwards((4, 1))()

    scatter(0, mix, wout, s1, s1r, k1, x1r, zs1, z1r, tok, after, (forwards((3, 2)), refill, forwards((3, 3))))
    state = gather_start(1, after, x2)
    far(6)

    forwards((4, 2), (5, 1))()
    relayed = gather_relay(state)
    forwards((4, 3), (6, 1))()
    gather_pass(state, relayed)
    forwards((5, 2))()
    gather_end(relayed)
    with scope("norm2"):
        norm(x2, gain2, nb)
    forwards((6, 2))()
    with scope("arrive34"):
        arrive(3)
        arrive(4)
    last = (((1,), (1,)), ((), ()))

    with scope("ffn"):
        gate_val = lax.dot_general(nb[...], wgate[...], last, preferred_element_type=jnp.float32)
        up_val = lax.dot_general(nb[...], wup[...], last, preferred_element_type=jnp.float32)
        hid[...] = (jax.nn.silu(gate_val) * up_val).astype(jnp.bfloat16)
    forwards((5, 3), (6, 3))()
    with scope("arrive5"):
        arrive(5)
    first = finish(0, hid)
    first[0]()
    with scope("arrive6"):
        arrive(6)
    second = finish(1, hid)
    second[0]()
    first[1]()
    second[1]()
    first[2]()
    second[2]()
    with scope("drain"):
        for copy in started:
            copy.wait_send()

        @pl.when(inner)
        def _():
            for group in groups:
                z_sends[group, 2].wait_send()
                relays[group].wait_send()


def on_device_paired(
    tokens, mix_gain, in_x_w, in_gate_w, conv_taps, gate_x_blocks, gate_a_blocks, forget_rate,
    out_w, ffn_gain, ffn_gate_w, ffn_up_w, ffn_down_w,
):
    rows, feats = tokens.shape
    model = mix_gain.shape[0]
    both = 2 * rows
    share = feats // PARTS
    wide = -(-ffn_down_w.shape[0] // (2 * LANES)) * LANES
    bf, dma = jnp.bfloat16, pltpu.SemaphoreType.DMA
    exchange = [
        pltpu.VMEM((both, model), bf),
        pltpu.VMEM((2, both, feats), bf),
        pltpu.VMEM((2, both, feats), bf),
        pltpu.VMEM((both, feats), bf),
    ]
    vmem = pl.BlockSpec(memory_space=pltpu.VMEM)
    operands = (
        tokens, mix_gain.reshape(1, model), in_x_w, in_gate_w, conv_taps, gate_x_blocks, gate_a_blocks,
        forget_rate.reshape(1, -1), out_w, ffn_gain.reshape(1, model), ffn_gate_w.T, ffn_up_w.T, ffn_down_w,
    )
    return pl.pallas_call(
        kernel,
        out_shape=jax.ShapeDtypeStruct((rows, feats), bf),
        in_specs=[pl.BlockSpec(memory_space=pltpu.HBM)] * 13,
        out_specs=vmem,
        scratch_shapes=[
            *[pltpu.VMEM(operand.shape, operand.dtype) for operand in operands],
            dma((13,)),
            pltpu.VMEM((both, model), bf),
            pltpu.VMEM((both, model), bf),
            pltpu.VMEM((model, 2 * LANES), bf),
            pltpu.VMEM((LANES, model), bf),
            pltpu.VMEM((wide, model), bf),
            pltpu.VMEM((wide, model), bf),
            pltpu.VMEM((PARTS, wide, model // PARTS), bf),
            *exchange,
            pltpu.VMEM((rows, feats), bf),
            pltpu.VMEM((rows, feats), bf),
            pltpu.VMEM((rows, feats), bf),
            pltpu.VMEM((both, LANES), bf),
            pltpu.VMEM((both, model), bf),
            pltpu.VMEM((both, wide), bf),
            pltpu.VMEM((PARTS, both, model // PARTS), bf),
            pltpu.VMEM((PARTS, 2, both, share), bf),
            pltpu.VMEM((PARTS, 2, both, share), bf),
            pltpu.VMEM((PARTS, both, share), bf),
            pltpu.VMEM((PARTS, rows, share), bf),
            pltpu.VMEM((PARTS, 2, rows, share), bf),
            dma((7, 4)), dma((7, 3)), dma((7, 4)), dma((7, 4)), dma((7,)),
            dma((2, 11)), dma((2, 11)), dma((1, 5)), dma((1, 5)), dma((PARTS, 8)), dma((PARTS, 8)),
        ],
        compiler_params=pltpu.CompilerParams(
            collective_id=0, has_side_effects=True, vmem_limit_bytes=48 * 1024 * 1024
        ),
    )(*[pltpu.with_memory_space_constraint(operand, pltpu.HBM) for operand in operands])


def solution(mesh):
    def body(*args):
        if paired(mesh, *args):
            return on_device_paired(*args)
        return on_device(*args)

    placed = (
        P("fs", "tp"),
        P(),
        P("fs", "tp"),
        P("fs", "tp"),
        P(None, "tp"),
        P("tp", None, None),
        P("tp", None, None),
        P("tp"),
        P("tp", "fs"),
        P(),
        P("fs", "tp"),
        P("fs", "tp"),
        P("tp", "fs"),
    )
    return jax.shard_map(
        body, mesh=mesh, in_specs=placed, out_specs=P("fs", "tp"), check_vma=False
    )
```

```python
import functools

import jax
import jax.numpy as jnp
from jax import lax
from jax.experimental import pallas as pl
from jax.experimental.pallas import tpu as pltpu
from jax.sharding import PartitionSpec as P

LANES = 128

epsilon = 1e-06
gate_power = 8.0


def rms_norm(values, gain):
    wide = values.astype(jnp.float32)
    mean_square = jnp.mean(wide * wide, axis=-1, keepdims=True)
    return (wide * lax.rsqrt(mean_square + epsilon) * gain).astype(jnp.bfloat16)


def full_rows(shard):
    return lax.all_gather(shard, "tp", axis=1, tiled=True)


def pair_folder(left_rows, pieces):
    return (
        jnp.dot(left_rows, pieces[0], preferred_element_type=jnp.float32),
        jnp.dot(left_rows, pieces[1], preferred_element_type=jnp.float32),
    )


def project_out(acts, weight):
    partial_terms = jnp.dot(
        acts, lax.all_gather(weight, "fs", axis=1, tiled=True), preferred_element_type=jnp.float32
    )
    return lax.psum_scatter(
        partial_terms.astype(jnp.bfloat16), "tp", scatter_dimension=1, tiled=True
    ).astype(jnp.float32)


def combine(earlier, later):
    return (earlier[0] * later[0], later[0] * earlier[1] + later[1])


def on_device(
    tokens,
    mix_gain,
    in_x_w,
    in_gate_w,
    conv_taps,
    gate_x_blocks,
    gate_a_blocks,
    forget_rate,
    out_w,
    ffn_gain,
    ffn_gate_w,
    ffn_up_w,
    ffn_down_w,
):
    normed = rms_norm(full_rows(tokens), mix_gain)
    length = normed.shape[0]
    chan_width = in_x_w.shape[1]
    branch_in, branch_gate = pair_folder(
        normed,
        (
            lax.all_gather(in_x_w, "fs", axis=0, tiled=True),
            lax.all_gather(in_gate_w, "fs", axis=0, tiled=True),
        ),
    )
    tap_count = conv_taps.shape[0]
    padded = jnp.pad(branch_in, ((tap_count - 1, 0), (0, 0)))
    conv_sum = padded[0:length] * conv_taps[0]
    for index in range(1, tap_count):
        conv_sum = conv_sum + padded[index : index + length] * conv_taps[index]
    conv_out = conv_sum.astype(jnp.bfloat16)
    blocks = gate_x_blocks.shape[0]
    block_dim = gate_x_blocks.shape[1]
    grouped = conv_out.reshape(length, blocks, block_dim)
    gate_x = jax.nn.sigmoid(
        jnp.einsum(
            "tbi,bij->tbj", grouped, gate_x_blocks, preferred_element_type=jnp.float32
        ).reshape(length, chan_width)
    )
    gate_a = jax.nn.sigmoid(
        jnp.einsum(
            "tbi,bij->tbj", grouped, gate_a_blocks, preferred_element_type=jnp.float32
        ).reshape(length, chan_width)
    )
    log_decay = -gate_power * gate_a * forget_rate
    decay = jnp.exp(log_decay)
    scale = jnp.sqrt(-jnp.expm1(2.0 * log_decay))
    scale = jnp.where((jnp.arange(length) == 0)[:, None], 1.0, scale)
    driven = conv_out.astype(jnp.float32) * gate_x * scale
    _, state = lax.associative_scan(combine, (decay, driven), axis=0)
    mixer_out = (state * jax.nn.gelu(branch_gate)).astype(jnp.bfloat16)
    after_mix = (tokens.astype(jnp.float32) + project_out(mixer_out, out_w)).astype(jnp.bfloat16)
    normed_ffn = rms_norm(full_rows(after_mix), ffn_gain)
    gate_val, up_val = pair_folder(
        normed_ffn,
        (
            lax.all_gather(ffn_gate_w, "fs", axis=0, tiled=True),
            lax.all_gather(ffn_up_w, "fs", axis=0, tiled=True),
        ),
    )
    hidden = (jax.nn.silu(gate_val) * up_val).astype(jnp.bfloat16)
    return (after_mix.astype(jnp.float32) + project_out(hidden, ffn_down_w)).astype(jnp.bfloat16)


def paired(mesh, tokens, mix_gain, in_x_w, in_gate_w, conv_taps, gate_x_blocks, *rest):
    ffn_down_w = rest[-1]
    return (
        mesh.shape["fs"] == 8
        and mesh.shape["tp"] == 4
        and gate_x_blocks.shape == (2, LANES, LANES)
        and tokens.shape[0] % 32 == 0
        and tokens.shape[1] == 4 * LANES
        and ffn_down_w.shape[1] == 2 * LANES
        and ffn_down_w.shape[0] % 32 == 0
    )


PARTS = 2


def kernel(
    h_tok, h_gain1, h_x, h_g, h_taps, h_gxb, h_gab, h_forget, h_out, h_gain2, h_gate, h_up, h_dn,
    result,
    tok, gain1, w_x, w_g, taps, gxb, gab, forget, w_out, gain2, w_gate, w_up, w_dn, load_sem,
    x1, nb, win, wout, wgate, wup, wdn, hidp, s1, s1r, k1, x1r, zs1, z1r, after, mix, x2, hid,
    k2, x2r, zs2, z2r,
    send_z, recv_z, send_y, recv_y, own_sem, ag_send, ag_recv, rs_send, rs_recv, fin_send, fin_recv,
    cross_recv, core_send, core_recv,
):
    f, t = lax.axis_index("fs"), lax.axis_index("tp")
    z, y = f // 2, f % 2
    h = z % 2
    outer = (z == 0) | (z == 3)
    inner = (z == 1) | (z == 2)
    rows, feats = tok.shape
    near_z = z + 1 - 2 * h
    far_outer = 3 * (1 - z // 2)
    far_inner = 2 - z // 2
    sources = (z, near_z, far_outer, far_inner)
    fz = tuple(zz * 2 + y for zz in sources)
    fy = z * 2 + 1 - y
    t_core = t + 1 - 2 * (t % 2)
    t_x = (t + 2) % 4
    t_xc = (t_core + 2) % 4
    model = x1.shape[1]
    scope = jax.named_scope

    held = (tok, w_x, w_g, w_out, w_gate, w_up, w_dn, gain1, taps, gxb, gab, forget, gain2)
    given = (h_tok, h_x, h_g, h_out, h_gate, h_up, h_dn, h_gain1, h_taps, h_gxb, h_gab, h_forget, h_gain2)
    loads = [pltpu.make_async_copy(src, dst, load_sem.at[i]) for i, (src, dst) in enumerate(zip(given, held))]
    for load in loads:
        load.start()

    barrier = pltpu.get_barrier_semaphore()
    peers = [(fz[1], t), (fz[3], t), (fy, t), (fy, t_core), (f, t_core), (f, t_x)]

    def greet(peer):
        pl.semaphore_signal(barrier, inc=1, device_id=peer, device_id_type=pl.DeviceIdType.MESH)

    for peer in peers:
        greet(peer)

    @pl.when(inner)
    def _():
        greet((fz[2], t))

    with scope("barrier"):
        pl.semaphore_wait(barrier, len(peers) + jnp.where(inner, 1, 0))

    started = []

    def describe(src, dst, s_sem, r_sem, peer):
        return pltpu.make_async_remote_copy(
            src_ref=src, dst_ref=dst, send_sem=s_sem, recv_sem=r_sem,
            device_id=peer, device_id_type=pl.DeviceIdType.MESH,
        )

    def send(src, dst, s_sem, r_sem, peer):
        copy = describe(src, dst, s_sem, r_sem, peer)
        copy.start()
        started.append(copy)
        return copy

    def span(index, width):
        return pl.ds(pl.multiple_of(index * width, width), width)

    depth = w_x.shape[0]
    cols = w_out.shape[1]
    part_cols = cols // PARTS
    half_ff = w_dn.shape[0] // 2
    fill = wgate.shape[0] - half_ff
    last_group = 5 + PARTS
    quarter = half_ff // 2
    core = t % 2

    def piece(group, half, stored=False):
        if group < 2:
            return ((h_x, h_g) if stored else (w_x, w_g))[group].at[:, span(half, LANES)]
        if group == 2:
            return (h_out if stored else w_out).at[span(half, LANES), :]
        if group < 5:
            return ((h_gate, h_up) if stored else (w_gate, w_up))[group - 3].at[span(half, half_ff), :]
        down = h_dn if stored else w_dn
        if group == 5:
            return down.at[span(half, half_ff), pl.ds(0, part_cols)]
        return down.at[span(2 * half + group - 6, quarter), pl.ds(part_cols, part_cols)]

    def place(group, source):
        if group < 2:
            return win.at[span(source, depth), pl.ds(group * LANES, LANES)]
        if group == 2:
            return wout.at[:, span(source, cols)]
        if group < 5:
            return (wgate, wup)[group - 3].at[pl.ds(0, half_ff), span(source, cols)]
        if group == 5:
            return wdn.at[0, core, pl.ds(0, half_ff), span(source, part_cols)]
        return wdn.at[1, core, pl.ds((group - 6) * quarter, quarter), span(source, part_cols)]

    groups = range(last_group + 1)
    own_copies = {}
    for group in groups:
        own_copies[group] = pltpu.make_async_copy(piece(group, h, True), place(group, f), own_sem.at[group])
        own_copies[group].start()

    slot = jnp.where(outer, 2, 3)
    z_sends = {}
    for group in groups:
        for way, peer in ((1, fz[1]), (2, fz[2]), (3, fz[3])):
            half = (1 - h, far_outer % 2, far_inner % 2)[way - 1]
            at = 1 if way == 1 else slot
            z_sends[group, way] = describe(
                piece(group, half), place(group, f), send_z.at[group, way - 1], recv_z.at[group, at - 1], (peer, t)
            )
            if way != 2:
                started.append(z_sends[group, way])
    y_copies, relays = {}, {}

    after_relay = {
        0: ((2, 2), (2, 3)), 2: ((3, 2), (3, 3)), 3: ((4, 2), (4, 3)), 4: ((5, 2), (5, 3)), 5: ((6, 2), (7, 2)), 6: ((6, 3),), 7: ((7, 3),),
    }

    def near(*names):
        for group in names:
            z_sends[group, 1].start()

    def far(*names):
        @pl.when(outer)
        def _():
            for group in names:
                z_sends[group, 3].start()

    core_copies = []

    def send_y_piece(group, d, src, dst, source_z):
        if group < 5:
            return describe(src, dst, send_y.at[group, d], recv_y.at[group, d], (fy, t))
        arrived = cross_recv.at[group - 5, core, source_z // 2]
        return describe(src, dst, send_y.at[group, d], arrived, (fy, t - core + source_z % 2))

    def pass_to_core(group, d, src, dst, source_z):
        if group >= 5:
            copy = describe(
                src, dst, core_send.at[group - 5, d], core_recv.at[group - 5, source_z // 2], (f, t_core)
            )
            other = source_z % 2 != core
            core_copies.append((other, copy))
            pl.when(other)(copy.start)

    for group in groups:
        y_copies[group, 0] = send_y_piece(group, 0, piece(group, h), place(group, f), z)
        started.append(y_copies[group, 0])

    def y_own(*names, role=None):
        def go():
            for group in names:
                y_copies[group, 0].start()

        go() if role is None else pl.when(role)(go)

    def core_own():
        for group in groups[5:]:
            pass_to_core(group, 0, piece(group, h), place(group, f), z)

    def pick(when_inner, when_outer):
        return jnp.where(inner, when_inner, when_outer)

    early = (pick(1, 3), pick(2, 1), pick(3, 2)), (pick(fz[1], fz[3]), pick(fz[2], fz[1]), pick(fz[3], fz[2]))
    middle = (1, 3, 2), (fz[1], fz[3], fz[2])
    late = (1, pick(2, 3), pick(3, 2)), (fz[1], pick(fz[2], fz[3]), pick(fz[3], fz[2]))

    def forward(group, d):
        arrival, arrival_fz = early if group < 3 else middle if group < 5 else late
        block = place(group, arrival_fz[d - 1])
        describe(
            block, block, send_z.at[group, 0], recv_z.at[group, arrival[d - 1] - 1], (fz[1], t)
        ).wait_recv()
        y_copies[group, d] = send_y_piece(group, d, block, block, arrival_fz[d - 1] // 2)
        y_copies[group, d].start()
        started.append(y_copies[group, d])
        pass_to_core(group, d, block, block, arrival_fz[d - 1] // 2)
        if d == 1:
            relays[group] = describe(block, block, send_z.at[group, 3], recv_z.at[group, 1], (fz[2], t))

            @pl.when(inner)
            def _():
                relays[group].start()
                for key in after_relay.get(group, ()):
                    z_sends[key].start()

    def arrive(group):
        own_copies[group].wait()
        if group < 5:
            for d in range(4):
                y_copies[group, d].wait_recv()
            return
        block = place(group, f)
        ready = [cross_recv.at[group - 5, i, j] for i in range(2) for j in range(2)]
        for semaphore in ready + [core_recv.at[group - 5, j] for j in range(2)]:
            describe(block, block, send_y.at[group, 0], semaphore, (fy, t)).wait_recv()

    mine, theirs = span(h, rows), span(1 - h, rows)
    cut = rows // 2

    def some(block, c):
        return pl.ds(pl.multiple_of(block * rows + c * cut, cut), cut)

    def gather_start(k, own, x):
        x_peer, core_peer = (f, t_x), (f, t_core)

        def go(i, src, dst, peer):
            return send(src, dst, ag_send.at[k, i], ag_recv.at[k, i], peer)

        at = span(t, feats)
        by_z = [go(c, own.at[pl.ds(c * cut, cut), :], x.at[some(h, c), at], (fz[1], t)) for c in range(2)]
        by_x = go(2, own, x.at[mine, at], x_peer)
        by_core = go(3, own, x.at[mine, at], core_peer)
        x[mine, at] = own[...]
        return go, by_z, by_x, by_core, x_peer, core_peer, x

    def gather_relay(state):
        go, by_z, by_x, by_core, x_peer, core_peer, x = state
        across, inside = [], [by_core]
        at = span(t, feats)
        with scope("byz"):
            for c in range(2):
                by_z[c].wait_recv()
                block = x.at[some(1 - h, c), at]
                across.append(go(4 + c, block, block, x_peer))
                inside.append(go(6 + c, block, block, core_peer))
        with scope("byx"):
            by_x.wait_recv()
        block = x.at[mine, span(t_x, feats)]
        inside.append(go(8, block, block, core_peer))
        return across, inside

    def gather_pass(state, relayed):
        go, core_peer, x = state[0], state[5], state[6]
        across, inside = relayed
        with scope("across"):
            for c in range(2):
                across[c].wait_recv()
                block = x.at[some(1 - h, c), span(t_x, feats)]
                inside.append(go(9 + c, block, block, core_peer))

    def gather_end(relayed):
        with scope("inside"):
            for copy in relayed[1]:
                copy.wait_recv()

    def norm(x, gain, out):
        step = 32

        def one(i, carry):
            at = pl.ds(pl.multiple_of(i * step, step), step)
            wide = x[at, :].astype(jnp.float32)
            scale = lax.rsqrt(jnp.mean(wide * wide, axis=-1, keepdims=True) + epsilon)
            out[at, :] = (wide * scale * gain[...]).astype(jnp.bfloat16)
            return carry

        lax.fori_loop(0, x.shape[0] // step, one, 0)

    def scatter(k, acts, weight, s, r1, keep, r2, s3, r3, base, out, hooks):
        core_peer, x_peer = (f, t_core), (f, t_x)

        def project(block):
            at = span(block, feats)
            s[:, at] = jnp.dot(acts[...], weight[:, at], preferred_element_type=jnp.float32).astype(jnp.bfloat16)
            return s.at[:, at]

        a = send(project(t_xc), r1.at[0], rs_send.at[k, 0], rs_recv.at[k, 0], core_peer)
        b = send(project(t_core), r1.at[1], rs_send.at[k, 1], rs_recv.at[k, 1], core_peer)
        project(t_x)
        project(t)
        with scope("rs_a"):
            a.wait_recv()
        at = span(t_x, feats)
        for i, block in ((0, theirs), (1, mine)):
            keep[0, block, :] = (s[block, at].astype(jnp.float32) + r1[0, block, :].astype(jnp.float32)).astype(jnp.bfloat16)
            copy = send(keep.at[0, block], r2.at[block], rs_send.at[k, 2 + i], rs_recv.at[k, 2 + i], x_peer)
            if i == 0:
                c0 = copy
        c1 = copy
        hooks[0]()
        with scope("rs_c0"):
            b.wait_recv()
            c0.wait_recv()

        def total(where):
            return (
                s[where, span(t, feats)].astype(jnp.float32)
                + r1[1, where, :].astype(jnp.float32)
                + r2[where, :].astype(jnp.float32)
            )

        s3[...] = total(theirs).astype(jnp.bfloat16)
        e = send(s3, r3, rs_send.at[k, 4], rs_recv.at[k, 4], (fz[1], t))
        hooks[1]()
        with scope("rs_c1"):
            c1.wait_recv()
        part = total(mine)
        hooks[2]()
        with scope("rs_e"):
            e.wait_recv()
        out[...] = (base[...].astype(jnp.float32) + (part + r3[...].astype(jnp.float32))).astype(jnp.bfloat16)

    def finish(p, acts):
        x_peer, z_peer = (f, t_x), (fz[1], t)
        wide = feats // PARTS
        low, high = pl.ds(0, wide // 2), pl.ds(wide // 2, wide // 2)
        keep, r2, s3, r3 = k2.at[p], x2r.at[p], zs2.at[p], z2r.at[p]

        def project_pair(block):
            at = span(block, wide)
            return jnp.dot(acts[...], wdn[p, core, :, at], preferred_element_type=jnp.float32) + jnp.dot(
                hidp[...], wdn[p, 1 - core, :, at], preferred_element_type=jnp.float32
            )

        def go(i, src, dst, peer):
            return send(src, dst, fin_send.at[p, i], fin_recv.at[p, i], peer)

        waits = {}

        def cross():
            keep[0] = project_pair(t_x).astype(jnp.bfloat16)
            waits["d"] = go(3, keep.at[0, theirs, high], r3.at[0, :, high], z_peer)
            waits["c"] = go(2, keep.at[0, theirs, low], r2.at[theirs, low], x_peer)
            waits["m"] = go(7, keep.at[0, mine, low], r2.at[mine, low], x_peer)
            keep[1] = project_pair(t).astype(jnp.bfloat16)
            waits["e"] = go(4, keep.at[1, theirs, high], r3.at[1, :, high], z_peer)

        def turn():
            with scope(f"fin_d{p}"):
                waits["d"].wait_recv()
            s3[:, high] = (
                keep[0, mine, high].astype(jnp.float32) + r3[0, :, high].astype(jnp.float32)
            ).astype(jnp.bfloat16)
            waits["g"] = go(5, s3.at[:, high], r2.at[pl.ds(0, rows), high], x_peer)
            with scope(f"fin_c{p}"):
                waits["c"].wait_recv()
            s3[:, low] = (
                keep[1, theirs, low].astype(jnp.float32) + r2[theirs, low].astype(jnp.float32)
            ).astype(jnp.bfloat16)
            waits["l"] = go(6, s3.at[:, low], r3.at[0, :, low], z_peer)

        def end():
            with scope(f"fin_g{p}"):
                waits["e"].wait_recv()
                waits["g"].wait_recv()
            left, right = pl.ds(p * part_cols, part_cols), pl.ds(cols + p * part_cols, part_cols)
            result[:, right] = (
                after[:, right].astype(jnp.float32)
                + (keep[1, mine, high].astype(jnp.float32) + r3[1, :, high].astype(jnp.float32))
                + r2[pl.ds(0, rows), high].astype(jnp.float32)
            ).astype(jnp.bfloat16)
            with scope(f"fin_l{p}"):
                waits["m"].wait_recv()
                waits["l"].wait_recv()
            result[:, left] = (
                after[:, left].astype(jnp.float32)
                + (keep[1, mine, low].astype(jnp.float32) + r2[mine, low].astype(jnp.float32))
                + r3[0, :, low].astype(jnp.float32)
            ).astype(jnp.bfloat16)

        return cross, turn, end

    def forwards(*pairs):
        def go():
            for group, d in pairs:
                with scope(f"fw{group}{d}"):
                    forward(group, d)

        return go

    nothing = forwards()
    for load in loads[:1]:
        load.wait()
    state = gather_start(0, tok, x1)
    for load in loads[1:]:
        load.wait()
    y_own(0, 1)

    for group in range(4):
        near(group)
        far(group)

    @pl.when(inner)
    def _():
        for group in range(2):
            z_sends[group, 2].start()
            z_sends[group, 3].start()

    y_own(2, 3)
    y_own(5, role=outer)
    core_own()
    if fill:
        for w in (wgate, wup):
            w[pl.ds(half_ff, fill), :] = jnp.zeros((fill, model), jnp.bfloat16)
        for p in range(PARTS):
            for i in range(2):
                wdn[p, i, pl.ds(half_ff, fill), :] = jnp.zeros((fill, wdn.shape[3]), jnp.bfloat16)
    relayed = gather_relay(state)
    forwards((0, 1), (0, 2), (0, 3), (1, 1), (1, 2))()
    y_own(6, 7, role=outer)
    forwards((1, 3))()
    gather_pass(state, relayed)
    forwards((2, 1))()
    gather_end(relayed)
    forwards((2, 2))()
    with scope("norm1"):
        norm(x1, gain1, nb)
    forwards((2, 3))()
    y_own(4)
    near(4)
    far(4)

    @pl.when(inner)
    def _():
        near(5, 6, 7)


    with scope("arrive01"):
        arrive(0)
        arrive(1)
    both = jnp.dot(nb[...], win[...], preferred_element_type=jnp.float32)
    branch_in, branch_gate = both[:, :LANES], both[:, LANES:]
    row = lax.broadcasted_iota(jnp.int32, branch_in.shape, 0)
    pos = jnp.where(row >= rows, row - rows, row)

    def shifted(values, by, fill):
        return jnp.where(pos >= by, pltpu.roll(values, by, 0), fill)

    tap_count = taps.shape[0]
    my = span(h, LANES)
    conv = branch_in * taps[tap_count - 1 :, my]
    for j in range(tap_count - 1):
        conv = conv + shifted(branch_in, tap_count - 1 - j, 0.0) * taps[j : j + 1, my]
    conv = conv.astype(jnp.bfloat16)
    gate_x = jax.nn.sigmoid(jnp.dot(conv, gxb[h], preferred_element_type=jnp.float32))
    gate_a = jax.nn.sigmoid(jnp.dot(conv, gab[h], preferred_element_type=jnp.float32))
    log_decay = -gate_power * gate_a * forget[:, my]
    decay = jnp.exp(log_decay)
    scale = jnp.sqrt(-jnp.tanh(log_decay) * (1.0 + decay * decay))
    scale = jnp.where(pos == 0, 1.0, scale)
    run = conv.astype(jnp.float32) * gate_x * scale
    by = 1
    while by < rows:
        run = decay * shifted(run, by, 0.0) + run
        decay = decay * shifted(decay, by, 1.0)
        by *= 2
    mix[...] = (run * jax.nn.gelu(branch_gate)).astype(jnp.bfloat16)
    y_own(5, 6, 7, role=inner)
    forwards((3, 1))()
    with scope("arrive2"):
        arrive(2)

    def refill():
        @pl.when(outer)
        def _():
            near(5, 6, 7)

        far(5)
        forwards((4, 1))()

    scatter(0, mix, wout, s1, s1r, k1, x1r, zs1, z1r, tok, after, (forwards((3, 2)), refill, forwards((3, 3))))
    state = gather_start(1, after, x2)
    far(6, 7)

    forwards((4, 2), (5, 1))()
    relayed = gather_relay(state)
    forwards((4, 3), (6, 1), (7, 1))()
    gather_pass(state, relayed)
    forwards((5, 2))()
    gather_end(relayed)
    with scope("norm2"):
        norm(x2, gain2, nb)
    forwards((5, 3))()
    with scope("arrive34"):
        arrive(3)
        arrive(4)
    last = (((1,), (1,)), ((), ()))

    with scope("ffn"):
        gate_val = lax.dot_general(nb[...], wgate[...], last, preferred_element_type=jnp.float32)
        up_val = lax.dot_general(nb[...], wup[...], last, preferred_element_type=jnp.float32)
        hid[...] = (jax.nn.silu(gate_val) * up_val).astype(jnp.bfloat16)
    hid_copy = send(hid, hidp, core_send.at[3, 0], core_recv.at[3, 0], (f, t_core))
    forwards((6, 2), (7, 2), (6, 3), (7, 3))()
    with scope("arrive5"):
        hid_copy.wait_recv()
        arrive(5)
    first = finish(0, hid)
    first[0]()
    with scope("arrive6"):
        arrive(6)
        arrive(7)
    second = finish(1, hid)
    second[0]()
    first[1]()
    second[1]()
    first[2]()
    second[2]()
    with scope("drain"):
        for copy in started:
            copy.wait_send()
        for other, copy in core_copies:
            pl.when(other)(copy.wait_send)

        @pl.when(inner)
        def _():
            for group in groups:
                z_sends[group, 2].wait_send()
                relays[group].wait_send()


def on_device_paired(
    tokens, mix_gain, in_x_w, in_gate_w, conv_taps, gate_x_blocks, gate_a_blocks, forget_rate,
    out_w, ffn_gain, ffn_gate_w, ffn_up_w, ffn_down_w,
):
    rows, feats = tokens.shape
    model = mix_gain.shape[0]
    both = 2 * rows
    share = feats // PARTS
    wide = -(-ffn_down_w.shape[0] // (2 * LANES)) * LANES
    bf, dma = jnp.bfloat16, pltpu.SemaphoreType.DMA
    exchange = [
        pltpu.VMEM((both, model), bf),
        pltpu.VMEM((2, both, feats), bf),
        pltpu.VMEM((2, both, feats), bf),
        pltpu.VMEM((both, feats), bf),
    ]
    vmem = pl.BlockSpec(memory_space=pltpu.VMEM)
    operands = (
        tokens, mix_gain.reshape(1, model), in_x_w, in_gate_w, conv_taps, gate_x_blocks, gate_a_blocks,
        forget_rate.reshape(1, -1), out_w, ffn_gain.reshape(1, model), ffn_gate_w.T, ffn_up_w.T, ffn_down_w,
    )
    return pl.pallas_call(
        kernel,
        out_shape=jax.ShapeDtypeStruct((rows, feats), bf),
        in_specs=[pl.BlockSpec(memory_space=pltpu.HBM)] * 13,
        out_specs=vmem,
        scratch_shapes=[
            *[pltpu.VMEM(operand.shape, operand.dtype) for operand in operands],
            dma((13,)),
            pltpu.VMEM((both, model), bf),
            pltpu.VMEM((both, model), bf),
            pltpu.VMEM((model, 2 * LANES), bf),
            pltpu.VMEM((LANES, model), bf),
            pltpu.VMEM((wide, model), bf),
            pltpu.VMEM((wide, model), bf),
            pltpu.VMEM((PARTS, 2, wide, model // PARTS), bf),
            pltpu.VMEM((both, wide), bf),
            *exchange,
            pltpu.VMEM((rows, feats), bf),
            pltpu.VMEM((rows, feats), bf),
            pltpu.VMEM((rows, feats), bf),
            pltpu.VMEM((both, LANES), bf),
            pltpu.VMEM((both, model), bf),
            pltpu.VMEM((both, wide), bf),
            pltpu.VMEM((PARTS, 2, both, share), bf),
            pltpu.VMEM((PARTS, both, share), bf),
            pltpu.VMEM((PARTS, rows, share), bf),
            pltpu.VMEM((PARTS, 2, rows, share), bf),
            dma((8, 4)), dma((8, 3)), dma((8, 4)), dma((8, 4)), dma((8,)),
            dma((2, 11)), dma((2, 11)), dma((1, 5)), dma((1, 5)), dma((PARTS, 8)), dma((PARTS, 8)),
            dma((3, 2, 2)), dma((4, 4)), dma((4, 2)),
        ],
        compiler_params=pltpu.CompilerParams(
            collective_id=0, has_side_effects=True, vmem_limit_bytes=48 * 1024 * 1024
        ),
    )(*[pltpu.with_memory_space_constraint(operand, pltpu.HBM) for operand in operands])


def solution(mesh):
    def body(*args):
        if paired(mesh, *args):
            return on_device_paired(*args)
        return on_device(*args)

    placed = (
        P("fs", "tp"),
        P(),
        P("fs", "tp"),
        P("fs", "tp"),
        P(None, "tp"),
        P("tp", None, None),
        P("tp", None, None),
        P("tp"),
        P("tp", "fs"),
        P(),
        P("fs", "tp"),
        P("fs", "tp"),
        P("tp", "fs"),
    )
    return jax.shard_map(
        body, mesh=mesh, in_specs=placed, out_specs=P("fs", "tp"), check_vma=False
    )
```

```python
import functools

import jax
import jax.numpy as jnp
from jax import lax
from jax.experimental import pallas as pl
from jax.experimental.pallas import tpu as pltpu
from jax.sharding import PartitionSpec as P

LANES = 128

epsilon = 1e-06
gate_power = 8.0


def rms_norm(values, gain):
    wide = values.astype(jnp.float32)
    mean_square = jnp.mean(wide * wide, axis=-1, keepdims=True)
    return (wide * lax.rsqrt(mean_square + epsilon) * gain).astype(jnp.bfloat16)


def full_rows(shard):
    return lax.all_gather(shard, "tp", axis=1, tiled=True)


def pair_folder(left_rows, pieces):
    return (
        jnp.dot(left_rows, pieces[0], preferred_element_type=jnp.float32),
        jnp.dot(left_rows, pieces[1], preferred_element_type=jnp.float32),
    )


def project_out(acts, weight):
    partial_terms = jnp.dot(
        acts, lax.all_gather(weight, "fs", axis=1, tiled=True), preferred_element_type=jnp.float32
    )
    return lax.psum_scatter(
        partial_terms.astype(jnp.bfloat16), "tp", scatter_dimension=1, tiled=True
    ).astype(jnp.float32)


def combine(earlier, later):
    return (earlier[0] * later[0], later[0] * earlier[1] + later[1])


def on_device(
    tokens,
    mix_gain,
    in_x_w,
    in_gate_w,
    conv_taps,
    gate_x_blocks,
    gate_a_blocks,
    forget_rate,
    out_w,
    ffn_gain,
    ffn_gate_w,
    ffn_up_w,
    ffn_down_w,
):
    normed = rms_norm(full_rows(tokens), mix_gain)
    length = normed.shape[0]
    chan_width = in_x_w.shape[1]
    branch_in, branch_gate = pair_folder(
        normed,
        (
            lax.all_gather(in_x_w, "fs", axis=0, tiled=True),
            lax.all_gather(in_gate_w, "fs", axis=0, tiled=True),
        ),
    )
    tap_count = conv_taps.shape[0]
    padded = jnp.pad(branch_in, ((tap_count - 1, 0), (0, 0)))
    conv_sum = padded[0:length] * conv_taps[0]
    for index in range(1, tap_count):
        conv_sum = conv_sum + padded[index : index + length] * conv_taps[index]
    conv_out = conv_sum.astype(jnp.bfloat16)
    blocks = gate_x_blocks.shape[0]
    block_dim = gate_x_blocks.shape[1]
    grouped = conv_out.reshape(length, blocks, block_dim)
    gate_x = jax.nn.sigmoid(
        jnp.einsum(
            "tbi,bij->tbj", grouped, gate_x_blocks, preferred_element_type=jnp.float32
        ).reshape(length, chan_width)
    )
    gate_a = jax.nn.sigmoid(
        jnp.einsum(
            "tbi,bij->tbj", grouped, gate_a_blocks, preferred_element_type=jnp.float32
        ).reshape(length, chan_width)
    )
    log_decay = -gate_power * gate_a * forget_rate
    decay = jnp.exp(log_decay)
    scale = jnp.sqrt(-jnp.expm1(2.0 * log_decay))
    scale = jnp.where((jnp.arange(length) == 0)[:, None], 1.0, scale)
    driven = conv_out.astype(jnp.float32) * gate_x * scale
    _, state = lax.associative_scan(combine, (decay, driven), axis=0)
    mixer_out = (state * jax.nn.gelu(branch_gate)).astype(jnp.bfloat16)
    after_mix = (tokens.astype(jnp.float32) + project_out(mixer_out, out_w)).astype(jnp.bfloat16)
    normed_ffn = rms_norm(full_rows(after_mix), ffn_gain)
    gate_val, up_val = pair_folder(
        normed_ffn,
        (
            lax.all_gather(ffn_gate_w, "fs", axis=0, tiled=True),
            lax.all_gather(ffn_up_w, "fs", axis=0, tiled=True),
        ),
    )
    hidden = (jax.nn.silu(gate_val) * up_val).astype(jnp.bfloat16)
    return (after_mix.astype(jnp.float32) + project_out(hidden, ffn_down_w)).astype(jnp.bfloat16)


def paired(mesh, tokens, mix_gain, in_x_w, in_gate_w, conv_taps, gate_x_blocks, *rest):
    ffn_down_w = rest[-1]
    return (
        mesh.shape["fs"] == 8
        and mesh.shape["tp"] == 4
        and gate_x_blocks.shape == (2, LANES, LANES)
        and tokens.shape[0] % 32 == 0
        and tokens.shape[1] == 4 * LANES
        and ffn_down_w.shape[1] == 2 * LANES
        and ffn_down_w.shape[0] % 32 == 0
    )


PARTS = 2


def kernel(
    h_tok, h_gain1, h_x, h_g, h_taps, h_gxb, h_gab, h_forget, h_out, h_gain2, h_gate, h_up, h_dn,
    result,
    tok, gain1, w_x, w_g, taps, gxb, gab, forget, w_out, gain2, w_gate, w_up, w_dn, load_sem,
    x1, nb, win, wout, wgate, wup, wdn, hidp, s1, s1r, k1, x1r, zs1, z1r, after, mix, x2, hid,
    k2, x2r, zs2, z2r,
    send_z, recv_z, send_y, recv_y, own_sem, ag_send, ag_recv, rs_send, rs_recv, fin_send, fin_recv,
    cross_recv, core_send, core_recv,
):
    f, t = lax.axis_index("fs"), lax.axis_index("tp")
    z, y = f // 2, f % 2
    h = z % 2
    outer = (z == 0) | (z == 3)
    inner = (z == 1) | (z == 2)
    rows, feats = tok.shape
    near_z = z + 1 - 2 * h
    far_outer = 3 * (1 - z // 2)
    far_inner = 2 - z // 2
    sources = (z, near_z, far_outer, far_inner)
    fz = tuple(zz * 2 + y for zz in sources)
    fy = z * 2 + 1 - y
    t_core = t + 1 - 2 * (t % 2)
    t_x = (t + 2) % 4
    t_xc = (t_core + 2) % 4
    model = x1.shape[1]
    scope = jax.named_scope

    held = (tok, w_x, w_g, w_out, w_gate, w_up, w_dn, gain1, taps, gxb, gab, forget, gain2)
    given = (h_tok, h_x, h_g, h_out, h_gate, h_up, h_dn, h_gain1, h_taps, h_gxb, h_gab, h_forget, h_gain2)
    loads = [pltpu.make_async_copy(src, dst, load_sem.at[i]) for i, (src, dst) in enumerate(zip(given, held))]
    for load in loads:
        load.start()

    barrier = pltpu.get_barrier_semaphore()
    peers = [(fz[1], t), (fz[3], t), (fy, t), (fy, t_core), (f, t_core), (f, t_x)]

    def greet(peer):
        pl.semaphore_signal(barrier, inc=1, device_id=peer, device_id_type=pl.DeviceIdType.MESH)

    for peer in peers:
        greet(peer)

    @pl.when(inner)
    def _():
        greet((fz[2], t))

    with scope("barrier"):
        pl.semaphore_wait(barrier, len(peers) + jnp.where(inner, 1, 0))

    started = []

    def describe(src, dst, s_sem, r_sem, peer):
        return pltpu.make_async_remote_copy(
            src_ref=src, dst_ref=dst, send_sem=s_sem, recv_sem=r_sem,
            device_id=peer, device_id_type=pl.DeviceIdType.MESH,
        )

    def send(src, dst, s_sem, r_sem, peer):
        copy = describe(src, dst, s_sem, r_sem, peer)
        copy.start()
        started.append(copy)
        return copy

    def span(index, width):
        return pl.ds(pl.multiple_of(index * width, width), width)

    depth = w_x.shape[0]
    cols = w_out.shape[1]
    part_cols = cols // PARTS
    half_ff = w_dn.shape[0] // 2
    fill = wgate.shape[0] - half_ff
    last_group = 5 + PARTS
    quarter = half_ff // 2
    core = t % 2

    def piece(group, half, stored=False):
        if group < 2:
            return ((h_x, h_g) if stored else (w_x, w_g))[group].at[:, span(half, LANES)]
        if group == 2:
            return (h_out if stored else w_out).at[span(half, LANES), :]
        if group < 5:
            return ((h_gate, h_up) if stored else (w_gate, w_up))[group - 3].at[span(half, half_ff), :]
        down = h_dn if stored else w_dn
        if group == 5:
            return down.at[span(half, half_ff), pl.ds(0, part_cols)]
        return down.at[span(2 * half + group - 6, quarter), pl.ds(part_cols, part_cols)]

    def place(group, source):
        if group < 2:
            return win.at[span(source, depth), pl.ds(group * LANES, LANES)]
        if group == 2:
            return wout.at[:, span(source, cols)]
        if group < 5:
            return (wgate, wup)[group - 3].at[pl.ds(0, half_ff), span(source, cols)]
        if group == 5:
            return wdn.at[0, core, pl.ds(0, half_ff), span(source, part_cols)]
        return wdn.at[1, core, pl.ds((group - 6) * quarter, quarter), span(source, part_cols)]

    groups = range(last_group + 1)
    own_copies = {}
    for group in groups:
        own_copies[group] = pltpu.make_async_copy(piece(group, h, True), place(group, f), own_sem.at[group])
        own_copies[group].start()

    slot = jnp.where(outer, 2, 3)
    z_sends = {}
    for group in groups:
        for way, peer in ((1, fz[1]), (2, fz[2]), (3, fz[3])):
            half = (1 - h, far_outer % 2, far_inner % 2)[way - 1]
            at = 1 if way == 1 else slot
            z_sends[group, way] = describe(
                piece(group, half), place(group, f), send_z.at[group, way - 1], recv_z.at[group, at - 1], (peer, t)
            )
            if way != 2:
                started.append(z_sends[group, way])
    y_copies, relays = {}, {}

    after_relay = {
        0: ((2, 2), (2, 3)), 2: ((3, 2), (3, 3)), 3: ((4, 2), (4, 3)), 4: ((5, 2), (5, 3)), 5: ((6, 2), (7, 2)), 6: ((6, 3),), 7: ((7, 3),),
    }

    def near(*names):
        for group in names:
            z_sends[group, 1].start()

    def far(*names):
        @pl.when(outer)
        def _():
            for group in names:
                z_sends[group, 3].start()

    core_copies = []

    def send_y_piece(group, d, src, dst, source_z):
        if group < 5:
            return describe(src, dst, send_y.at[group, d], recv_y.at[group, d], (fy, t))
        arrived = cross_recv.at[group - 5, core, source_z // 2]
        return describe(src, dst, send_y.at[group, d], arrived, (fy, t - core + source_z % 2))

    def pass_to_core(group, d, src, dst, source_z):
        if group >= 5:
            copy = describe(
                src, dst, core_send.at[group - 5, d], core_recv.at[group - 5, source_z // 2], (f, t_core)
            )
            other = source_z % 2 != core
            core_copies.append((other, copy))
            pl.when(other)(copy.start)

    for group in groups:
        y_copies[group, 0] = send_y_piece(group, 0, piece(group, h), place(group, f), z)
        started.append(y_copies[group, 0])

    def y_own(*names, role=None):
        def go():
            for group in names:
                y_copies[group, 0].start()

        go() if role is None else pl.when(role)(go)

    def core_own():
        for group in groups[5:]:
            pass_to_core(group, 0, piece(group, h), place(group, f), z)

    def pick(when_inner, when_outer):
        return jnp.where(inner, when_inner, when_outer)

    early = (pick(1, 3), pick(2, 1), pick(3, 2)), (pick(fz[1], fz[3]), pick(fz[2], fz[1]), pick(fz[3], fz[2]))
    middle = (1, 3, 2), (fz[1], fz[3], fz[2])
    late = (1, pick(2, 3), pick(3, 2)), (fz[1], pick(fz[2], fz[3]), pick(fz[3], fz[2]))

    def forward(group, d):
        arrival, arrival_fz = early if group < 3 else middle if group < 5 else late
        block = place(group, arrival_fz[d - 1])
        describe(
            block, block, send_z.at[group, 0], recv_z.at[group, arrival[d - 1] - 1], (fz[1], t)
        ).wait_recv()
        y_copies[group, d] = send_y_piece(group, d, block, block, arrival_fz[d - 1] // 2)
        y_copies[group, d].start()
        started.append(y_copies[group, d])
        pass_to_core(group, d, block, block, arrival_fz[d - 1] // 2)
        if d == 1:
            relays[group] = describe(block, block, send_z.at[group, 3], recv_z.at[group, 1], (fz[2], t))

            @pl.when(inner)
            def _():
                relays[group].start()
                for key in after_relay.get(group, ()):
                    z_sends[key].start()

    def arrive(group):
        own_copies[group].wait()
        if group < 5:
            for d in range(4):
                y_copies[group, d].wait_recv()
            return
        block = place(group, f)
        ready = [cross_recv.at[group - 5, i, j] for i in range(2) for j in range(2)]
        for semaphore in ready + [core_recv.at[group - 5, j] for j in range(2)]:
            describe(block, block, send_y.at[group, 0], semaphore, (fy, t)).wait_recv()

    mine, theirs = span(h, rows), span(1 - h, rows)
    cut = rows // 2

    def some(block, c):
        return pl.ds(pl.multiple_of(block * rows + c * cut, cut), cut)

    def gather_start(k, own, x):
        x_peer, core_peer = (f, t_x), (f, t_core)

        def go(i, src, dst, peer):
            return send(src, dst, ag_send.at[k, i], ag_recv.at[k, i], peer)

        at = span(t, feats)
        by_z = [go(c, own.at[pl.ds(c * cut, cut), :], x.at[some(h, c), at], (fz[1], t)) for c in range(2)]
        by_x = go(2, own, x.at[mine, at], x_peer)
        by_core = go(3, own, x.at[mine, at], core_peer)
        x[mine, at] = own[...]
        return go, by_z, by_x, by_core, x_peer, core_peer, x

    def gather_relay(state):
        go, by_z, by_x, by_core, x_peer, core_peer, x = state
        across, inside = [], [by_core]
        at = span(t, feats)
        with scope("byz"):
            for c in range(2):
                by_z[c].wait_recv()
                block = x.at[some(1 - h, c), at]
                across.append(go(4 + c, block, block, x_peer))
                inside.append(go(6 + c, block, block, core_peer))
        with scope("byx"):
            by_x.wait_recv()
        block = x.at[mine, span(t_x, feats)]
        inside.append(go(8, block, block, core_peer))
        return across, inside

    def gather_pass(state, relayed):
        go, core_peer, x = state[0], state[5], state[6]
        across, inside = relayed
        with scope("across"):
            for c in range(2):
                across[c].wait_recv()
                block = x.at[some(1 - h, c), span(t_x, feats)]
                inside.append(go(9 + c, block, block, core_peer))

    def gather_end(relayed):
        with scope("inside"):
            for copy in relayed[1]:
                copy.wait_recv()

    def norm(x, gain, out):
        step = 32

        def one(i, carry):
            at = pl.ds(pl.multiple_of(i * step, step), step)
            wide = x[at, :].astype(jnp.float32)
            scale = lax.rsqrt(jnp.mean(wide * wide, axis=-1, keepdims=True) + epsilon)
            out[at, :] = (wide * scale * gain[...]).astype(jnp.bfloat16)
            return carry

        lax.fori_loop(0, x.shape[0] // step, one, 0)

    def scatter(k, acts, weight, s, r1, keep, r2, s3, r3, base, out, hooks):
        core_peer, x_peer = (f, t_core), (f, t_x)

        def project(block):
            at = span(block, feats)
            s[:, at] = jnp.dot(acts[...], weight[:, at], preferred_element_type=jnp.float32).astype(jnp.bfloat16)
            return s.at[:, at]

        a = send(project(t_xc), r1.at[0], rs_send.at[k, 0], rs_recv.at[k, 0], core_peer)
        b = send(project(t_core), r1.at[1], rs_send.at[k, 1], rs_recv.at[k, 1], core_peer)
        project(t_x)
        project(t)
        with scope("rs_a"):
            a.wait_recv()
        at = span(t_x, feats)
        for i, block in ((0, theirs), (1, mine)):
            keep[0, block, :] = (s[block, at].astype(jnp.float32) + r1[0, block, :].astype(jnp.float32)).astype(jnp.bfloat16)
            copy = send(keep.at[0, block], r2.at[block], rs_send.at[k, 2 + i], rs_recv.at[k, 2 + i], x_peer)
            if i == 0:
                c0 = copy
        c1 = copy
        hooks[0]()
        with scope("rs_c0"):
            b.wait_recv()
            c0.wait_recv()

        def total(where):
            return (
                s[where, span(t, feats)].astype(jnp.float32)
                + r1[1, where, :].astype(jnp.float32)
                + r2[where, :].astype(jnp.float32)
            )

        s3[...] = total(theirs).astype(jnp.bfloat16)
        e = send(s3, r3, rs_send.at[k, 4], rs_recv.at[k, 4], (fz[1], t))
        hooks[1]()
        with scope("rs_c1"):
            c1.wait_recv()
        part = total(mine)
        hooks[2]()
        with scope("rs_e"):
            e.wait_recv()
        out[...] = (base[...].astype(jnp.float32) + (part + r3[...].astype(jnp.float32))).astype(jnp.bfloat16)

    def finish(p, acts):
        x_peer, z_peer = (f, t_x), (fz[1], t)
        wide = feats // PARTS
        low, high = pl.ds(0, wide // 2), pl.ds(wide // 2, wide // 2)
        keep, r2, s3, r3 = k2.at[p], x2r.at[p], zs2.at[p], z2r.at[p]

        def project_pair(i, block, where):
            at = span(block, wide)
            keep[i, where, :] = (
                jnp.dot(acts[where, :], wdn[p, core, :, at], preferred_element_type=jnp.float32)
                + jnp.dot(hidp[where, :], wdn[p, 1 - core, :, at], preferred_element_type=jnp.float32)
            ).astype(jnp.bfloat16)

        def go(i, src, dst, peer):
            return send(src, dst, fin_send.at[p, i], fin_recv.at[p, i], peer)

        waits = {}

        def cross():
            project_pair(0, t_x, theirs)
            waits["d"] = go(3, keep.at[0, theirs, high], r3.at[0, :, high], z_peer)
            waits["c"] = go(2, keep.at[0, theirs, low], r2.at[theirs, low], x_peer)
            project_pair(1, t, theirs)
            waits["e"] = go(4, keep.at[1, theirs, high], r3.at[1, :, high], z_peer)
            project_pair(0, t_x, mine)
            waits["m"] = go(7, keep.at[0, mine, low], r2.at[mine, low], x_peer)
            project_pair(1, t, mine)

        def turn():
            with scope(f"fin_d{p}"):
                waits["d"].wait_recv()
            s3[:, high] = (
                keep[0, mine, high].astype(jnp.float32) + r3[0, :, high].astype(jnp.float32)
            ).astype(jnp.bfloat16)
            waits["g"] = go(5, s3.at[:, high], r2.at[pl.ds(0, rows), high], x_peer)
            with scope(f"fin_c{p}"):
                waits["c"].wait_recv()
            s3[:, low] = (
                keep[1, theirs, low].astype(jnp.float32) + r2[theirs, low].astype(jnp.float32)
            ).astype(jnp.bfloat16)
            waits["l"] = go(6, s3.at[:, low], r3.at[0, :, low], z_peer)

        def end():
            with scope(f"fin_g{p}"):
                waits["e"].wait_recv()
                waits["g"].wait_recv()
            left, right = pl.ds(p * part_cols, part_cols), pl.ds(cols + p * part_cols, part_cols)
            result[:, right] = (
                after[:, right].astype(jnp.float32)
                + (keep[1, mine, high].astype(jnp.float32) + r3[1, :, high].astype(jnp.float32))
                + r2[pl.ds(0, rows), high].astype(jnp.float32)
            ).astype(jnp.bfloat16)
            with scope(f"fin_l{p}"):
                waits["m"].wait_recv()
                waits["l"].wait_recv()
            result[:, left] = (
                after[:, left].astype(jnp.float32)
                + (keep[1, mine, low].astype(jnp.float32) + r2[mine, low].astype(jnp.float32))
                + r3[0, :, low].astype(jnp.float32)
            ).astype(jnp.bfloat16)

        return cross, turn, end

    def forwards(*pairs):
        def go():
            for group, d in pairs:
                with scope(f"fw{group}{d}"):
                    forward(group, d)

        return go

    nothing = forwards()
    for load in loads[:1]:
        load.wait()
    state = gather_start(0, tok, x1)
    for load in loads[1:]:
        load.wait()
    y_own(0, 1)

    for group in range(4):
        near(group)
        far(group)

    @pl.when(inner)
    def _():
        for group in range(2):
            z_sends[group, 2].start()
            z_sends[group, 3].start()

    y_own(2, 3)
    y_own(5, role=outer)
    core_own()
    if fill:
        for w in (wgate, wup):
            w[pl.ds(half_ff, fill), :] = jnp.zeros((fill, model), jnp.bfloat16)
        for p in range(PARTS):
            for i in range(2):
                wdn[p, i, pl.ds(half_ff, fill), :] = jnp.zeros((fill, wdn.shape[3]), jnp.bfloat16)
    relayed = gather_relay(state)
    forwards((0, 1), (0, 2), (0, 3), (1, 1), (1, 2))()
    y_own(6, 7, role=outer)
    forwards((1, 3))()
    gather_pass(state, relayed)
    forwards((2, 1))()
    gather_end(relayed)
    forwards((2, 2))()
    with scope("norm1"):
        norm(x1, gain1, nb)
    forwards((2, 3))()
    y_own(4)
    near(4)
    far(4)

    @pl.when(inner)
    def _():
        near(5, 6, 7)


    with scope("arrive01"):
        arrive(0)
        arrive(1)
    both = jnp.dot(nb[...], win[...], preferred_element_type=jnp.float32)
    branch_in, branch_gate = both[:, :LANES], both[:, LANES:]
    row = lax.broadcasted_iota(jnp.int32, branch_in.shape, 0)
    pos = jnp.where(row >= rows, row - rows, row)

    def shifted(values, by, fill):
        return jnp.where(pos >= by, pltpu.roll(values, by, 0), fill)

    tap_count = taps.shape[0]
    my = span(h, LANES)
    conv = branch_in * taps[tap_count - 1 :, my]
    for j in range(tap_count - 1):
        conv = conv + shifted(branch_in, tap_count - 1 - j, 0.0) * taps[j : j + 1, my]
    conv = conv.astype(jnp.bfloat16)
    gate_x = jax.nn.sigmoid(jnp.dot(conv, gxb[h], preferred_element_type=jnp.float32))
    gate_a = jax.nn.sigmoid(jnp.dot(conv, gab[h], preferred_element_type=jnp.float32))
    log_decay = -gate_power * gate_a * forget[:, my]
    decay = jnp.exp(log_decay)
    scale = jnp.sqrt(-jnp.tanh(log_decay) * (1.0 + decay * decay))
    scale = jnp.where(pos == 0, 1.0, scale)
    run = conv.astype(jnp.float32) * gate_x * scale
    by = 1
    while by < rows:
        run = decay * shifted(run, by, 0.0) + run
        decay = decay * shifted(decay, by, 1.0)
        by *= 2
    mix[...] = (run * jax.nn.gelu(branch_gate)).astype(jnp.bfloat16)
    y_own(5, 6, 7, role=inner)
    forwards((3, 1))()
    with scope("arrive2"):
        arrive(2)

    def refill():
        @pl.when(outer)
        def _():
            near(5, 6, 7)

        far(5)
        forwards((4, 1))()

    scatter(0, mix, wout, s1, s1r, k1, x1r, zs1, z1r, tok, after, (forwards((3, 2)), refill, forwards((3, 3))))
    state = gather_start(1, after, x2)
    far(6, 7)

    forwards((4, 2), (5, 1), (6, 1), (7, 1))()
    relayed = gather_relay(state)
    forwards((4, 3))()
    gather_pass(state, relayed)
    forwards((5, 2))()
    gather_end(relayed)
    with scope("norm2"):
        norm(x2, gain2, nb)
    forwards((5, 3))()
    with scope("arrive34"):
        arrive(3)
        arrive(4)
    last = (((1,), (1,)), ((), ()))

    with scope("ffn"):
        gate_val = lax.dot_general(nb[...], wgate[...], last, preferred_element_type=jnp.float32)
        up_val = lax.dot_general(nb[...], wup[...], last, preferred_element_type=jnp.float32)
        hid[...] = (jax.nn.silu(gate_val) * up_val).astype(jnp.bfloat16)
    hid_copy = send(hid, hidp, core_send.at[3, 0], core_recv.at[3, 0], (f, t_core))
    forwards((6, 2), (7, 2), (6, 3), (7, 3))()
    with scope("arrive5"):
        hid_copy.wait_recv()
        arrive(5)
    sent = len(started)
    first = finish(0, hid)
    first[0]()
    with scope("arrive6"):
        arrive(6)
        arrive(7)
    second = finish(1, hid)
    second[0]()
    first[1]()
    second[1]()
    for copy in started[:sent]:
        copy.wait_send()
    for other, copy in core_copies:
        pl.when(other)(copy.wait_send)

    @pl.when(inner)
    def _():
        for group in groups:
            z_sends[group, 2].wait_send()
            relays[group].wait_send()

    first[2]()
    second[2]()
    with scope("drain"):
        for copy in started[sent:]:
            copy.wait_send()


def on_device_paired(
    tokens, mix_gain, in_x_w, in_gate_w, conv_taps, gate_x_blocks, gate_a_blocks, forget_rate,
    out_w, ffn_gain, ffn_gate_w, ffn_up_w, ffn_down_w,
):
    rows, feats = tokens.shape
    model = mix_gain.shape[0]
    both = 2 * rows
    share = feats // PARTS
    wide = -(-ffn_down_w.shape[0] // (2 * LANES)) * LANES
    bf, dma = jnp.bfloat16, pltpu.SemaphoreType.DMA
    exchange = [
        pltpu.VMEM((both, model), bf),
        pltpu.VMEM((2, both, feats), bf),
        pltpu.VMEM((2, both, feats), bf),
        pltpu.VMEM((both, feats), bf),
    ]
    vmem = pl.BlockSpec(memory_space=pltpu.VMEM)
    operands = (
        tokens, mix_gain.reshape(1, model), in_x_w, in_gate_w, conv_taps, gate_x_blocks, gate_a_blocks,
        forget_rate.reshape(1, -1), out_w, ffn_gain.reshape(1, model), ffn_gate_w.T, ffn_up_w.T, ffn_down_w,
    )
    return pl.pallas_call(
        kernel,
        out_shape=jax.ShapeDtypeStruct((rows, feats), bf),
        in_specs=[pl.BlockSpec(memory_space=pltpu.HBM)] * 13,
        out_specs=vmem,
        scratch_shapes=[
            *[pltpu.VMEM(operand.shape, operand.dtype) for operand in operands],
            dma((13,)),
            pltpu.VMEM((both, model), bf),
            pltpu.VMEM((both, model), bf),
            pltpu.VMEM((model, 2 * LANES), bf),
            pltpu.VMEM((LANES, model), bf),
            pltpu.VMEM((wide, model), bf),
            pltpu.VMEM((wide, model), bf),
            pltpu.VMEM((PARTS, 2, wide, model // PARTS), bf),
            pltpu.VMEM((both, wide), bf),
            *exchange,
            pltpu.VMEM((rows, feats), bf),
            pltpu.VMEM((rows, feats), bf),
            pltpu.VMEM((rows, feats), bf),
            pltpu.VMEM((both, LANES), bf),
            pltpu.VMEM((both, model), bf),
            pltpu.VMEM((both, wide), bf),
            pltpu.VMEM((PARTS, 2, both, share), bf),
            pltpu.VMEM((PARTS, both, share), bf),
            pltpu.VMEM((PARTS, rows, share), bf),
            pltpu.VMEM((PARTS, 2, rows, share), bf),
            dma((8, 4)), dma((8, 3)), dma((8, 4)), dma((8, 4)), dma((8,)),
            dma((2, 11)), dma((2, 11)), dma((1, 5)), dma((1, 5)), dma((PARTS, 8)), dma((PARTS, 8)),
            dma((3, 2, 2)), dma((4, 4)), dma((4, 2)),
        ],
        compiler_params=pltpu.CompilerParams(
            collective_id=0, has_side_effects=True, vmem_limit_bytes=48 * 1024 * 1024
        ),
    )(*[pltpu.with_memory_space_constraint(operand, pltpu.HBM) for operand in operands])


def solution(mesh):
    def body(*args):
        if paired(mesh, *args):
            return on_device_paired(*args)
        return on_device(*args)

    placed = (
        P("fs", "tp"),
        P(),
        P("fs", "tp"),
        P("fs", "tp"),
        P(None, "tp"),
        P("tp", None, None),
        P("tp", None, None),
        P("tp"),
        P("tp", "fs"),
        P(),
        P("fs", "tp"),
        P("fs", "tp"),
        P("tp", "fs"),
    )
    return jax.shard_map(
        body, mesh=mesh, in_specs=placed, out_specs=P("fs", "tp"), check_vma=False
    )
```

```python
import functools

import jax
import jax.numpy as jnp
from jax import lax
from jax.experimental import pallas as pl
from jax.experimental.pallas import tpu as pltpu
from jax.sharding import PartitionSpec as P

LANES = 128

epsilon = 1e-06
gate_power = 8.0


def rms_norm(values, gain):
    wide = values.astype(jnp.float32)
    mean_square = jnp.mean(wide * wide, axis=-1, keepdims=True)
    return (wide * lax.rsqrt(mean_square + epsilon) * gain).astype(jnp.bfloat16)


def full_rows(shard):
    return lax.all_gather(shard, "tp", axis=1, tiled=True)


def pair_folder(left_rows, pieces):
    return (
        jnp.dot(left_rows, pieces[0], preferred_element_type=jnp.float32),
        jnp.dot(left_rows, pieces[1], preferred_element_type=jnp.float32),
    )


def project_out(acts, weight):
    partial_terms = jnp.dot(
        acts, lax.all_gather(weight, "fs", axis=1, tiled=True), preferred_element_type=jnp.float32
    )
    return lax.psum_scatter(
        partial_terms.astype(jnp.bfloat16), "tp", scatter_dimension=1, tiled=True
    ).astype(jnp.float32)


def combine(earlier, later):
    return (earlier[0] * later[0], later[0] * earlier[1] + later[1])


def on_device(
    tokens,
    mix_gain,
    in_x_w,
    in_gate_w,
    conv_taps,
    gate_x_blocks,
    gate_a_blocks,
    forget_rate,
    out_w,
    ffn_gain,
    ffn_gate_w,
    ffn_up_w,
    ffn_down_w,
):
    normed = rms_norm(full_rows(tokens), mix_gain)
    length = normed.shape[0]
    chan_width = in_x_w.shape[1]
    branch_in, branch_gate = pair_folder(
        normed,
        (
            lax.all_gather(in_x_w, "fs", axis=0, tiled=True),
            lax.all_gather(in_gate_w, "fs", axis=0, tiled=True),
        ),
    )
    tap_count = conv_taps.shape[0]
    padded = jnp.pad(branch_in, ((tap_count - 1, 0), (0, 0)))
    conv_sum = padded[0:length] * conv_taps[0]
    for index in range(1, tap_count):
        conv_sum = conv_sum + padded[index : index + length] * conv_taps[index]
    conv_out = conv_sum.astype(jnp.bfloat16)
    blocks = gate_x_blocks.shape[0]
    block_dim = gate_x_blocks.shape[1]
    grouped = conv_out.reshape(length, blocks, block_dim)
    gate_x = jax.nn.sigmoid(
        jnp.einsum(
            "tbi,bij->tbj", grouped, gate_x_blocks, preferred_element_type=jnp.float32
        ).reshape(length, chan_width)
    )
    gate_a = jax.nn.sigmoid(
        jnp.einsum(
            "tbi,bij->tbj", grouped, gate_a_blocks, preferred_element_type=jnp.float32
        ).reshape(length, chan_width)
    )
    log_decay = -gate_power * gate_a * forget_rate
    decay = jnp.exp(log_decay)
    scale = jnp.sqrt(-jnp.expm1(2.0 * log_decay))
    scale = jnp.where((jnp.arange(length) == 0)[:, None], 1.0, scale)
    driven = conv_out.astype(jnp.float32) * gate_x * scale
    _, state = lax.associative_scan(combine, (decay, driven), axis=0)
    mixer_out = (state * jax.nn.gelu(branch_gate)).astype(jnp.bfloat16)
    after_mix = (tokens.astype(jnp.float32) + project_out(mixer_out, out_w)).astype(jnp.bfloat16)
    normed_ffn = rms_norm(full_rows(after_mix), ffn_gain)
    gate_val, up_val = pair_folder(
        normed_ffn,
        (
            lax.all_gather(ffn_gate_w, "fs", axis=0, tiled=True),
            lax.all_gather(ffn_up_w, "fs", axis=0, tiled=True),
        ),
    )
    hidden = (jax.nn.silu(gate_val) * up_val).astype(jnp.bfloat16)
    return (after_mix.astype(jnp.float32) + project_out(hidden, ffn_down_w)).astype(jnp.bfloat16)


def paired(mesh, tokens, mix_gain, in_x_w, in_gate_w, conv_taps, gate_x_blocks, *rest):
    ffn_down_w = rest[-1]
    return (
        mesh.shape["fs"] == 8
        and mesh.shape["tp"] == 4
        and gate_x_blocks.shape == (2, LANES, LANES)
        and tokens.shape[0] % 32 == 0
        and tokens.shape[1] == 4 * LANES
        and ffn_down_w.shape[1] == 2 * LANES
        and ffn_down_w.shape[0] % 32 == 0
    )


PARTS = 2


def kernel(
    h_tok, h_gain1, h_x, h_g, h_taps, h_gxb, h_gab, h_forget, h_out, h_gain2, h_gate, h_up, h_dn,
    result,
    tok, gain1, w_x, w_g, taps, gxb, gab, forget, w_out, gain2, w_gate, w_up, w_dn, load_sem,
    x1, nb, win, wout, wgate, wup, wdn, hidp, s1, s1r, k1, x1r, zs1, z1r, after, mix, x2, hid,
    k2, x2r, zs2, z2r,
    send_z, recv_z, send_y, recv_y, own_sem, ag_send, ag_recv, rs_send, rs_recv, fin_send, fin_recv,
    cross_recv, core_send, core_recv,
):
    f, t = lax.axis_index("fs"), lax.axis_index("tp")
    z, y = f // 2, f % 2
    h = z % 2
    outer = (z == 0) | (z == 3)
    inner = (z == 1) | (z == 2)
    rows, feats = tok.shape
    near_z = z + 1 - 2 * h
    far_outer = 3 * (1 - z // 2)
    far_inner = 2 - z // 2
    sources = (z, near_z, far_outer, far_inner)
    fz = tuple(zz * 2 + y for zz in sources)
    fy = z * 2 + 1 - y
    t_core = t + 1 - 2 * (t % 2)
    t_x = (t + 2) % 4
    t_xc = (t_core + 2) % 4
    model = x1.shape[1]
    scope = jax.named_scope

    held = (tok, w_x, w_g, w_out, w_gate, w_up, w_dn, gain1, taps, gxb, gab, forget, gain2)
    given = (h_tok, h_x, h_g, h_out, h_gate, h_up, h_dn, h_gain1, h_taps, h_gxb, h_gab, h_forget, h_gain2)
    loads = [pltpu.make_async_copy(src, dst, load_sem.at[i]) for i, (src, dst) in enumerate(zip(given, held))]
    for load in loads:
        load.start()

    barrier = pltpu.get_barrier_semaphore()
    peers = [(fz[1], t), (fz[3], t), (fy, t), (fy, t_core), (f, t_core), (f, t_x)]

    def greet(peer):
        pl.semaphore_signal(barrier, inc=1, device_id=peer, device_id_type=pl.DeviceIdType.MESH)

    for peer in peers:
        greet(peer)

    @pl.when(inner)
    def _():
        greet((fz[2], t))

    with scope("barrier"):
        pl.semaphore_wait(barrier, len(peers) + jnp.where(inner, 1, 0))

    started = []

    def describe(src, dst, s_sem, r_sem, peer):
        return pltpu.make_async_remote_copy(
            src_ref=src, dst_ref=dst, send_sem=s_sem, recv_sem=r_sem,
            device_id=peer, device_id_type=pl.DeviceIdType.MESH,
        )

    def send(src, dst, s_sem, r_sem, peer):
        copy = describe(src, dst, s_sem, r_sem, peer)
        copy.start()
        started.append(copy)
        return copy

    def span(index, width):
        return pl.ds(pl.multiple_of(index * width, width), width)

    depth = w_x.shape[0]
    cols = w_out.shape[1]
    part_cols = cols // PARTS
    half_ff = w_dn.shape[0] // 2
    fill = wgate.shape[0] - half_ff
    last_group = 5 + PARTS
    quarter = half_ff // 2
    core = t % 2

    def piece(group, half, stored=False):
        if group < 2:
            return ((h_x, h_g) if stored else (w_x, w_g))[group].at[:, span(half, LANES)]
        if group == 2:
            return (h_out if stored else w_out).at[span(half, LANES), :]
        if group < 5:
            return ((h_gate, h_up) if stored else (w_gate, w_up))[group - 3].at[span(half, half_ff), :]
        down = h_dn if stored else w_dn
        if group == 5:
            return down.at[span(half, half_ff), pl.ds(0, part_cols)]
        return down.at[span(2 * half + group - 6, quarter), pl.ds(part_cols, part_cols)]

    def place(group, source):
        if group < 2:
            return win.at[span(source, depth), pl.ds(group * LANES, LANES)]
        if group == 2:
            return wout.at[:, span(source, cols)]
        if group < 5:
            return (wgate, wup)[group - 3].at[pl.ds(0, half_ff), span(source, cols)]
        if group == 5:
            return wdn.at[0, core, pl.ds(0, half_ff), span(source, part_cols)]
        return wdn.at[1, core, pl.ds((group - 6) * quarter, quarter), span(source, part_cols)]

    groups = range(last_group + 1)
    own_copies = {}
    for group in groups:
        own_copies[group] = pltpu.make_async_copy(piece(group, h, True), place(group, f), own_sem.at[group])
        own_copies[group].start()

    slot = jnp.where(outer, 2, 3)
    z_sends = {}
    for group in groups:
        for way, peer in ((1, fz[1]), (2, fz[2]), (3, fz[3])):
            half = (1 - h, far_outer % 2, far_inner % 2)[way - 1]
            at = 1 if way == 1 else slot
            z_sends[group, way] = describe(
                piece(group, half), place(group, f), send_z.at[group, way - 1], recv_z.at[group, at - 1], (peer, t)
            )
            if way != 2:
                started.append(z_sends[group, way])
    y_copies, relays = {}, {}

    after_relay = {
        0: ((2, 2), (2, 3)), 2: ((3, 2), (3, 3)), 3: ((4, 2), (4, 3)), 4: ((5, 2), (5, 3)), 5: ((6, 2), (7, 2)), 7: ((6, 3), (7, 3)),
    }

    def near(*names):
        for group in names:
            z_sends[group, 1].start()

    def far(*names):
        @pl.when(outer)
        def _():
            for group in names:
                z_sends[group, 3].start()

    core_copies = []

    def send_y_piece(group, d, src, dst, source_z):
        if group < 5:
            return describe(src, dst, send_y.at[group, d], recv_y.at[group, d], (fy, t))
        arrived = cross_recv.at[group - 5, core, source_z // 2]
        return describe(src, dst, send_y.at[group, d], arrived, (fy, t - core + source_z % 2))

    def pass_to_core(group, d, src, dst, source_z):
        if group >= 5:
            copy = describe(
                src, dst, core_send.at[group - 5, d], core_recv.at[group - 5, source_z // 2], (f, t_core)
            )
            other = source_z % 2 != core
            core_copies.append((other, copy))
            pl.when(other)(copy.start)

    for group in groups:
        y_copies[group, 0] = send_y_piece(group, 0, piece(group, h), place(group, f), z)
        started.append(y_copies[group, 0])

    def y_own(*names, role=None):
        def go():
            for group in names:
                y_copies[group, 0].start()

        go() if role is None else pl.when(role)(go)

    def core_own():
        for group in groups[5:]:
            pass_to_core(group, 0, piece(group, h), place(group, f), z)

    def pick(when_inner, when_outer):
        return jnp.where(inner, when_inner, when_outer)

    early = (pick(1, 3), pick(2, 1), pick(3, 2)), (pick(fz[1], fz[3]), pick(fz[2], fz[1]), pick(fz[3], fz[2]))
    middle = (1, 3, 2), (fz[1], fz[3], fz[2])
    late = (1, pick(2, 3), pick(3, 2)), (fz[1], pick(fz[2], fz[3]), pick(fz[3], fz[2]))

    def forward(group, d):
        arrival, arrival_fz = early if group < 3 else middle if group < 5 else late
        block = place(group, arrival_fz[d - 1])
        describe(
            block, block, send_z.at[group, 0], recv_z.at[group, arrival[d - 1] - 1], (fz[1], t)
        ).wait_recv()
        y_copies[group, d] = send_y_piece(group, d, block, block, arrival_fz[d - 1] // 2)
        y_copies[group, d].start()
        started.append(y_copies[group, d])
        pass_to_core(group, d, block, block, arrival_fz[d - 1] // 2)
        if d == 1:
            relays[group] = describe(block, block, send_z.at[group, 3], recv_z.at[group, 1], (fz[2], t))

            @pl.when(inner)
            def _():
                relays[group].start()
                for key in after_relay.get(group, ()):
                    z_sends[key].start()

    def arrive(group):
        own_copies[group].wait()
        if group < 5:
            for d in range(4):
                y_copies[group, d].wait_recv()
            return
        block = place(group, f)
        ready = [cross_recv.at[group - 5, i, j] for i in range(2) for j in range(2)]
        for semaphore in ready + [core_recv.at[group - 5, j] for j in range(2)]:
            describe(block, block, send_y.at[group, 0], semaphore, (fy, t)).wait_recv()

    mine, theirs = span(h, rows), span(1 - h, rows)
    cut = rows // 2

    def some(block, c):
        return pl.ds(pl.multiple_of(block * rows + c * cut, cut), cut)

    def gather_start(k, own, x):
        x_peer, core_peer = (f, t_x), (f, t_core)

        def go(i, src, dst, peer):
            return send(src, dst, ag_send.at[k, i], ag_recv.at[k, i], peer)

        at = span(t, feats)
        by_z = [go(c, own.at[pl.ds(c * cut, cut), :], x.at[some(h, c), at], (fz[1], t)) for c in range(2)]
        by_x = go(2, own, x.at[mine, at], x_peer)
        by_core = go(3, own, x.at[mine, at], core_peer)
        x[mine, at] = own[...]
        return go, by_z, by_x, by_core, x_peer, core_peer, x

    def gather_relay(state):
        go, by_z, by_x, by_core, x_peer, core_peer, x = state
        across, inside = [], [by_core]
        at = span(t, feats)
        with scope("byz"):
            for c in range(2):
                by_z[c].wait_recv()
                block = x.at[some(1 - h, c), at]
                across.append(go(4 + c, block, block, x_peer))
                inside.append(go(6 + c, block, block, core_peer))
        with scope("byx"):
            by_x.wait_recv()
        block = x.at[mine, span(t_x, feats)]
        inside.append(go(8, block, block, core_peer))
        return across, inside

    def gather_pass(state, relayed):
        go, core_peer, x = state[0], state[5], state[6]
        across, inside = relayed
        with scope("across"):
            for c in range(2):
                across[c].wait_recv()
                block = x.at[some(1 - h, c), span(t_x, feats)]
                inside.append(go(9 + c, block, block, core_peer))

    def gather_end(relayed):
        with scope("inside"):
            for copy in relayed[1]:
                copy.wait_recv()

    def norm(x, gain, out):
        step = 32

        def one(i, carry):
            at = pl.ds(pl.multiple_of(i * step, step), step)
            wide = x[at, :].astype(jnp.float32)
            scale = lax.rsqrt(jnp.mean(wide * wide, axis=-1, keepdims=True) + epsilon)
            out[at, :] = (wide * scale * gain[...]).astype(jnp.bfloat16)
            return carry

        lax.fori_loop(0, x.shape[0] // step, one, 0)

    def scatter(k, acts, weight, s, r1, keep, r2, s3, r3, base, out, hooks):
        core_peer, x_peer = (f, t_core), (f, t_x)

        def project(block):
            at = span(block, feats)
            s[:, at] = jnp.dot(acts[...], weight[:, at], preferred_element_type=jnp.float32).astype(jnp.bfloat16)
            return s.at[:, at]

        a = send(project(t_xc), r1.at[0], rs_send.at[k, 0], rs_recv.at[k, 0], core_peer)
        b = send(project(t_core), r1.at[1], rs_send.at[k, 1], rs_recv.at[k, 1], core_peer)
        project(t_x)
        project(t)
        with scope("rs_a"):
            a.wait_recv()
        at = span(t_x, feats)
        for i, block in ((0, theirs), (1, mine)):
            keep[0, block, :] = (s[block, at].astype(jnp.float32) + r1[0, block, :].astype(jnp.float32)).astype(jnp.bfloat16)
            copy = send(keep.at[0, block], r2.at[block], rs_send.at[k, 2 + i], rs_recv.at[k, 2 + i], x_peer)
            if i == 0:
                c0 = copy
        c1 = copy
        hooks[0]()
        with scope("rs_c0"):
            b.wait_recv()
            c0.wait_recv()

        def total(where):
            return (
                s[where, span(t, feats)].astype(jnp.float32)
                + r1[1, where, :].astype(jnp.float32)
                + r2[where, :].astype(jnp.float32)
            )

        s3[...] = total(theirs).astype(jnp.bfloat16)
        e = send(s3, r3, rs_send.at[k, 4], rs_recv.at[k, 4], (fz[1], t))
        hooks[1]()
        with scope("rs_c1"):
            c1.wait_recv()
        part = total(mine)
        hooks[2]()
        with scope("rs_e"):
            e.wait_recv()
        out[...] = (base[...].astype(jnp.float32) + (part + r3[...].astype(jnp.float32))).astype(jnp.bfloat16)

    def finish(p, acts):
        x_peer, z_peer = (f, t_x), (fz[1], t)
        wide = feats // PARTS
        low, high = pl.ds(0, wide // 2), pl.ds(wide // 2, wide // 2)
        keep, r2, s3, r3 = k2.at[p], x2r.at[p], zs2.at[p], z2r.at[p]

        def project_pair(i, block, where):
            at = span(block, wide)
            keep[i, where, :] = (
                jnp.dot(acts[where, :], wdn[p, core, :, at], preferred_element_type=jnp.float32)
                + jnp.dot(hidp[where, :], wdn[p, 1 - core, :, at], preferred_element_type=jnp.float32)
            ).astype(jnp.bfloat16)

        def go(i, src, dst, peer):
            return send(src, dst, fin_send.at[p, i], fin_recv.at[p, i], peer)

        waits = {}

        def cross():
            project_pair(0, t_x, theirs)
            waits["d"] = go(3, keep.at[0, theirs, high], r3.at[0, :, high], z_peer)
            waits["c"] = go(2, keep.at[0, theirs, low], r2.at[theirs, low], x_peer)
            project_pair(1, t, theirs)
            waits["e"] = go(4, keep.at[1, theirs, high], r3.at[1, :, high], z_peer)
            project_pair(0, t_x, mine)
            waits["m"] = go(7, keep.at[0, mine, low], r2.at[mine, low], x_peer)
            project_pair(1, t, mine)

        def turn():
            with scope(f"fin_d{p}"):
                waits["d"].wait_recv()
            s3[:, high] = (
                keep[0, mine, high].astype(jnp.float32) + r3[0, :, high].astype(jnp.float32)
            ).astype(jnp.bfloat16)
            waits["g"] = go(5, s3.at[:, high], r2.at[pl.ds(0, rows), high], x_peer)
            with scope(f"fin_c{p}"):
                waits["c"].wait_recv()
            s3[:, low] = (
                keep[1, theirs, low].astype(jnp.float32) + r2[theirs, low].astype(jnp.float32)
            ).astype(jnp.bfloat16)
            waits["l"] = go(6, s3.at[:, low], r3.at[0, :, low], z_peer)

        def end():
            with scope(f"fin_g{p}"):
                waits["e"].wait_recv()
                waits["g"].wait_recv()
            left, right = pl.ds(p * part_cols, part_cols), pl.ds(cols + p * part_cols, part_cols)
            result[:, right] = (
                after[:, right].astype(jnp.float32)
                + (keep[1, mine, high].astype(jnp.float32) + r3[1, :, high].astype(jnp.float32))
                + r2[pl.ds(0, rows), high].astype(jnp.float32)
            ).astype(jnp.bfloat16)
            with scope(f"fin_l{p}"):
                waits["m"].wait_recv()
                waits["l"].wait_recv()
            result[:, left] = (
                after[:, left].astype(jnp.float32)
                + (keep[1, mine, low].astype(jnp.float32) + r2[mine, low].astype(jnp.float32))
                + r3[0, :, low].astype(jnp.float32)
            ).astype(jnp.bfloat16)

        return cross, turn, end

    def forwards(*pairs):
        def go():
            for group, d in pairs:
                with scope(f"fw{group}{d}"):
                    forward(group, d)

        return go

    nothing = forwards()
    for load in loads[:1]:
        load.wait()
    state = gather_start(0, tok, x1)
    for load in loads[1:]:
        load.wait()
    y_own(0, 1)

    for group in range(4):
        near(group)
        far(group)

    @pl.when(inner)
    def _():
        for group in range(2):
            z_sends[group, 2].start()
            z_sends[group, 3].start()

    y_own(2, 3)
    y_own(5, role=outer)
    core_own()
    if fill:
        for w in (wgate, wup):
            w[pl.ds(half_ff, fill), :] = jnp.zeros((fill, model), jnp.bfloat16)
        for p in range(PARTS):
            for i in range(2):
                wdn[p, i, pl.ds(half_ff, fill), :] = jnp.zeros((fill, wdn.shape[3]), jnp.bfloat16)
    relayed = gather_relay(state)
    forwards((0, 1), (0, 2), (0, 3), (1, 1), (1, 2))()
    y_own(6, 7, role=outer)
    forwards((1, 3))()
    gather_pass(state, relayed)
    forwards((2, 1))()
    gather_end(relayed)
    forwards((2, 2))()
    with scope("norm1"):
        norm(x1, gain1, nb)
    forwards((2, 3))()
    y_own(4)
    near(4)
    far(4)

    @pl.when(inner)
    def _():
        near(5, 6, 7)


    with scope("arrive01"):
        arrive(0)
        arrive(1)
    both = jnp.dot(nb[...], win[...], preferred_element_type=jnp.float32)
    branch_in, branch_gate = both[:, :LANES], both[:, LANES:]
    row = lax.broadcasted_iota(jnp.int32, branch_in.shape, 0)
    pos = jnp.where(row >= rows, row - rows, row)

    def shifted(values, by, fill):
        return jnp.where(pos >= by, pltpu.roll(values, by, 0), fill)

    tap_count = taps.shape[0]
    my = span(h, LANES)
    conv = branch_in * taps[tap_count - 1 :, my]
    for j in range(tap_count - 1):
        conv = conv + shifted(branch_in, tap_count - 1 - j, 0.0) * taps[j : j + 1, my]
    conv = conv.astype(jnp.bfloat16)
    gate_x = jax.nn.sigmoid(jnp.dot(conv, gxb[h], preferred_element_type=jnp.float32))
    gate_a = jax.nn.sigmoid(jnp.dot(conv, gab[h], preferred_element_type=jnp.float32))
    log_decay = -gate_power * gate_a * forget[:, my]
    decay = jnp.exp(log_decay)
    scale = jnp.sqrt(-jnp.tanh(log_decay) * (1.0 + decay * decay))
    scale = jnp.where(pos == 0, 1.0, scale)
    run = conv.astype(jnp.float32) * gate_x * scale
    by = 1
    while by < rows:
        run = decay * shifted(run, by, 0.0) + run
        decay = decay * shifted(decay, by, 1.0)
        by *= 2
    mix[...] = (run * jax.nn.gelu(branch_gate)).astype(jnp.bfloat16)
    y_own(5, 6, 7, role=inner)
    forwards((3, 1))()
    with scope("arrive2"):
        arrive(2)

    def refill():
        @pl.when(outer)
        def _():
            near(5, 6, 7)

        far(5)
        forwards((4, 1))()

    scatter(0, mix, wout, s1, s1r, k1, x1r, zs1, z1r, tok, after, (forwards((3, 2)), refill, forwards((3, 3))))
    state = gather_start(1, after, x2)
    far(6, 7)

    forwards((4, 2), (5, 1), (6, 1), (7, 1))()
    relayed = gather_relay(state)
    forwards((4, 3))()
    gather_pass(state, relayed)
    forwards((5, 2))()
    gather_end(relayed)
    with scope("norm2"):
        norm(x2, gain2, nb)
    forwards((5, 3))()
    with scope("arrive34"):
        arrive(3)
        arrive(4)
    last = (((1,), (1,)), ((), ()))

    with scope("ffn"):
        gate_val = lax.dot_general(nb[...], wgate[...], last, preferred_element_type=jnp.float32)
        up_val = lax.dot_general(nb[...], wup[...], last, preferred_element_type=jnp.float32)
        hid[...] = (jax.nn.silu(gate_val) * up_val).astype(jnp.bfloat16)
    hid_copy = send(hid, hidp, core_send.at[3, 0], core_recv.at[3, 0], (f, t_core))
    forwards((6, 2), (7, 2), (6, 3), (7, 3))()
    with scope("arrive5"):
        hid_copy.wait_recv()
        arrive(5)
    sent = len(started)
    first = finish(0, hid)
    first[0]()
    with scope("arrive6"):
        arrive(6)
        arrive(7)
    second = finish(1, hid)
    second[0]()
    first[1]()
    second[1]()
    for copy in started[:sent]:
        copy.wait_send()
    for other, copy in core_copies:
        pl.when(other)(copy.wait_send)

    @pl.when(inner)
    def _():
        for group in groups:
            z_sends[group, 2].wait_send()
            relays[group].wait_send()

    first[2]()
    second[2]()
    with scope("drain"):
        for copy in started[sent:]:
            copy.wait_send()


def on_device_paired(
    tokens, mix_gain, in_x_w, in_gate_w, conv_taps, gate_x_blocks, gate_a_blocks, forget_rate,
    out_w, ffn_gain, ffn_gate_w, ffn_up_w, ffn_down_w,
):
    rows, feats = tokens.shape
    model = mix_gain.shape[0]
    both = 2 * rows
    share = feats // PARTS
    wide = -(-ffn_down_w.shape[0] // (2 * LANES)) * LANES
    bf, dma = jnp.bfloat16, pltpu.SemaphoreType.DMA
    exchange = [
        pltpu.VMEM((both, model), bf),
        pltpu.VMEM((2, both, feats), bf),
        pltpu.VMEM((2, both, feats), bf),
        pltpu.VMEM((both, feats), bf),
    ]
    vmem = pl.BlockSpec(memory_space=pltpu.VMEM)
    operands = (
        tokens, mix_gain.reshape(1, model), in_x_w, in_gate_w, conv_taps, gate_x_blocks, gate_a_blocks,
        forget_rate.reshape(1, -1), out_w, ffn_gain.reshape(1, model), ffn_gate_w.T, ffn_up_w.T, ffn_down_w,
    )
    return pl.pallas_call(
        kernel,
        out_shape=jax.ShapeDtypeStruct((rows, feats), bf),
        in_specs=[pl.BlockSpec(memory_space=pltpu.HBM)] * 13,
        out_specs=vmem,
        scratch_shapes=[
            *[pltpu.VMEM(operand.shape, operand.dtype) for operand in operands],
            dma((13,)),
            pltpu.VMEM((both, model), bf),
            pltpu.VMEM((both, model), bf),
            pltpu.VMEM((model, 2 * LANES), bf),
            pltpu.VMEM((LANES, model), bf),
            pltpu.VMEM((wide, model), bf),
            pltpu.VMEM((wide, model), bf),
            pltpu.VMEM((PARTS, 2, wide, model // PARTS), bf),
            pltpu.VMEM((both, wide), bf),
            *exchange,
            pltpu.VMEM((rows, feats), bf),
            pltpu.VMEM((rows, feats), bf),
            pltpu.VMEM((rows, feats), bf),
            pltpu.VMEM((both, LANES), bf),
            pltpu.VMEM((both, model), bf),
            pltpu.VMEM((both, wide), bf),
            pltpu.VMEM((PARTS, 2, both, share), bf),
            pltpu.VMEM((PARTS, both, share), bf),
            pltpu.VMEM((PARTS, rows, share), bf),
            pltpu.VMEM((PARTS, 2, rows, share), bf),
            dma((8, 4)), dma((8, 3)), dma((8, 4)), dma((8, 4)), dma((8,)),
            dma((2, 11)), dma((2, 11)), dma((1, 5)), dma((1, 5)), dma((PARTS, 8)), dma((PARTS, 8)),
            dma((3, 2, 2)), dma((4, 4)), dma((4, 2)),
        ],
        compiler_params=pltpu.CompilerParams(
            collective_id=0, has_side_effects=True, vmem_limit_bytes=48 * 1024 * 1024
        ),
    )(*[pltpu.with_memory_space_constraint(operand, pltpu.HBM) for operand in operands])


def solution(mesh):
    def body(*args):
        if paired(mesh, *args):
            return on_device_paired(*args)
        return on_device(*args)

    placed = (
        P("fs", "tp"),
        P(),
        P("fs", "tp"),
        P("fs", "tp"),
        P(None, "tp"),
        P("tp", None, None),
        P("tp", None, None),
        P("tp"),
        P("tp", "fs"),
        P(),
        P("fs", "tp"),
        P("fs", "tp"),
        P("tp", "fs"),
    )
    return jax.shard_map(
        body, mesh=mesh, in_specs=placed, out_specs=P("fs", "tp"), check_vma=False
    )
```

```python
import functools

import jax
import jax.numpy as jnp
from jax import lax
from jax.experimental import pallas as pl
from jax.experimental.pallas import tpu as pltpu
from jax.sharding import PartitionSpec as P

LANES = 128

epsilon = 1e-06
gate_power = 8.0


def rms_norm(values, gain):
    wide = values.astype(jnp.float32)
    mean_square = jnp.mean(wide * wide, axis=-1, keepdims=True)
    return (wide * lax.rsqrt(mean_square + epsilon) * gain).astype(jnp.bfloat16)


def full_rows(shard):
    return lax.all_gather(shard, "tp", axis=1, tiled=True)


def pair_folder(left_rows, pieces):
    return (
        jnp.dot(left_rows, pieces[0], preferred_element_type=jnp.float32),
        jnp.dot(left_rows, pieces[1], preferred_element_type=jnp.float32),
    )


def project_out(acts, weight):
    partial_terms = jnp.dot(
        acts, lax.all_gather(weight, "fs", axis=1, tiled=True), preferred_element_type=jnp.float32
    )
    return lax.psum_scatter(
        partial_terms.astype(jnp.bfloat16), "tp", scatter_dimension=1, tiled=True
    ).astype(jnp.float32)


def combine(earlier, later):
    return (earlier[0] * later[0], later[0] * earlier[1] + later[1])


def on_device(
    tokens,
    mix_gain,
    in_x_w,
    in_gate_w,
    conv_taps,
    gate_x_blocks,
    gate_a_blocks,
    forget_rate,
    out_w,
    ffn_gain,
    ffn_gate_w,
    ffn_up_w,
    ffn_down_w,
):
    normed = rms_norm(full_rows(tokens), mix_gain)
    length = normed.shape[0]
    chan_width = in_x_w.shape[1]
    branch_in, branch_gate = pair_folder(
        normed,
        (
            lax.all_gather(in_x_w, "fs", axis=0, tiled=True),
            lax.all_gather(in_gate_w, "fs", axis=0, tiled=True),
        ),
    )
    tap_count = conv_taps.shape[0]
    padded = jnp.pad(branch_in, ((tap_count - 1, 0), (0, 0)))
    conv_sum = padded[0:length] * conv_taps[0]
    for index in range(1, tap_count):
        conv_sum = conv_sum + padded[index : index + length] * conv_taps[index]
    conv_out = conv_sum.astype(jnp.bfloat16)
    blocks = gate_x_blocks.shape[0]
    block_dim = gate_x_blocks.shape[1]
    grouped = conv_out.reshape(length, blocks, block_dim)
    gate_x = jax.nn.sigmoid(
        jnp.einsum(
            "tbi,bij->tbj", grouped, gate_x_blocks, preferred_element_type=jnp.float32
        ).reshape(length, chan_width)
    )
    gate_a = jax.nn.sigmoid(
        jnp.einsum(
            "tbi,bij->tbj", grouped, gate_a_blocks, preferred_element_type=jnp.float32
        ).reshape(length, chan_width)
    )
    log_decay = -gate_power * gate_a * forget_rate
    decay = jnp.exp(log_decay)
    scale = jnp.sqrt(-jnp.expm1(2.0 * log_decay))
    scale = jnp.where((jnp.arange(length) == 0)[:, None], 1.0, scale)
    driven = conv_out.astype(jnp.float32) * gate_x * scale
    _, state = lax.associative_scan(combine, (decay, driven), axis=0)
    mixer_out = (state * jax.nn.gelu(branch_gate)).astype(jnp.bfloat16)
    after_mix = (tokens.astype(jnp.float32) + project_out(mixer_out, out_w)).astype(jnp.bfloat16)
    normed_ffn = rms_norm(full_rows(after_mix), ffn_gain)
    gate_val, up_val = pair_folder(
        normed_ffn,
        (
            lax.all_gather(ffn_gate_w, "fs", axis=0, tiled=True),
            lax.all_gather(ffn_up_w, "fs", axis=0, tiled=True),
        ),
    )
    hidden = (jax.nn.silu(gate_val) * up_val).astype(jnp.bfloat16)
    return (after_mix.astype(jnp.float32) + project_out(hidden, ffn_down_w)).astype(jnp.bfloat16)


def paired(mesh, tokens, mix_gain, in_x_w, in_gate_w, conv_taps, gate_x_blocks, *rest):
    ffn_down_w = rest[-1]
    return (
        mesh.shape["fs"] == 8
        and mesh.shape["tp"] == 4
        and gate_x_blocks.shape == (2, LANES, LANES)
        and tokens.shape[0] % 32 == 0
        and tokens.shape[1] == 4 * LANES
        and ffn_down_w.shape[1] == 2 * LANES
        and ffn_down_w.shape[0] % 32 == 0
    )


PARTS = 2


def kernel(
    h_tok, h_gain1, h_x, h_g, h_taps, h_gxb, h_gab, h_forget, h_out, h_gain2, h_gate, h_up, h_dn,
    result,
    tok, gain1, w_x, w_g, taps, gxb, gab, forget, w_out, gain2, w_gate, w_up, w_dn, load_sem,
    x1, nb, win, wout, wgate, wup, wdn, hidp, s1, s1r, k1, x1r, zs1, z1r, after, mix, x2, hid,
    k2, x2r, zs2, z2r,
    send_z, recv_z, send_y, recv_y, own_sem, ag_send, ag_recv, rs_send, rs_recv, fin_send, fin_recv,
    cross_recv, core_send, core_recv,
):
    f, t = lax.axis_index("fs"), lax.axis_index("tp")
    z, y = f // 2, f % 2
    h = z % 2
    outer = (z == 0) | (z == 3)
    inner = (z == 1) | (z == 2)
    rows, feats = tok.shape
    near_z = z + 1 - 2 * h
    far_outer = 3 * (1 - z // 2)
    far_inner = 2 - z // 2
    sources = (z, near_z, far_outer, far_inner)
    fz = tuple(zz * 2 + y for zz in sources)
    fy = z * 2 + 1 - y
    t_core = t + 1 - 2 * (t % 2)
    t_x = (t + 2) % 4
    t_xc = (t_core + 2) % 4
    model = x1.shape[1]
    scope = jax.named_scope

    held = (tok, w_x, w_g, w_out, w_gate, w_up, w_dn, gain1, taps, gxb, gab, forget, gain2)
    given = (h_tok, h_x, h_g, h_out, h_gate, h_up, h_dn, h_gain1, h_taps, h_gxb, h_gab, h_forget, h_gain2)
    loads = [pltpu.make_async_copy(src, dst, load_sem.at[i]) for i, (src, dst) in enumerate(zip(given, held))]
    for load in loads:
        load.start()

    barrier = pltpu.get_barrier_semaphore()
    peers = [(fz[1], t), (fz[3], t), (fy, t), (fy, t_core), (f, t_core), (f, t_x)]

    def greet(peer):
        pl.semaphore_signal(barrier, inc=1, device_id=peer, device_id_type=pl.DeviceIdType.MESH)

    for peer in peers:
        greet(peer)

    @pl.when(inner)
    def _():
        greet((fz[2], t))

    with scope("barrier"):
        pl.semaphore_wait(barrier, len(peers) + jnp.where(inner, 1, 0))

    started = []

    def describe(src, dst, s_sem, r_sem, peer):
        return pltpu.make_async_remote_copy(
            src_ref=src, dst_ref=dst, send_sem=s_sem, recv_sem=r_sem,
            device_id=peer, device_id_type=pl.DeviceIdType.MESH,
        )

    def send(src, dst, s_sem, r_sem, peer):
        copy = describe(src, dst, s_sem, r_sem, peer)
        copy.start()
        started.append(copy)
        return copy

    def span(index, width):
        return pl.ds(pl.multiple_of(index * width, width), width)

    depth = w_x.shape[0]
    cols = w_out.shape[1]
    part_cols = cols // PARTS
    half_ff = w_dn.shape[0] // 2
    fill = wgate.shape[0] - half_ff
    last_group = 5 + PARTS
    quarter = half_ff // 2
    core = t % 2

    def piece(group, half, stored=False):
        if group < 2:
            return ((h_x, h_g) if stored else (w_x, w_g))[group].at[:, span(half, LANES)]
        if group == 2:
            return (h_out if stored else w_out).at[span(half, LANES), :]
        if group < 5:
            return ((h_gate, h_up) if stored else (w_gate, w_up))[group - 3].at[span(half, half_ff), :]
        down = h_dn if stored else w_dn
        if group == 5:
            return down.at[span(half, half_ff), pl.ds(0, part_cols)]
        return down.at[span(2 * half + group - 6, quarter), pl.ds(part_cols, part_cols)]

    def place(group, source):
        if group < 2:
            return win.at[span(source, depth), pl.ds(group * LANES, LANES)]
        if group == 2:
            return wout.at[:, span(source, cols)]
        if group < 5:
            return (wgate, wup)[group - 3].at[pl.ds(0, half_ff), span(source, cols)]
        if group == 5:
            return wdn.at[0, core, pl.ds(0, half_ff), span(source, part_cols)]
        return wdn.at[1, core, pl.ds((group - 6) * quarter, quarter), span(source, part_cols)]

    groups = range(last_group + 1)
    own_copies = {}
    for group in groups:
        own_copies[group] = pltpu.make_async_copy(piece(group, h, True), place(group, f), own_sem.at[group])
        own_copies[group].start()

    slot = jnp.where(outer, 2, 3)
    z_sends = {}
    for group in groups:
        for way, peer in ((1, fz[1]), (2, fz[2]), (3, fz[3])):
            half = (1 - h, far_outer % 2, far_inner % 2)[way - 1]
            at = 1 if way == 1 else slot
            z_sends[group, way] = describe(
                piece(group, half), place(group, f), send_z.at[group, way - 1], recv_z.at[group, at - 1], (peer, t)
            )
            if way != 2:
                started.append(z_sends[group, way])
    y_copies, relays = {}, {}

    after_relay = {
        0: ((2, 2), (2, 3)), 2: ((3, 2), (3, 3)), 3: ((4, 2), (4, 3)), 4: ((5, 2), (5, 3)), 5: ((6, 2), (7, 2)), 7: ((6, 3), (7, 3)),
    }

    def near(*names):
        for group in names:
            z_sends[group, 1].start()

    def far(*names):
        @pl.when(outer)
        def _():
            for group in names:
                z_sends[group, 3].start()

    core_copies = []

    def send_y_piece(group, d, src, dst, source_z):
        if group < 5:
            return describe(src, dst, send_y.at[group, d], recv_y.at[group, d], (fy, t))
        arrived = cross_recv.at[group - 5, core, source_z // 2]
        return describe(src, dst, send_y.at[group, d], arrived, (fy, t - core + source_z % 2))

    def pass_to_core(group, d, src, dst, source_z):
        if group >= 5:
            copy = describe(
                src, dst, core_send.at[group - 5, d], core_recv.at[group - 5, source_z // 2], (f, t_core)
            )
            other = source_z % 2 != core
            core_copies.append((other, copy))
            pl.when(other)(copy.start)

    for group in groups:
        y_copies[group, 0] = send_y_piece(group, 0, piece(group, h), place(group, f), z)
        started.append(y_copies[group, 0])

    def y_own(*names, role=None):
        def go():
            for group in names:
                y_copies[group, 0].start()

        go() if role is None else pl.when(role)(go)

    def core_own():
        for group in groups[5:]:
            pass_to_core(group, 0, piece(group, h), place(group, f), z)

    def pick(when_inner, when_outer):
        return jnp.where(inner, when_inner, when_outer)

    early = (pick(1, 3), pick(2, 1), pick(3, 2)), (pick(fz[1], fz[3]), pick(fz[2], fz[1]), pick(fz[3], fz[2]))
    middle = (1, 3, 2), (fz[1], fz[3], fz[2])
    late = (1, pick(2, 3), pick(3, 2)), (fz[1], pick(fz[2], fz[3]), pick(fz[3], fz[2]))

    def forward(group, d):
        arrival, arrival_fz = early if group < 3 else middle if group < 5 else late
        block = place(group, arrival_fz[d - 1])
        describe(
            block, block, send_z.at[group, 0], recv_z.at[group, arrival[d - 1] - 1], (fz[1], t)
        ).wait_recv()
        y_copies[group, d] = send_y_piece(group, d, block, block, arrival_fz[d - 1] // 2)
        y_copies[group, d].start()
        started.append(y_copies[group, d])
        pass_to_core(group, d, block, block, arrival_fz[d - 1] // 2)
        if d == 1:
            relays[group] = describe(block, block, send_z.at[group, 3], recv_z.at[group, 1], (fz[2], t))

            @pl.when(inner)
            def _():
                relays[group].start()
                for key in after_relay.get(group, ()):
                    z_sends[key].start()

    def arrive(group):
        own_copies[group].wait()
        if group < 5:
            for d in range(4):
                y_copies[group, d].wait_recv()
            return
        block = place(group, f)
        ready = [cross_recv.at[group - 5, i, j] for i in range(2) for j in range(2)]
        for semaphore in ready + [core_recv.at[group - 5, j] for j in range(2)]:
            describe(block, block, send_y.at[group, 0], semaphore, (fy, t)).wait_recv()

    mine, theirs = span(h, rows), span(1 - h, rows)
    cut = rows // 2

    def some(block, c):
        return pl.ds(pl.multiple_of(block * rows + c * cut, cut), cut)

    def gather_start(k, own, x):
        x_peer, core_peer = (f, t_x), (f, t_core)

        def go(i, src, dst, peer):
            return send(src, dst, ag_send.at[k, i], ag_recv.at[k, i], peer)

        at = span(t, feats)
        by_z = [go(c, own.at[pl.ds(c * cut, cut), :], x.at[some(h, c), at], (fz[1], t)) for c in range(2)]
        by_x = go(2, own, x.at[mine, at], x_peer)
        by_core = go(3, own, x.at[mine, at], core_peer)
        x[mine, at] = own[...]
        return go, by_z, by_x, by_core, x_peer, core_peer, x

    def gather_relay(state):
        go, by_z, by_x, by_core, x_peer, core_peer, x = state
        across, inside = [], [by_core]
        at = span(t, feats)
        with scope("byz"):
            for c in range(2):
                by_z[c].wait_recv()
                block = x.at[some(1 - h, c), at]
                across.append(go(4 + c, block, block, x_peer))
                inside.append(go(6 + c, block, block, core_peer))
        with scope("byx"):
            by_x.wait_recv()
        block = x.at[mine, span(t_x, feats)]
        inside.append(go(8, block, block, core_peer))
        return across, inside

    def gather_pass(state, relayed):
        go, core_peer, x = state[0], state[5], state[6]
        across, inside = relayed
        with scope("across"):
            for c in range(2):
                across[c].wait_recv()
                block = x.at[some(1 - h, c), span(t_x, feats)]
                inside.append(go(9 + c, block, block, core_peer))

    def gather_end(relayed):
        with scope("inside"):
            for copy in relayed[1]:
                copy.wait_recv()

    def norm(x, gain, out):
        step = 32

        def one(i, carry):
            at = pl.ds(pl.multiple_of(i * step, step), step)
            wide = x[at, :].astype(jnp.float32)
            scale = lax.rsqrt(jnp.mean(wide * wide, axis=-1, keepdims=True) + epsilon)
            out[at, :] = (wide * scale * gain[...]).astype(jnp.bfloat16)
            return carry

        lax.fori_loop(0, x.shape[0] // step, one, 0)

    def scatter(k, acts, weight, s, r1, keep, r2, s3, r3, base, out, hooks):
        core_peer, x_peer = (f, t_core), (f, t_x)

        def project(block):
            at = span(block, feats)
            s[:, at] = jnp.dot(acts[...], weight[:, at], preferred_element_type=jnp.float32).astype(jnp.bfloat16)
            return s.at[:, at]

        a = send(project(t_xc), r1.at[0], rs_send.at[k, 0], rs_recv.at[k, 0], core_peer)
        b = send(project(t_core), r1.at[1], rs_send.at[k, 1], rs_recv.at[k, 1], core_peer)
        project(t_x)
        project(t)
        with scope("rs_a"):
            a.wait_recv()
        at = span(t_x, feats)
        for i, block in ((0, theirs), (1, mine)):
            keep[0, block, :] = (s[block, at].astype(jnp.float32) + r1[0, block, :].astype(jnp.float32)).astype(jnp.bfloat16)
            copy = send(keep.at[0, block], r2.at[block], rs_send.at[k, 2 + i], rs_recv.at[k, 2 + i], x_peer)
            if i == 0:
                c0 = copy
        c1 = copy
        hooks[0]()
        with scope("rs_c0"):
            b.wait_recv()
            c0.wait_recv()

        def total(where):
            return (
                s[where, span(t, feats)].astype(jnp.float32)
                + r1[1, where, :].astype(jnp.float32)
                + r2[where, :].astype(jnp.float32)
            )

        s3[...] = total(theirs).astype(jnp.bfloat16)
        e = send(s3, r3, rs_send.at[k, 4], rs_recv.at[k, 4], (fz[1], t))
        hooks[1]()
        with scope("rs_c1"):
            c1.wait_recv()
        part = total(mine)
        hooks[2]()
        with scope("rs_e"):
            e.wait_recv()
        out[...] = (base[...].astype(jnp.float32) + (part + r3[...].astype(jnp.float32))).astype(jnp.bfloat16)

    def finish(p, acts):
        x_peer, z_peer = (f, t_x), (fz[1], t)
        wide = feats // PARTS
        low, high = pl.ds(0, wide // 2), pl.ds(wide // 2, wide // 2)
        keep, r2, s3, r3 = k2.at[p], x2r.at[p], zs2.at[p], z2r.at[p]

        def project_pair(i, block, where):
            at = span(block, wide)
            keep[i, where, :] = (
                jnp.dot(acts[where, :], wdn[p, core, :, at], preferred_element_type=jnp.float32)
                + jnp.dot(hidp[where, :], wdn[p, 1 - core, :, at], preferred_element_type=jnp.float32)
            ).astype(jnp.bfloat16)

        def go(i, src, dst, peer):
            return send(src, dst, fin_send.at[p, i], fin_recv.at[p, i], peer)

        waits = {}

        def cross():
            project_pair(0, t_x, theirs)
            waits["d"] = go(3, keep.at[0, theirs, high], r3.at[0, :, high], z_peer)
            waits["c"] = go(2, keep.at[0, theirs, low], r2.at[theirs, low], x_peer)
            project_pair(1, t, theirs)
            waits["e"] = go(4, keep.at[1, theirs, high], r3.at[1, :, high], z_peer)
            project_pair(0, t_x, mine)
            waits["m"] = go(7, keep.at[0, mine, low], r2.at[mine, low], x_peer)
            project_pair(1, t, mine)

        def turn():
            with scope(f"fin_d{p}"):
                waits["d"].wait_recv()
            s3[:, high] = (
                keep[0, mine, high].astype(jnp.float32) + r3[0, :, high].astype(jnp.float32)
            ).astype(jnp.bfloat16)
            waits["g"] = go(5, s3.at[:, high], r2.at[pl.ds(0, rows), high], x_peer)
            with scope(f"fin_c{p}"):
                waits["c"].wait_recv()
            s3[:, low] = (
                keep[1, theirs, low].astype(jnp.float32) + r2[theirs, low].astype(jnp.float32)
            ).astype(jnp.bfloat16)
            waits["l"] = go(6, s3.at[:, low], r3.at[0, :, low], z_peer)

        def end():
            with scope(f"fin_g{p}"):
                waits["e"].wait_recv()
                waits["g"].wait_recv()
            left, right = pl.ds(p * part_cols, part_cols), pl.ds(cols + p * part_cols, part_cols)
            result[:, right] = (
                after[:, right].astype(jnp.float32)
                + (keep[1, mine, high].astype(jnp.float32) + r3[1, :, high].astype(jnp.float32))
                + r2[pl.ds(0, rows), high].astype(jnp.float32)
            ).astype(jnp.bfloat16)
            with scope(f"fin_l{p}"):
                waits["m"].wait_recv()
                waits["l"].wait_recv()
            result[:, left] = (
                after[:, left].astype(jnp.float32)
                + (keep[1, mine, low].astype(jnp.float32) + r2[mine, low].astype(jnp.float32))
                + r3[0, :, low].astype(jnp.float32)
            ).astype(jnp.bfloat16)

        return cross, turn, end

    def forwards(*pairs):
        def go():
            for group, d in pairs:
                with scope(f"fw{group}{d}"):
                    forward(group, d)

        return go

    nothing = forwards()
    for load in loads[:1]:
        load.wait()
    state = gather_start(0, tok, x1)
    for load in loads[1:]:
        load.wait()
    y_own(0, 1)

    for group in range(4):
        near(group)
        far(group)

    @pl.when(inner)
    def _():
        for group in range(2):
            z_sends[group, 2].start()
            z_sends[group, 3].start()

    y_own(2, 3)
    y_own(5, role=outer)
    core_own()
    if fill:
        for w in (wgate, wup):
            w[pl.ds(half_ff, fill), :] = jnp.zeros((fill, model), jnp.bfloat16)
        for p in range(PARTS):
            for i in range(2):
                wdn[p, i, pl.ds(half_ff, fill), :] = jnp.zeros((fill, wdn.shape[3]), jnp.bfloat16)
    relayed = gather_relay(state)
    forwards((0, 1), (0, 2), (0, 3), (1, 1), (1, 2))()
    y_own(6, 7, role=outer)
    forwards((1, 3))()
    gather_pass(state, relayed)
    forwards((2, 1))()
    gather_end(relayed)
    forwards((2, 2))()
    with scope("norm1"):
        norm(x1, gain1, nb)
    forwards((2, 3))()
    y_own(4)
    near(4)
    far(4)

    @pl.when(inner)
    def _():
        near(5, 6, 7)


    with scope("arrive01"):
        arrive(0)
        arrive(1)
    both = jnp.dot(nb[...], win[...], preferred_element_type=jnp.float32)
    branch_in, branch_gate = both[:, :LANES], both[:, LANES:]
    row = lax.broadcasted_iota(jnp.int32, branch_in.shape, 0)
    pos = jnp.where(row >= rows, row - rows, row)

    def shifted(values, by, fill):
        return jnp.where(pos >= by, pltpu.roll(values, by, 0), fill)

    tap_count = taps.shape[0]
    my = span(h, LANES)
    conv = branch_in * taps[tap_count - 1 :, my]
    for j in range(tap_count - 1):
        conv = conv + shifted(branch_in, tap_count - 1 - j, 0.0) * taps[j : j + 1, my]
    conv = conv.astype(jnp.bfloat16)
    gate_x = jax.nn.sigmoid(jnp.dot(conv, gxb[h], preferred_element_type=jnp.float32))
    gate_a = jax.nn.sigmoid(jnp.dot(conv, gab[h], preferred_element_type=jnp.float32))
    log_decay = -gate_power * gate_a * forget[:, my]
    decay = jnp.exp(log_decay)
    scale = jnp.sqrt(-jnp.tanh(log_decay) * (1.0 + decay * decay))
    scale = jnp.where(pos == 0, 1.0, scale)
    run = conv.astype(jnp.float32) * gate_x * scale
    by = 1
    while by < rows:
        run = decay * shifted(run, by, 0.0) + run
        decay = decay * shifted(decay, by, 1.0)
        by *= 2
    mix[...] = (run * jax.nn.gelu(branch_gate)).astype(jnp.bfloat16)
    y_own(5, 6, 7, role=inner)
    forwards((3, 1))()
    with scope("arrive2"):
        arrive(2)

    def refill():
        @pl.when(outer)
        def _():
            near(5, 6, 7)

        far(5)
        forwards((4, 1))()

    scatter(0, mix, wout, s1, s1r, k1, x1r, zs1, z1r, tok, after, (forwards((3, 2)), refill, forwards((3, 3))))
    state = gather_start(1, after, x2)
    far(6, 7)

    forwards((4, 2), (5, 1), (6, 1), (7, 1))()
    relayed = gather_relay(state)
    forwards((4, 3))()
    gather_pass(state, relayed)
    forwards((5, 2))()
    gather_end(relayed)
    with scope("norm2"):
        norm(x2, gain2, nb)
    forwards((5, 3), (6, 2))()
    with scope("arrive34"):
        arrive(3)
        arrive(4)
    last = (((1,), (1,)), ((), ()))

    with scope("ffn"):
        gate_val = lax.dot_general(nb[...], wgate[...], last, preferred_element_type=jnp.float32)
        up_val = lax.dot_general(nb[...], wup[...], last, preferred_element_type=jnp.float32)
        hid[...] = (jax.nn.silu(gate_val) * up_val).astype(jnp.bfloat16)
    hid_copy = send(hid, hidp, core_send.at[3, 0], core_recv.at[3, 0], (f, t_core))
    forwards((7, 2), (6, 3), (7, 3))()
    with scope("arrive5"):
        hid_copy.wait_recv()
        arrive(5)
    sent = len(started)
    first = finish(0, hid)
    first[0]()
    with scope("arrive6"):
        arrive(6)
        arrive(7)
    second = finish(1, hid)
    second[0]()
    first[1]()
    second[1]()
    for copy in started[:sent]:
        copy.wait_send()
    for other, copy in core_copies:
        pl.when(other)(copy.wait_send)

    @pl.when(inner)
    def _():
        for group in groups:
            z_sends[group, 2].wait_send()
            relays[group].wait_send()

    first[2]()
    second[2]()
    with scope("drain"):
        for copy in started[sent:]:
            copy.wait_send()


def on_device_paired(
    tokens, mix_gain, in_x_w, in_gate_w, conv_taps, gate_x_blocks, gate_a_blocks, forget_rate,
    out_w, ffn_gain, ffn_gate_w, ffn_up_w, ffn_down_w,
):
    rows, feats = tokens.shape
    model = mix_gain.shape[0]
    both = 2 * rows
    share = feats // PARTS
    wide = -(-ffn_down_w.shape[0] // (2 * LANES)) * LANES
    bf, dma = jnp.bfloat16, pltpu.SemaphoreType.DMA
    exchange = [
        pltpu.VMEM((both, model), bf),
        pltpu.VMEM((2, both, feats), bf),
        pltpu.VMEM((2, both, feats), bf),
        pltpu.VMEM((both, feats), bf),
    ]
    vmem = pl.BlockSpec(memory_space=pltpu.VMEM)
    operands = (
        tokens, mix_gain.reshape(1, model), in_x_w, in_gate_w, conv_taps, gate_x_blocks, gate_a_blocks,
        forget_rate.reshape(1, -1), out_w, ffn_gain.reshape(1, model), ffn_gate_w.T, ffn_up_w.T, ffn_down_w,
    )
    return pl.pallas_call(
        kernel,
        out_shape=jax.ShapeDtypeStruct((rows, feats), bf),
        in_specs=[pl.BlockSpec(memory_space=pltpu.HBM)] * 13,
        out_specs=vmem,
        scratch_shapes=[
            *[pltpu.VMEM(operand.shape, operand.dtype) for operand in operands],
            dma((13,)),
            pltpu.VMEM((both, model), bf),
            pltpu.VMEM((both, model), bf),
            pltpu.VMEM((model, 2 * LANES), bf),
            pltpu.VMEM((LANES, model), bf),
            pltpu.VMEM((wide, model), bf),
            pltpu.VMEM((wide, model), bf),
            pltpu.VMEM((PARTS, 2, wide, model // PARTS), bf),
            pltpu.VMEM((both, wide), bf),
            *exchange,
            pltpu.VMEM((rows, feats), bf),
            pltpu.VMEM((rows, feats), bf),
            pltpu.VMEM((rows, feats), bf),
            pltpu.VMEM((both, LANES), bf),
            pltpu.VMEM((both, model), bf),
            pltpu.VMEM((both, wide), bf),
            pltpu.VMEM((PARTS, 2, both, share), bf),
            pltpu.VMEM((PARTS, both, share), bf),
            pltpu.VMEM((PARTS, rows, share), bf),
            pltpu.VMEM((PARTS, 2, rows, share), bf),
            dma((8, 4)), dma((8, 3)), dma((8, 4)), dma((8, 4)), dma((8,)),
            dma((2, 11)), dma((2, 11)), dma((1, 5)), dma((1, 5)), dma((PARTS, 8)), dma((PARTS, 8)),
            dma((3, 2, 2)), dma((4, 4)), dma((4, 2)),
        ],
        compiler_params=pltpu.CompilerParams(
            collective_id=0, has_side_effects=True, vmem_limit_bytes=48 * 1024 * 1024
        ),
    )(*[pltpu.with_memory_space_constraint(operand, pltpu.HBM) for operand in operands])


def solution(mesh):
    def body(*args):
        if paired(mesh, *args):
            return on_device_paired(*args)
        return on_device(*args)

    placed = (
        P("fs", "tp"),
        P(),
        P("fs", "tp"),
        P("fs", "tp"),
        P(None, "tp"),
        P("tp", None, None),
        P("tp", None, None),
        P("tp"),
        P("tp", "fs"),
        P(),
        P("fs", "tp"),
        P("fs", "tp"),
        P("tp", "fs"),
    )
    return jax.shard_map(
        body, mesh=mesh, in_specs=placed, out_specs=P("fs", "tp"), check_vma=False
    )
```

```python
import functools

import jax
import jax.numpy as jnp
from jax import lax
from jax.experimental import pallas as pl
from jax.experimental.pallas import tpu as pltpu
from jax.sharding import PartitionSpec as P

LANES = 128

epsilon = 1e-06
gate_power = 8.0


def rms_norm(values, gain):
    wide = values.astype(jnp.float32)
    mean_square = jnp.mean(wide * wide, axis=-1, keepdims=True)
    return (wide * lax.rsqrt(mean_square + epsilon) * gain).astype(jnp.bfloat16)


def full_rows(shard):
    return lax.all_gather(shard, "tp", axis=1, tiled=True)


def pair_folder(left_rows, pieces):
    return (
        jnp.dot(left_rows, pieces[0], preferred_element_type=jnp.float32),
        jnp.dot(left_rows, pieces[1], preferred_element_type=jnp.float32),
    )


def project_out(acts, weight):
    partial_terms = jnp.dot(
        acts, lax.all_gather(weight, "fs", axis=1, tiled=True), preferred_element_type=jnp.float32
    )
    return lax.psum_scatter(
        partial_terms.astype(jnp.bfloat16), "tp", scatter_dimension=1, tiled=True
    ).astype(jnp.float32)


def combine(earlier, later):
    return (earlier[0] * later[0], later[0] * earlier[1] + later[1])


def on_device(
    tokens,
    mix_gain,
    in_x_w,
    in_gate_w,
    conv_taps,
    gate_x_blocks,
    gate_a_blocks,
    forget_rate,
    out_w,
    ffn_gain,
    ffn_gate_w,
    ffn_up_w,
    ffn_down_w,
):
    normed = rms_norm(full_rows(tokens), mix_gain)
    length = normed.shape[0]
    chan_width = in_x_w.shape[1]
    branch_in, branch_gate = pair_folder(
        normed,
        (
            lax.all_gather(in_x_w, "fs", axis=0, tiled=True),
            lax.all_gather(in_gate_w, "fs", axis=0, tiled=True),
        ),
    )
    tap_count = conv_taps.shape[0]
    padded = jnp.pad(branch_in, ((tap_count - 1, 0), (0, 0)))
    conv_sum = padded[0:length] * conv_taps[0]
    for index in range(1, tap_count):
        conv_sum = conv_sum + padded[index : index + length] * conv_taps[index]
    conv_out = conv_sum.astype(jnp.bfloat16)
    blocks = gate_x_blocks.shape[0]
    block_dim = gate_x_blocks.shape[1]
    grouped = conv_out.reshape(length, blocks, block_dim)
    gate_x = jax.nn.sigmoid(
        jnp.einsum(
            "tbi,bij->tbj", grouped, gate_x_blocks, preferred_element_type=jnp.float32
        ).reshape(length, chan_width)
    )
    gate_a = jax.nn.sigmoid(
        jnp.einsum(
            "tbi,bij->tbj", grouped, gate_a_blocks, preferred_element_type=jnp.float32
        ).reshape(length, chan_width)
    )
    log_decay = -gate_power * gate_a * forget_rate
    decay = jnp.exp(log_decay)
    scale = jnp.sqrt(-jnp.expm1(2.0 * log_decay))
    scale = jnp.where((jnp.arange(length) == 0)[:, None], 1.0, scale)
    driven = conv_out.astype(jnp.float32) * gate_x * scale
    _, state = lax.associative_scan(combine, (decay, driven), axis=0)
    mixer_out = (state * jax.nn.gelu(branch_gate)).astype(jnp.bfloat16)
    after_mix = (tokens.astype(jnp.float32) + project_out(mixer_out, out_w)).astype(jnp.bfloat16)
    normed_ffn = rms_norm(full_rows(after_mix), ffn_gain)
    gate_val, up_val = pair_folder(
        normed_ffn,
        (
            lax.all_gather(ffn_gate_w, "fs", axis=0, tiled=True),
            lax.all_gather(ffn_up_w, "fs", axis=0, tiled=True),
        ),
    )
    hidden = (jax.nn.silu(gate_val) * up_val).astype(jnp.bfloat16)
    return (after_mix.astype(jnp.float32) + project_out(hidden, ffn_down_w)).astype(jnp.bfloat16)


def paired(mesh, tokens, mix_gain, in_x_w, in_gate_w, conv_taps, gate_x_blocks, *rest):
    ffn_down_w = rest[-1]
    return (
        mesh.shape["fs"] == 8
        and mesh.shape["tp"] == 4
        and gate_x_blocks.shape == (2, LANES, LANES)
        and tokens.shape[0] % 32 == 0
        and tokens.shape[1] == 4 * LANES
        and ffn_down_w.shape[1] == 2 * LANES
        and ffn_down_w.shape[0] % 32 == 0
    )


PARTS = 2


def kernel(
    h_tok, h_gain1, h_x, h_g, h_taps, h_gxb, h_gab, h_forget, h_out, h_gain2, h_gate, h_up, h_dn,
    result,
    tok, gain1, w_x, w_g, taps, gxb, gab, forget, w_out, gain2, w_gate, w_up, w_dn, load_sem,
    x1, nb, win, wout, wgate, wup, wdn, hidp, s1, s1r, k1, x1r, zs1, z1r, after, mix, x2, hid,
    k2, x2r, zs2, z2r,
    send_z, recv_z, send_y, recv_y, own_sem, ag_send, ag_recv, rs_send, rs_recv, fin_send, fin_recv,
    cross_recv, core_send, core_recv,
):
    f, t = lax.axis_index("fs"), lax.axis_index("tp")
    z, y = f // 2, f % 2
    h = z % 2
    outer = (z == 0) | (z == 3)
    inner = (z == 1) | (z == 2)
    rows, feats = tok.shape
    near_z = z + 1 - 2 * h
    far_outer = 3 * (1 - z // 2)
    far_inner = 2 - z // 2
    sources = (z, near_z, far_outer, far_inner)
    fz = tuple(zz * 2 + y for zz in sources)
    fy = z * 2 + 1 - y
    t_core = t + 1 - 2 * (t % 2)
    t_x = (t + 2) % 4
    t_xc = (t_core + 2) % 4
    model = x1.shape[1]
    scope = jax.named_scope

    held = (tok, w_x, w_g, w_out, w_gate, w_up, w_dn, gain1, taps, gxb, gab, forget, gain2)
    given = (h_tok, h_x, h_g, h_out, h_gate, h_up, h_dn, h_gain1, h_taps, h_gxb, h_gab, h_forget, h_gain2)
    loads = [pltpu.make_async_copy(src, dst, load_sem.at[i]) for i, (src, dst) in enumerate(zip(given, held))]
    for load in loads:
        load.start()

    barrier = pltpu.get_barrier_semaphore()
    peers = [(fz[1], t), (fz[3], t), (fy, t), (fy, t_core), (f, t_core), (f, t_x)]

    def greet(peer):
        pl.semaphore_signal(barrier, inc=1, device_id=peer, device_id_type=pl.DeviceIdType.MESH)

    for peer in peers:
        greet(peer)

    @pl.when(inner)
    def _():
        greet((fz[2], t))

    with scope("barrier"):
        pl.semaphore_wait(barrier, len(peers) + jnp.where(inner, 1, 0))

    started = []

    def describe(src, dst, s_sem, r_sem, peer):
        return pltpu.make_async_remote_copy(
            src_ref=src, dst_ref=dst, send_sem=s_sem, recv_sem=r_sem,
            device_id=peer, device_id_type=pl.DeviceIdType.MESH,
        )

    def send(src, dst, s_sem, r_sem, peer):
        copy = describe(src, dst, s_sem, r_sem, peer)
        copy.start()
        started.append(copy)
        return copy

    def span(index, width):
        return pl.ds(pl.multiple_of(index * width, width), width)

    depth = w_x.shape[0]
    cols = w_out.shape[1]
    part_cols = cols // PARTS
    half_ff = w_dn.shape[0] // 2
    fill = wgate.shape[0] - half_ff
    last_group = 5 + PARTS
    quarter = half_ff // 2
    core = t % 2

    def piece(group, half, stored=False):
        if group < 2:
            return ((h_x, h_g) if stored else (w_x, w_g))[group].at[:, span(half, LANES)]
        if group == 2:
            return (h_out if stored else w_out).at[span(half, LANES), :]
        if group < 5:
            return ((h_gate, h_up) if stored else (w_gate, w_up))[group - 3].at[span(half, half_ff), :]
        down = h_dn if stored else w_dn
        if group == 5:
            return down.at[span(half, half_ff), pl.ds(0, part_cols)]
        return down.at[span(2 * half + group - 6, quarter), pl.ds(part_cols, part_cols)]

    def place(group, source):
        if group < 2:
            return win.at[span(source, depth), pl.ds(group * LANES, LANES)]
        if group == 2:
            return wout.at[:, span(source, cols)]
        if group < 5:
            return (wgate, wup)[group - 3].at[pl.ds(0, half_ff), span(source, cols)]
        if group == 5:
            return wdn.at[0, core, pl.ds(0, half_ff), span(source, part_cols)]
        return wdn.at[1, core, pl.ds((group - 6) * quarter, quarter), span(source, part_cols)]

    groups = range(last_group + 1)
    own_copies = {}
    for group in groups:
        own_copies[group] = pltpu.make_async_copy(piece(group, h, True), place(group, f), own_sem.at[group])
        own_copies[group].start()

    slot = jnp.where(outer, 2, 3)
    z_sends = {}
    for group in groups:
        for way, peer in ((1, fz[1]), (2, fz[2]), (3, fz[3])):
            half = (1 - h, far_outer % 2, far_inner % 2)[way - 1]
            at = 1 if way == 1 else slot
            z_sends[group, way] = describe(
                piece(group, half), place(group, f), send_z.at[group, way - 1], recv_z.at[group, at - 1], (peer, t)
            )
            if way != 2:
                started.append(z_sends[group, way])
    y_copies, relays = {}, {}

    after_relay = {
        0: ((2, 2), (2, 3)), 2: ((3, 2), (3, 3)), 3: ((4, 2), (4, 3)), 4: ((5, 2), (5, 3)), 5: ((6, 2), (7, 2)), 7: ((6, 3), (7, 3)),
    }

    def near(*names):
        for group in names:
            z_sends[group, 1].start()

    def far(*names):
        @pl.when(outer)
        def _():
            for group in names:
                z_sends[group, 3].start()

    core_copies = []

    def send_y_piece(group, d, src, dst, source_z):
        if group < 5:
            return describe(src, dst, send_y.at[group, d], recv_y.at[group, d], (fy, t))
        arrived = cross_recv.at[group - 5, core, source_z // 2]
        return describe(src, dst, send_y.at[group, d], arrived, (fy, t - core + source_z % 2))

    def pass_to_core(group, d, src, dst, source_z):
        if group >= 5:
            copy = describe(
                src, dst, core_send.at[group - 5, d], core_recv.at[group - 5, source_z // 2], (f, t_core)
            )
            other = source_z % 2 != core
            core_copies.append((other, copy))
            pl.when(other)(copy.start)

    for group in groups:
        y_copies[group, 0] = send_y_piece(group, 0, piece(group, h), place(group, f), z)
        started.append(y_copies[group, 0])

    def y_own(*names, role=None):
        def go():
            for group in names:
                y_copies[group, 0].start()

        go() if role is None else pl.when(role)(go)

    def core_own():
        for group in groups[5:]:
            pass_to_core(group, 0, piece(group, h), place(group, f), z)

    def pick(when_inner, when_outer):
        return jnp.where(inner, when_inner, when_outer)

    early = (pick(1, 3), pick(2, 1), pick(3, 2)), (pick(fz[1], fz[3]), pick(fz[2], fz[1]), pick(fz[3], fz[2]))
    middle = (1, 3, 2), (fz[1], fz[3], fz[2])
    late = (1, pick(2, 3), pick(3, 2)), (fz[1], pick(fz[2], fz[3]), pick(fz[3], fz[2]))

    def forward(group, d):
        arrival, arrival_fz = early if group < 3 else middle if group < 5 else late
        block = place(group, arrival_fz[d - 1])
        describe(
            block, block, send_z.at[group, 0], recv_z.at[group, arrival[d - 1] - 1], (fz[1], t)
        ).wait_recv()
        y_copies[group, d] = send_y_piece(group, d, block, block, arrival_fz[d - 1] // 2)
        y_copies[group, d].start()
        started.append(y_copies[group, d])
        pass_to_core(group, d, block, block, arrival_fz[d - 1] // 2)
        if d == 1:
            relays[group] = describe(block, block, send_z.at[group, 3], recv_z.at[group, 1], (fz[2], t))

            @pl.when(inner)
            def _():
                relays[group].start()
                for key in after_relay.get(group, ()):
                    z_sends[key].start()

    def arrive(group):
        own_copies[group].wait()
        if group < 5:
            for d in range(4):
                y_copies[group, d].wait_recv()
            return
        block = place(group, f)
        ready = [cross_recv.at[group - 5, i, j] for i in range(2) for j in range(2)]
        for semaphore in ready + [core_recv.at[group - 5, j] for j in range(2)]:
            describe(block, block, send_y.at[group, 0], semaphore, (fy, t)).wait_recv()

    mine, theirs = span(h, rows), span(1 - h, rows)
    cut = rows // 2

    def some(block, c):
        return pl.ds(pl.multiple_of(block * rows + c * cut, cut), cut)

    def gather_start(k, own, x):
        x_peer, core_peer = (f, t_x), (f, t_core)

        def go(i, src, dst, peer):
            return send(src, dst, ag_send.at[k, i], ag_recv.at[k, i], peer)

        at = span(t, feats)
        by_z = [go(c, own.at[pl.ds(c * cut, cut), :], x.at[some(h, c), at], (fz[1], t)) for c in range(2)]
        by_x = go(2, own, x.at[mine, at], x_peer)
        by_core = go(3, own, x.at[mine, at], core_peer)
        x[mine, at] = own[...]
        return go, by_z, by_x, by_core, x_peer, core_peer, x

    def gather_relay(state):
        go, by_z, by_x, by_core, x_peer, core_peer, x = state
        across, inside = [], [by_core]
        at = span(t, feats)
        with scope("byz"):
            for c in range(2):
                by_z[c].wait_recv()
                block = x.at[some(1 - h, c), at]
                across.append(go(4 + c, block, block, x_peer))
                inside.append(go(6 + c, block, block, core_peer))
        with scope("byx"):
            by_x.wait_recv()
        block = x.at[mine, span(t_x, feats)]
        inside.append(go(8, block, block, core_peer))
        return across, inside

    def gather_pass(state, relayed):
        go, core_peer, x = state[0], state[5], state[6]
        across, inside = relayed
        with scope("across"):
            for c in range(2):
                across[c].wait_recv()
                block = x.at[some(1 - h, c), span(t_x, feats)]
                inside.append(go(9 + c, block, block, core_peer))

    def gather_end(relayed):
        with scope("inside"):
            for copy in relayed[1]:
                copy.wait_recv()

    def norm(x, gain, out):
        step = 32

        def one(i, carry):
            at = pl.ds(pl.multiple_of(i * step, step), step)
            wide = x[at, :].astype(jnp.float32)
            scale = lax.rsqrt(jnp.mean(wide * wide, axis=-1, keepdims=True) + epsilon)
            out[at, :] = (wide * scale * gain[...]).astype(jnp.bfloat16)
            return carry

        lax.fori_loop(0, x.shape[0] // step, one, 0)

    def scatter(k, acts, weight, s, r1, keep, r2, s3, r3, base, out, hooks):
        core_peer, x_peer = (f, t_core), (f, t_x)

        def project(block):
            at = span(block, feats)
            s[:, at] = jnp.dot(acts[...], weight[:, at], preferred_element_type=jnp.float32).astype(jnp.bfloat16)
            return s.at[:, at]

        a = send(project(t_xc), r1.at[0], rs_send.at[k, 0], rs_recv.at[k, 0], core_peer)
        b = send(project(t_core), r1.at[1], rs_send.at[k, 1], rs_recv.at[k, 1], core_peer)
        project(t_x)
        project(t)
        with scope("rs_a"):
            a.wait_recv()
        at = span(t_x, feats)
        for i, block in ((0, theirs), (1, mine)):
            keep[0, block, :] = (s[block, at].astype(jnp.float32) + r1[0, block, :].astype(jnp.float32)).astype(jnp.bfloat16)
            copy = send(keep.at[0, block], r2.at[block], rs_send.at[k, 2 + i], rs_recv.at[k, 2 + i], x_peer)
            if i == 0:
                c0 = copy
        c1 = copy
        hooks[0]()
        with scope("rs_c0"):
            b.wait_recv()
            c0.wait_recv()

        def total(where):
            return (
                s[where, span(t, feats)].astype(jnp.float32)
                + r1[1, where, :].astype(jnp.float32)
                + r2[where, :].astype(jnp.float32)
            )

        s3[...] = total(theirs).astype(jnp.bfloat16)
        e = send(s3, r3, rs_send.at[k, 4], rs_recv.at[k, 4], (fz[1], t))
        hooks[1]()
        with scope("rs_c1"):
            c1.wait_recv()
        part = total(mine)
        hooks[2]()
        with scope("rs_e"):
            e.wait_recv()
        out[...] = (base[...].astype(jnp.float32) + (part + r3[...].astype(jnp.float32))).astype(jnp.bfloat16)

    def finish(p, acts):
        x_peer, z_peer = (f, t_x), (fz[1], t)
        wide = feats // PARTS
        low, high = pl.ds(0, wide // 2), pl.ds(wide // 2, wide // 2)
        keep, r2, s3, r3 = k2.at[p], x2r.at[p], zs2.at[p], z2r.at[p]

        def project_pair(i, block, where):
            at = span(block, wide)
            keep[i, where, :] = (
                jnp.dot(acts[where, :], wdn[p, core, :, at], preferred_element_type=jnp.float32)
                + jnp.dot(hidp[where, :], wdn[p, 1 - core, :, at], preferred_element_type=jnp.float32)
            ).astype(jnp.bfloat16)

        def go(i, src, dst, peer):
            return send(src, dst, fin_send.at[p, i], fin_recv.at[p, i], peer)

        waits = {}

        def cross():
            project_pair(0, t_x, theirs)
            waits["c"] = go(2, keep.at[0, theirs, low], r2.at[theirs, low], x_peer)
            waits["d"] = go(3, keep.at[0, theirs, high], r3.at[0, :, high], z_peer)
            project_pair(1, t, theirs)
            waits["e"] = go(4, keep.at[1, theirs, high], r3.at[1, :, high], z_peer)
            project_pair(0, t_x, mine)
            waits["m"] = go(7, keep.at[0, mine, low], r2.at[mine, low], x_peer)
            project_pair(1, t, mine)

        def turn():
            with scope(f"fin_d{p}"):
                waits["d"].wait_recv()
            s3[:, high] = (
                keep[0, mine, high].astype(jnp.float32) + r3[0, :, high].astype(jnp.float32)
            ).astype(jnp.bfloat16)
            waits["g"] = go(5, s3.at[:, high], r2.at[pl.ds(0, rows), high], x_peer)
            with scope(f"fin_c{p}"):
                waits["c"].wait_recv()
            s3[:, low] = (
                keep[1, theirs, low].astype(jnp.float32) + r2[theirs, low].astype(jnp.float32)
            ).astype(jnp.bfloat16)
            waits["l"] = go(6, s3.at[:, low], r3.at[0, :, low], z_peer)

        def end():
            with scope(f"fin_g{p}"):
                waits["e"].wait_recv()
                waits["g"].wait_recv()
            left, right = pl.ds(p * part_cols, part_cols), pl.ds(cols + p * part_cols, part_cols)
            result[:, right] = (
                after[:, right].astype(jnp.float32)
                + (keep[1, mine, high].astype(jnp.float32) + r3[1, :, high].astype(jnp.float32))
                + r2[pl.ds(0, rows), high].astype(jnp.float32)
            ).astype(jnp.bfloat16)
            with scope(f"fin_l{p}"):
                waits["m"].wait_recv()
                waits["l"].wait_recv()
            result[:, left] = (
                after[:, left].astype(jnp.float32)
                + (keep[1, mine, low].astype(jnp.float32) + r2[mine, low].astype(jnp.float32))
                + r3[0, :, low].astype(jnp.float32)
            ).astype(jnp.bfloat16)

        return cross, turn, end

    def forwards(*pairs):
        def go():
            for group, d in pairs:
                with scope(f"fw{group}{d}"):
                    forward(group, d)

        return go

    nothing = forwards()
    for load in loads[:1]:
        load.wait()
    state = gather_start(0, tok, x1)
    for load in loads[1:]:
        load.wait()
    y_own(0, 1)

    for group in range(4):
        near(group)
        far(group)

    @pl.when(inner)
    def _():
        for group in range(2):
            z_sends[group, 2].start()
            z_sends[group, 3].start()

    y_own(2, 3)
    y_own(5, role=outer)
    core_own()
    if fill:
        for w in (wgate, wup):
            w[pl.ds(half_ff, fill), :] = jnp.zeros((fill, model), jnp.bfloat16)
        for p in range(PARTS):
            for i in range(2):
                wdn[p, i, pl.ds(half_ff, fill), :] = jnp.zeros((fill, wdn.shape[3]), jnp.bfloat16)
    relayed = gather_relay(state)
    forwards((0, 1), (0, 2), (0, 3), (1, 1), (1, 2))()
    y_own(6, 7, role=outer)
    forwards((1, 3))()
    gather_pass(state, relayed)
    forwards((2, 1))()
    gather_end(relayed)
    forwards((2, 2))()
    with scope("norm1"):
        norm(x1, gain1, nb)
    forwards((2, 3))()
    y_own(4)
    near(4)
    far(4)

    @pl.when(inner)
    def _():
        near(5, 6, 7)


    with scope("arrive01"):
        arrive(0)
        arrive(1)
    both = jnp.dot(nb[...], win[...], preferred_element_type=jnp.float32)
    branch_in, branch_gate = both[:, :LANES], both[:, LANES:]
    row = lax.broadcasted_iota(jnp.int32, branch_in.shape, 0)
    pos = jnp.where(row >= rows, row - rows, row)

    def shifted(values, by, fill):
        return jnp.where(pos >= by, pltpu.roll(values, by, 0), fill)

    tap_count = taps.shape[0]
    my = span(h, LANES)
    conv = branch_in * taps[tap_count - 1 :, my]
    for j in range(tap_count - 1):
        conv = conv + shifted(branch_in, tap_count - 1 - j, 0.0) * taps[j : j + 1, my]
    conv = conv.astype(jnp.bfloat16)
    gate_x = jax.nn.sigmoid(jnp.dot(conv, gxb[h], preferred_element_type=jnp.float32))
    gate_a = jax.nn.sigmoid(jnp.dot(conv, gab[h], preferred_element_type=jnp.float32))
    log_decay = -gate_power * gate_a * forget[:, my]
    decay = jnp.exp(log_decay)
    scale = jnp.sqrt(-jnp.tanh(log_decay) * (1.0 + decay * decay))
    scale = jnp.where(pos == 0, 1.0, scale)
    run = conv.astype(jnp.float32) * gate_x * scale
    by = 1
    while by < rows:
        run = decay * shifted(run, by, 0.0) + run
        decay = decay * shifted(decay, by, 1.0)
        by *= 2
    mix[...] = (run * jax.nn.gelu(branch_gate)).astype(jnp.bfloat16)
    y_own(5, 6, 7, role=inner)
    forwards((3, 1))()
    with scope("arrive2"):
        arrive(2)

    def refill():
        @pl.when(outer)
        def _():
            near(5, 6, 7)

        far(5)
        forwards((4, 1))()

    scatter(0, mix, wout, s1, s1r, k1, x1r, zs1, z1r, tok, after, (forwards((3, 2)), refill, forwards((3, 3))))
    state = gather_start(1, after, x2)
    far(6, 7)

    forwards((4, 2), (5, 1), (6, 1), (7, 1))()
    relayed = gather_relay(state)
    forwards((4, 3))()
    gather_pass(state, relayed)
    forwards((5, 2))()
    gather_end(relayed)
    with scope("norm2"):
        norm(x2, gain2, nb)
    forwards((5, 3), (6, 2))()
    with scope("arrive34"):
        arrive(3)
        arrive(4)
    last = (((1,), (1,)), ((), ()))

    with scope("ffn"):
        gate_val = lax.dot_general(nb[...], wgate[...], last, preferred_element_type=jnp.float32)
        up_val = lax.dot_general(nb[...], wup[...], last, preferred_element_type=jnp.float32)
        hid[...] = (jax.nn.silu(gate_val) * up_val).astype(jnp.bfloat16)
    hid_copy = send(hid, hidp, core_send.at[3, 0], core_recv.at[3, 0], (f, t_core))
    forwards((7, 2), (6, 3), (7, 3))()
    with scope("arrive5"):
        hid_copy.wait_recv()
        arrive(5)
    sent = len(started)
    first = finish(0, hid)
    first[0]()
    with scope("arrive6"):
        arrive(6)
        arrive(7)
    second = finish(1, hid)
    second[0]()
    first[1]()
    second[1]()
    for copy in started[:sent]:
        copy.wait_send()
    for other, copy in core_copies:
        pl.when(other)(copy.wait_send)

    @pl.when(inner)
    def _():
        for group in groups:
            z_sends[group, 2].wait_send()
            relays[group].wait_send()

    first[2]()
    second[2]()
    with scope("drain"):
        for copy in started[sent:]:
            copy.wait_send()


def on_device_paired(
    tokens, mix_gain, in_x_w, in_gate_w, conv_taps, gate_x_blocks, gate_a_blocks, forget_rate,
    out_w, ffn_gain, ffn_gate_w, ffn_up_w, ffn_down_w,
):
    rows, feats = tokens.shape
    model = mix_gain.shape[0]
    both = 2 * rows
    share = feats // PARTS
    wide = -(-ffn_down_w.shape[0] // (2 * LANES)) * LANES
    bf, dma = jnp.bfloat16, pltpu.SemaphoreType.DMA
    exchange = [
        pltpu.VMEM((both, model), bf),
        pltpu.VMEM((2, both, feats), bf),
        pltpu.VMEM((2, both, feats), bf),
        pltpu.VMEM((both, feats), bf),
    ]
    vmem = pl.BlockSpec(memory_space=pltpu.VMEM)
    operands = (
        tokens, mix_gain.reshape(1, model), in_x_w, in_gate_w, conv_taps, gate_x_blocks, gate_a_blocks,
        forget_rate.reshape(1, -1), out_w, ffn_gain.reshape(1, model), ffn_gate_w.T, ffn_up_w.T, ffn_down_w,
    )
    return pl.pallas_call(
        kernel,
        out_shape=jax.ShapeDtypeStruct((rows, feats), bf),
        in_specs=[pl.BlockSpec(memory_space=pltpu.HBM)] * 13,
        out_specs=vmem,
        scratch_shapes=[
            *[pltpu.VMEM(operand.shape, operand.dtype) for operand in operands],
            dma((13,)),
            pltpu.VMEM((both, model), bf),
            pltpu.VMEM((both, model), bf),
            pltpu.VMEM((model, 2 * LANES), bf),
            pltpu.VMEM((LANES, model), bf),
            pltpu.VMEM((wide, model), bf),
            pltpu.VMEM((wide, model), bf),
            pltpu.VMEM((PARTS, 2, wide, model // PARTS), bf),
            pltpu.VMEM((both, wide), bf),
            *exchange,
            pltpu.VMEM((rows, feats), bf),
            pltpu.VMEM((rows, feats), bf),
            pltpu.VMEM((rows, feats), bf),
            pltpu.VMEM((both, LANES), bf),
            pltpu.VMEM((both, model), bf),
            pltpu.VMEM((both, wide), bf),
            pltpu.VMEM((PARTS, 2, both, share), bf),
            pltpu.VMEM((PARTS, both, share), bf),
            pltpu.VMEM((PARTS, rows, share), bf),
            pltpu.VMEM((PARTS, 2, rows, share), bf),
            dma((8, 4)), dma((8, 3)), dma((8, 4)), dma((8, 4)), dma((8,)),
            dma((2, 11)), dma((2, 11)), dma((1, 5)), dma((1, 5)), dma((PARTS, 8)), dma((PARTS, 8)),
            dma((3, 2, 2)), dma((4, 4)), dma((4, 2)),
        ],
        compiler_params=pltpu.CompilerParams(
            collective_id=0, has_side_effects=True, vmem_limit_bytes=48 * 1024 * 1024
        ),
    )(*[pltpu.with_memory_space_constraint(operand, pltpu.HBM) for operand in operands])


def solution(mesh):
    def body(*args):
        if paired(mesh, *args):
            return on_device_paired(*args)
        return on_device(*args)

    placed = (
        P("fs", "tp"),
        P(),
        P("fs", "tp"),
        P("fs", "tp"),
        P(None, "tp"),
        P("tp", None, None),
        P("tp", None, None),
        P("tp"),
        P("tp", "fs"),
        P(),
        P("fs", "tp"),
        P("fs", "tp"),
        P("tp", "fs"),
    )
    return jax.shard_map(
        body, mesh=mesh, in_specs=placed, out_specs=P("fs", "tp"), check_vma=False
    )
```
